32 devices in a mesh: kv: 8 (over z, x), tp: 4 (over y, core).
Axes of the slice: x: 2, y: 2, z: 4, core: 2. Of those that a mesh axis runs over, the one named last changes fastest.
Arguments:
- tokens: bfloat16 [288, 4096], P(None, 'kv'), may hold values from -40 to 40
- norm_gain: float32 [4096], P('kv'), may hold values from 0.1 to 1.9
- query_weight: bfloat16 [4096, 2048], P('kv', 'tp'), may hold values from -0.09375 to 0.09375
- key_weight: bfloat16 [4096, 2048], P('kv', 'tp'), may hold values from -0.09375 to 0.09375
- value_weight: bfloat16 [4096, 2048], P('kv', 'tp'), may hold values from -0.09375 to 0.09375
- gate_weight: bfloat16 [4096, 32], replicated, may hold values from -0.09375 to 0.09375
- gate_bias: float32 [32], replicated, may hold values from -0.5 to 3
- out_weight: bfloat16 [2048, 4096], P('tp', 'kv'), may hold values from -0.125 to 0.125
- cache_keys: bfloat16 [12, 3072, 2048], P(None, 'kv', 'tp'), may hold values from -1000 to 1000
- cache_values: bfloat16 [12, 3072, 2048], P(None, 'kv', 'tp'), may hold values from -6 to 6
- cache_decay: float32 [12, 32, 3072], P(None, 'tp', 'kv'), may hold values from -3072 to 0, as said below
- lengths: int32 [12], replicated, may hold values from 1537 to 3072
- parents: int32 [12, 24], replicated, may hold values from 0 to 23, as said below
Outputs:
- mixed: bfloat16 [288, 4096], P('tp', 'kv')
The draws below stay inside these ranges and needn't reach their ends.
Inputs may be any that keep to these rules, and one draw needn't show every extreme that they name: `cache_decay`: zero at and beyond lengths of the sequence. parents[s, 0] = 0 and parents[s, n] < n for n > 0.
All inputs are finite; a program needn't handle non-finite values.
Results may differ from the reference program's by a relative error of at most 0.014.
The reference program's roundings to bfloat16 on the way count: a program that leaves them out, or rounds other values in their place, can miss the bound.
Values may be sent and summed in bfloat16 or wider, within the bound.
A program may use at most 64 MiB of HBM per device.

```python
import jax
import jax.numpy as jnp
from jax import lax

D = 4096
ATTENTION_HEADS = 32
HEAD_DIM = 64
SEQUENCE_COUNT = 12
PROPS = 24
POS_DEV = 384
ROWS = 288
CACHE_LENGTH = 3072
GROUP_HEADS = 8
N_KV = 8
N_TP = 4


def length_draw(key):
    drawn = jax.random.randint(jax.random.fold_in(key, 11), (SEQUENCE_COUNT,), CACHE_LENGTH // 2 + 1, CACHE_LENGTH + 1).astype(jnp.int32)
    order = jax.random.permutation(jax.random.fold_in(key, 12), SEQUENCE_COUNT)
    drawn = jnp.where(order == 0, CACHE_LENGTH, drawn)
    return drawn.astype(jnp.int32)


def draw_lengths(key, part):
    return length_draw(key)


def draw_parents(key, part):
    nodes = jnp.arange(PROPS, dtype=jnp.int32)
    lowest = jnp.maximum(nodes - 4, 0)
    spread = jnp.maximum(nodes - lowest, 1)
    raw = jax.random.randint(jax.random.fold_in(key, 3), (SEQUENCE_COUNT, PROPS), 0, 1 << 20)
    picked = lowest[None, :] + raw % spread[None, :]
    return jnp.where(nodes[None, :] > 0, picked, 0).astype(jnp.int32)


def draw_tokens(key, part):
    column = jnp.arange(D, dtype=jnp.float32) / D
    jitter = jnp.exp(jax.random.uniform(jax.random.fold_in(key, 1), (D,), jnp.float32, -0.5, 0.5))
    ramp = jnp.exp(jnp.log(0.4) + jnp.log(9.0) * column)
    base = jnp.clip(jax.random.normal(jax.random.fold_in(key, 2), (ROWS, D), jnp.float32), -6.0, 6.0)
    values = base * ramp[None, :] * jitter[None, :]
    return values.astype(jnp.bfloat16)


def draw_cache_keys(key, part):
    shape = (SEQUENCE_COUNT, CACHE_LENGTH, ATTENTION_HEADS * HEAD_DIM)
    base = jnp.clip(jax.random.normal(jax.random.fold_in(key, 1), shape, jnp.float32), -6.0, 6.0)
    return base.astype(jnp.bfloat16)


def draw_cache_decay(key, part):
    lengths = length_draw(key)
    order = jax.random.permutation(jax.random.fold_in(key, 21), ATTENTION_HEADS)
    slow_decay = order < ATTENTION_HEADS // 2
    slow_rate = 0.6 / CACHE_LENGTH * jnp.exp(jax.random.uniform(jax.random.fold_in(key, 22), (ATTENTION_HEADS,), jnp.float32, -0.7, 0.7))
    fast_rate = jnp.exp(-jax.random.uniform(jax.random.fold_in(key, 23), (ATTENTION_HEADS,), jnp.float32, jnp.log(30.0), jnp.log(100.0)))
    rate = jnp.where(slow_decay, slow_rate, fast_rate)
    rough = jnp.exp(jax.random.uniform(jax.random.fold_in(key, 24), (SEQUENCE_COUNT, ATTENTION_HEADS, CACHE_LENGTH), jnp.float32, -0.7, 0.7))
    blocks = jnp.exp(jax.random.uniform(jax.random.fold_in(key, 25), (SEQUENCE_COUNT, ATTENTION_HEADS, CACHE_LENGTH // POS_DEV), jnp.float32, -0.7, 0.7))
    blocks = jnp.repeat(blocks, POS_DEV, axis=2)
    forget_gates = -rate[None, :, None] * rough * blocks
    window_count = jax.random.randint(jax.random.fold_in(key, 26), (SEQUENCE_COUNT, ATTENTION_HEADS, CACHE_LENGTH), 0, CACHE_LENGTH) < 3
    window_length = jax.random.uniform(jax.random.fold_in(key, 27), (SEQUENCE_COUNT, ATTENTION_HEADS, CACHE_LENGTH), jnp.float32, 0.22, 0.69)
    forget_gates = forget_gates - jnp.where(window_count & slow_decay[None, :, None], window_length, 0.0)
    position = jnp.arange(CACHE_LENGTH, dtype=jnp.int32)
    live = position[None, None, :] < lengths[:, None, None]
    forget_gates = jnp.where(live, forget_gates, 0.0)
    running = jnp.cumsum(forget_gates, axis=2)
    return jnp.where(live, running[:, :, -1:] - running, 0.0)


def shard_levels(rng, shape, pieces, least, largest):
    factor_of, own = 1.0, jax.random.fold_in(rng, 6)
    for dim, blocks in pieces:
        steps = jnp.exp(jax.random.uniform(jax.random.fold_in(own, dim), (blocks,), jnp.float32, least / len(pieces), largest / len(pieces)))
        factor_of = factor_of * jnp.repeat(steps, shape[dim] // blocks).reshape([-1 if axis == dim else 1 for axis in range(len(shape))])
    return factor_of


def noise(rng, shape, width, bound, cuts=(), held_as=jnp.bfloat16):
    factor_of = shard_levels(rng, shape, cuts, -0.22, 0.18) if cuts else 1.0
    values = jax.random.normal(rng, shape, jnp.float32) * width * factor_of
    return jnp.minimum(jnp.maximum(values, -bound), bound).astype(held_as)


def setup_inputs(seed: int = 0) -> dict:
    streams_of = jax.random.split(jax.random.key(seed), 14)
    tokens = draw_tokens(jax.random.fold_in(streams_of[13], 71), 0)
    norm_gain = jnp.clip(1.0 + 0.18 * jax.random.normal(streams_of[1], (D,), jnp.float32), 0.1, 1.9)
    query_weight = noise(streams_of[2], (D, ATTENTION_HEADS * HEAD_DIM), D ** -0.5, 0.09375, ((0, 8), (1, 4)))
    key_weight = noise(streams_of[3], (D, ATTENTION_HEADS * HEAD_DIM), D ** -0.5, 0.09375, ((0, 8), (1, 4)))
    value_weight = noise(streams_of[4], (D, ATTENTION_HEADS * HEAD_DIM), D ** -0.5, 0.09375, ((0, 8), (1, 4)))
    gate_weight = noise(streams_of[5], (D, ATTENTION_HEADS), D ** -0.5, 0.09375)
    gate_bias = jnp.clip(jax.random.uniform(streams_of[6], (ATTENTION_HEADS,), jnp.float32, -0.5, 3.0), -0.5, 3.0)
    out_weight = noise(streams_of[7], (ATTENTION_HEADS * HEAD_DIM, D), (ATTENTION_HEADS * HEAD_DIM) ** -0.5, 0.125, ((0, 4), (1, 8)))
    cache_keys = draw_cache_keys(jax.random.fold_in(streams_of[13], 71), 0)
    cache_values = noise(streams_of[9], (SEQUENCE_COUNT, CACHE_LENGTH, ATTENTION_HEADS * HEAD_DIM), 1.0, 6.0, ((1, 8), (2, 4)))
    cache_decay = draw_cache_decay(jax.random.fold_in(streams_of[13], 71), 0)
    lengths = draw_lengths(jax.random.fold_in(streams_of[13], 71), 0)
    parents = draw_parents(jax.random.fold_in(streams_of[13], 71), 0)
    return dict(tokens=tokens, norm_gain=norm_gain, query_weight=query_weight, key_weight=key_weight, value_weight=value_weight, gate_weight=gate_weight, gate_bias=gate_bias, out_weight=out_weight, cache_keys=cache_keys, cache_values=cache_values, cache_decay=cache_decay, lengths=lengths, parents=parents)


def ancestry_of(parents):
    count = parents.shape[1]
    nodes = jnp.arange(count, dtype=jnp.int32)
    link = (parents[:, :, None] == nodes[None, None, :]).astype(jnp.float32)
    link = jnp.maximum(link, jnp.eye(count, dtype=jnp.float32)[None])
    for _ in range(count.bit_length()):
        link = jnp.minimum(jnp.einsum('snm,smk->snk', link, link, precision=lax.Precision.HIGHEST), 1.0)
    return link

def reference(tokens, norm_gain, query_weight, key_weight, value_weight, gate_weight, gate_bias, out_weight, cache_keys, cache_values, cache_decay, lengths, parents):
    scale = HEAD_DIM ** (-0.5)
    xf = tokens.astype(jnp.float32)
    inverse = lax.rsqrt(lax.optimization_barrier(jnp.mean(xf * xf, axis=1, keepdims=True)) + 1e-06)
    normed = (xf * norm_gain).astype(jnp.bfloat16)

    def project(weight):
        return (inverse * jnp.dot(normed, weight, preferred_element_type=jnp.float32)).astype(jnp.bfloat16)
    queries = project(query_weight).astype(jnp.float32).reshape(SEQUENCE_COUNT, PROPS, ATTENTION_HEADS, HEAD_DIM)
    new_keys = project(key_weight).astype(jnp.float32).reshape(SEQUENCE_COUNT, PROPS, ATTENTION_HEADS, HEAD_DIM)
    new_values = project(value_weight).astype(jnp.float32).reshape(SEQUENCE_COUNT, PROPS, ATTENTION_HEADS, HEAD_DIM)
    log_gates = jax.nn.log_sigmoid(inverse * jnp.dot(normed, gate_weight, preferred_element_type=jnp.float32) + gate_bias)
    log_gates = log_gates.reshape(SEQUENCE_COUNT, PROPS, ATTENTION_HEADS)
    ancestry = ancestry_of(parents)
    path = jnp.einsum('snk,skh->snh', ancestry, log_gates, precision=lax.Precision.HIGHEST)

    def cache_block(block):
        start = (block * POS_DEV).astype(jnp.int32)
        keys_blk = lax.dynamic_slice_in_dim(cache_keys, start, POS_DEV, 1).astype(jnp.float32).reshape(SEQUENCE_COUNT, POS_DEV, ATTENTION_HEADS, HEAD_DIM)
        vals_blk = lax.dynamic_slice_in_dim(cache_values, start, POS_DEV, 1).astype(jnp.float32).reshape(SEQUENCE_COUNT, POS_DEV, ATTENTION_HEADS, HEAD_DIM)
        decay_blk = lax.dynamic_slice_in_dim(cache_decay, start, POS_DEV, 2)
        scores = jnp.einsum('snhd,sjhd->snhj', queries, keys_blk) * scale
        scores = scores + path[..., None] + decay_blk[:, None, :, :]
        position = start + jnp.arange(POS_DEV, dtype=jnp.int32)
        live = (position[None, :] < lengths[:, None])[:, None, None, :]
        scores = jnp.where(live, scores, -1e+30)
        top = lax.optimization_barrier(jnp.max(scores, axis=-1))
        weights = jnp.where(live, jnp.exp(scores - top[..., None]), 0.0)
        total = lax.optimization_barrier(jnp.sum(weights, axis=-1))
        rounded = lax.optimization_barrier(weights.astype(jnp.bfloat16)).astype(jnp.float32)
        mix = jnp.einsum('snhj,sjhd->snhd', rounded, vals_blk)
        return (top, total, mix)
    tops, totals, mixes = lax.map(cache_block, jnp.arange(N_KV, dtype=jnp.int32))
    tree_scores = jnp.einsum('snhd,skhd->snhk', queries, new_keys) * scale
    tree_scores = tree_scores + path[..., None] - jnp.swapaxes(path, 1, 2)[:, None, :, :]
    tree_live = ancestry[:, :, None, :] > 0.5
    tree_scores = jnp.where(tree_live, tree_scores, -1e+30)
    tree_top = lax.optimization_barrier(jnp.max(tree_scores, axis=-1))
    tree_weights = jnp.where(tree_live, jnp.exp(tree_scores - tree_top[..., None]), 0.0)
    tree_total = lax.optimization_barrier(jnp.sum(tree_weights, axis=-1))
    tree_rounded = lax.optimization_barrier(tree_weights.astype(jnp.bfloat16)).astype(jnp.float32)
    tree_mix = jnp.einsum('snhk,skhd->snhd', tree_rounded, new_values)
    best = jnp.maximum(lax.optimization_barrier(jnp.max(tops, axis=0)), tree_top)
    factors = jnp.exp(tops - best[None])
    tree_factor = jnp.exp(tree_top - best)
    numer = lax.optimization_barrier(jnp.sum(factors[..., None] * mixes, axis=0)) + tree_factor[..., None] * tree_mix
    denom = lax.optimization_barrier(jnp.sum(factors * totals, axis=0)) + tree_factor * tree_total
    attended = (numer / denom[..., None]).reshape(ROWS, ATTENTION_HEADS * HEAD_DIM).astype(jnp.bfloat16)
    group = GROUP_HEADS * HEAD_DIM
    mixed = jnp.zeros((ROWS, D), jnp.float32)
    for index in range(N_TP):
        part = jnp.dot(attended[:, index * group:(index + 1) * group], out_weight[index * group:(index + 1) * group], preferred_element_type=jnp.float32)
        mixed = mixed + lax.optimization_barrier(part.astype(jnp.bfloat16)).astype(jnp.float32)
    return mixed.astype(jnp.bfloat16)
```

```python
import functools

import jax
import jax.numpy as jnp
from jax import lax
from jax.experimental import pallas as pl
from jax.experimental.pallas import tpu as pltpu
from jax.sharding import PartitionSpec as P

F32 = jnp.float32
BF16 = jnp.bfloat16
LANES = 128
LOW = -1e30
NT = (((1,), (1,)), ((), ()))
HIGH = lax.Precision.HIGHEST


def dot(a, b, precision=None):
    return jnp.dot(a, b, preferred_element_type=F32, precision=precision)


def dot_nt(a, b, precision=None):
    return lax.dot_general(a, b, NT, preferred_element_type=F32, precision=precision)


def fold(x):
    half = x.shape[1] // 2
    return jnp.concatenate([x[:, :half], x[:, half:]], axis=0)


def unfold(x):
    rows = x.shape[0] // 2
    x = x.astype(F32)
    return jnp.concatenate([x[:rows], x[rows:]], axis=1)


def kernel(
    n,
    n_tp,
    tokens_hbm,
    gain_hbm,
    query_hbm,
    key_hbm,
    value_hbm,
    gate_hbm,
    bias_hbm,
    out_hbm,
    keys_hbm,
    values_hbm,
    decay_hbm,
    lengths_hbm,
    parents_hbm,
    out,
    tokens,
    gain,
    query_w,
    key_w,
    value_w,
    bias,
    decay,
    lengths,
    parents,
    small_sem,
    part,
    part_v,
    pair_in,
    pair_in_v,
    part_in,
    part_in_v,
    gate_w,
    out_w,
    keys,
    values,
    qbuf,
    mix,
    stat,
    mix_in,
    stat_in,
    att,
    anc,
    path_s,
    tmix,
    tstat,
    kvnew,
    terms,
    terms_in,
    par_pad,
    load_sem,
    cache_sem,
    p_send,
    p_recv,
    a_send,
    a_recv,
    b_send,
    b_recv,
    c_send,
    c_recv,
    d_send,
    d_recv,
    e_send,
    e_recv,
):
    me = lax.axis_index("kv")
    tp = lax.axis_index("tp")
    rows, depth = tokens.shape
    seqs, props = parents.shape
    heads = decay.shape[1]
    pos_dev = keys.shape[1]
    width = query_w.shape[1]
    head_dim = width // heads
    scale = head_dim ** (-0.5)
    slots = part_in.shape[1]
    parity = lax.rem(tp, 2)
    left_over = seqs % n
    hp = heads * props

    barrier = pltpu.get_barrier_semaphore()
    for k in range(1, n):
        pl.semaphore_signal(barrier, inc=1, device_id={"kv": lax.rem(me + k, n)})
    for k in range(1, n_tp):
        pl.semaphore_signal(barrier, inc=1, device_id={"tp": lax.rem(tp + k, n_tp)})

    pairs = (
        (tokens_hbm, tokens),
        (gain_hbm, gain),
        (query_hbm, query_w),
        (key_hbm, key_w),
        (value_hbm, value_w),
        (bias_hbm, bias),
        (parents_hbm, parents),
        (decay_hbm, decay),
        (lengths_hbm, lengths),
    )
    small_loads = [
        pltpu.make_async_copy(src, dst, small_sem.at[i]) for i, (src, dst) in enumerate(pairs)
    ]
    for load in small_loads:
        load.start()
    gate_load = pltpu.make_async_copy(
        gate_hbm.at[:, pl.ds(pl.multiple_of(me * depth, depth), depth)], gate_w, load_sem.at[0]
    )
    gate_load.start()
    cache_loads = []
    for s in range(seqs):
        k_load = pltpu.make_async_copy(keys_hbm.at[s], keys.at[s], cache_sem.at[0, s])
        v_load = pltpu.make_async_copy(values_hbm.at[s], values.at[s], cache_sem.at[1, s])
        k_load.start()
        v_load.start()
        cache_loads.append((k_load, v_load))
    out_load = pltpu.make_async_copy(out_hbm, out_w, load_sem.at[1])
    out_load.start()

    def owner_of(s):
        if isinstance(s, int):
            place = s % n
            shift = parity * left_over if s // n == seqs // n else 0
        else:
            place = lax.rem(s, n)
            shift = jnp.where(lax.div(s, n) == seqs // n, parity * left_over, 0)
        return lax.rem(place + shift, n)

    def slot_seq(r):
        shift = parity * left_over if r == seqs // n else 0
        return r * n + lax.rem(me + 2 * n - shift, n)

    def for_slot(r, f):
        if (r + 1) * n <= seqs:
            f()
        else:
            pl.when(slot_seq(r) < seqs)(f)

    for load in small_loads:
        load.wait()
    xf = tokens[...].astype(F32)
    squares = jnp.sum(xf * xf, axis=1, keepdims=True)
    normed = (xf * gain[...]).astype(BF16)
    sel_rows = lax.broadcasted_iota(jnp.int32, (bias.shape[1], LANES), 0)
    sel_cols = lax.broadcasted_iota(jnp.int32, (bias.shape[1], LANES), 1)
    select = ((sel_rows == sel_cols + tp * heads) & (sel_cols < heads)).astype(F32)
    for i, w in enumerate((query_w, key_w)):
        part[:, :, i * width : (i + 1) * width] = dot(normed, w[...]).reshape(seqs, props, width)
    value_part = dot(normed, value_w[...])
    for s in range(seqs):
        part_v[s] = fold(value_part[s * props : (s + 1) * props]).astype(BF16)
    gate_load.wait()
    gates_w = lax.dot_general(
        select.astype(BF16), gate_w[...], (((0,), (0,)), ((), ())), preferred_element_type=F32
    )
    gate_part = dot_nt(normed, gates_w.astype(BF16))
    lane = lax.broadcasted_iota(jnp.int32, (rows, LANES), 1)
    gate_part = jnp.where(lane == LANES // 2, squares, gate_part)
    part[:, :, 2 * width :] = gate_part.reshape(seqs, props, LANES)
    pl.semaphore_wait(barrier, n + n_tp - 2)

    side = lax.rem(me, 2)
    partner = me + 1 - 2 * side
    n_far = n // 2
    shares = ((part, pair_in, part_in), (part_v, pair_in_v, part_in_v))

    def p_copy(s, which):
        src, dst, _ = shares[which]
        return pltpu.make_async_remote_copy(
            src_ref=src.at[s],
            dst_ref=dst.at[s],
            send_sem=p_send.at[which, s],
            recv_sem=p_recv.at[which, s],
            device_id={"kv": partner},
        )

    def a_copy(s, which):
        src, _, dst = shares[which]
        d = owner_of(s)
        k = jnp.maximum(lax.rem(lax.div(me, 2) - lax.div(d, 2) + n_far, n_far) - 1, 0)
        return pltpu.make_async_remote_copy(
            src_ref=src.at[s],
            dst_ref=dst.at[k, s // n],
            send_sem=a_send.at[which, s],
            recv_sem=a_recv.at[which, k, s // n],
            device_id={"kv": d},
        )

    def crosses(s):
        return lax.rem(owner_of(s), 2) != side

    def passes(s):
        d = owner_of(s)
        return (lax.rem(d, 2) == side) & (d != me)

    for s in range(seqs):
        for which in range(2):
            pl.when(crosses(s))(p_copy(s, which).start)

    par_pad[...] = jnp.zeros(par_pad.shape, jnp.int32)
    par_pad[0:seqs, 0:props] = parents[...]
    r_i = lax.broadcasted_iota(jnp.int32, (LANES, LANES), 0)
    c_i = lax.broadcasted_iota(jnp.int32, (LANES, LANES), 1)
    eye = (r_i == c_i).astype(F32)
    bias_row = dot(jnp.broadcast_to(bias[...], (8, bias.shape[1])), select, HIGH)[0:1]

    def ancestry(r):
        s = slot_seq(r)
        row = par_pad[pl.ds(s, 1), :]
        link = jnp.maximum((row == r_i).astype(F32), eye).astype(BF16)
        for _ in range(props.bit_length()):
            link = jnp.minimum(dot(link, link), 1.0).astype(BF16)
        anc[r] = dot_nt(eye.astype(BF16), link)[:props]

    for r in range(slots):
        for_slot(r, functools.partial(ancestry, r))

    def pass_on(s):
        for which in range(2):
            p_copy(s, which).wait_recv()
        part[s] = part[s] + pair_in[s]
        part_v[s] = (part_v[s].astype(F32) + pair_in_v[s].astype(F32)).astype(BF16)
        for which in range(2):
            a_copy(s, which).start()

    for s in range(seqs):
        pl.when(passes(s))(functools.partial(pass_on, s))

    lane_p = lax.broadcasted_iota(jnp.int32, (props, LANES), 1)
    bd_row = lax.broadcasted_iota(jnp.int32, (heads, props, width), 0)
    bd_col = lax.broadcasted_iota(jnp.int32, (heads, props, width), 2)
    diag = (lax.div(bd_col, head_dim) == bd_row).reshape(hp, width)

    def spread(q):
        wide = jnp.broadcast_to(q[None], (heads, props, width)).reshape(hp, width)
        return jnp.where(diag, wide, 0.0).astype(BF16)

    def gather_diag(m):
        return jnp.sum(jnp.where(diag, m, 0.0).reshape(heads, props, width), axis=0)

    def to_lanes(col, first):
        acc = jnp.zeros((props, LANES), F32)
        for h in range(heads):
            acc = jnp.where(lane_p == h + first, col[h * props : (h + 1) * props], acc)
        return acc

    def b_copy(r, k, buf, send, recv):
        s = slot_seq(r)
        return pltpu.make_async_remote_copy(
            src_ref=buf.at[s],
            dst_ref=buf.at[s],
            send_sem=send.at[r, k - 1],
            recv_sem=recv.at[s],
            device_id={"kv": lax.rem(me + k, n)},
        )

    pad_rows = LANES - props

    def project(r):
        s = slot_seq(r)
        for which, (src, near, far) in enumerate(shares):
            pltpu.make_async_remote_copy(
                src_ref=src.at[0],
                dst_ref=near.at[s],
                send_sem=p_send.at[which, 0],
                recv_sem=p_recv.at[which, s],
                device_id={"kv": partner},
            ).wait_recv()
            for k in range(1, n_far):
                pltpu.make_async_remote_copy(
                    src_ref=src.at[0],
                    dst_ref=far.at[k - 1, r],
                    send_sem=a_send.at[which, 0],
                    recv_sem=a_recv.at[which, k - 1, r],
                    device_id={"kv": lax.rem(me + 2 * k, n)},
                ).wait_recv()
        total = part[s] + pair_in[s]
        total_v = unfold(part_v[s]) + unfold(pair_in_v[s])
        for k in range(1, n_far):
            total = total + part_in[k - 1, r]
            total_v = total_v + unfold(part_in_v[k - 1, r])
        tail = total[:, 2 * width :]
        square = jnp.sum(jnp.where(lane_p == LANES // 2, tail, 0.0), axis=1, keepdims=True)
        inverse = lax.rsqrt(square / (depth * n) + 1e-06)
        q = inverse * total[:, :width]
        qbuf[s] = fold(q).astype(BF16)
        for k in range(1, n):
            b_copy(r, k, qbuf, b_send, b_recv).start()
        kvnew[r, 0, 0:props] = inverse * total[:, width : 2 * width]
        kvnew[r, 1, 0:props] = inverse * total_v
        kvnew[r, :, props:] = jnp.zeros((2, pad_rows, width), F32)
        x = inverse * tail + bias_row
        log_gate = jnp.minimum(x, 0.0) - jnp.log1p(jnp.exp(-jnp.abs(x)))
        padded = jnp.concatenate([log_gate, jnp.zeros((pad_rows, LANES), F32)], axis=0)
        path_s[r] = dot(anc[r], padded, HIGH)

    def tree(r):
        s = slot_seq(r)
        path = path_s[r]
        q = spread(unfold(qbuf[s]))
        head_of = lax.broadcasted_iota(jnp.int32, (heads, props, LANES), 0)
        lane_of = lax.broadcasted_iota(jnp.int32, (heads, props, LANES), 2)
        pick = (head_of == lane_of).reshape(hp, LANES)
        tiled = jnp.broadcast_to(path[None], (heads, props, LANES)).reshape(hp, LANES)
        own = jnp.sum(jnp.where(pick, tiled, 0.0), axis=1, keepdims=True)
        padded = jnp.concatenate([path, jnp.zeros((pad_rows, LANES), F32)], axis=0)
        other = dot_nt(pick.astype(F32), padded, HIGH)
        scores = dot_nt(q, kvnew[r, 0].astype(BF16)) * scale + own - other
        live = jnp.broadcast_to(anc[r][None], (heads, props, LANES)).reshape(hp, LANES) > 0.5
        scores = jnp.where(live, scores, LOW)
        top = jnp.max(scores, axis=1, keepdims=True)
        w = jnp.where(live, jnp.exp(scores - top), 0.0)
        total = jnp.sum(w, axis=1, keepdims=True)
        tmix[r] = gather_diag(dot(w.astype(BF16), kvnew[r, 1].astype(BF16)))
        tstat[r, 0] = to_lanes(top, 0)
        tstat[r, 1] = to_lanes(total, 0)

    position = lax.broadcasted_iota(jnp.int32, (hp, pos_dev), 1) + me * pos_dev

    def c_copy(s, which, src, dst):
        d = owner_of(s)
        k = jnp.maximum(lax.rem(me - d + n, n) - 1, 0)
        slot = s // n if isinstance(s, int) else lax.div(s, n)
        return d, pltpu.make_async_remote_copy(
            src_ref=src.at[s],
            dst_ref=dst.at[k, slot],
            send_sem=c_send.at[which, s],
            recv_sem=c_recv.at[which, k, slot],
            device_id={"kv": d},
        )

    def shard(s, carry):
        d = owner_of(s)

        @pl.when(d != me)
        def _():
            pltpu.make_async_remote_copy(
                src_ref=qbuf.at[s],
                dst_ref=qbuf.at[s],
                send_sem=b_send.at[0, 0],
                recv_sem=b_recv.at[s],
                device_id={"kv": d},
            ).wait_recv()

        pltpu.make_async_copy(keys_hbm.at[s], keys.at[s], cache_sem.at[0, s]).wait()
        pltpu.make_async_copy(values_hbm.at[s], values.at[s], cache_sem.at[1, s]).wait()
        q = spread(unfold(qbuf[s]))
        fade = decay[s]
        fade = jnp.concatenate(
            [jnp.broadcast_to(fade[h : h + 1], (props, pos_dev)) for h in range(heads)], axis=0
        )
        scores = dot_nt(q, keys[s]) * scale + fade
        live = position < lengths[s]
        scores = jnp.where(live, scores, LOW)
        top = jnp.max(scores, axis=1, keepdims=True)
        w = jnp.where(live, jnp.exp(scores - top), 0.0)
        total = jnp.sum(w, axis=1, keepdims=True)
        mix[s] = fold(gather_diag(dot(w.astype(BF16), values[s]))).astype(BF16)
        stat[s] = to_lanes(top, 0) + to_lanes(total, heads)
        for which, (src, dst) in enumerate(((mix, mix_in), (stat, stat_in))):
            _, copy = c_copy(s, which, src, dst)
            pl.when(d != me)(copy.start)
        return carry

    ex_r = lax.broadcasted_iota(jnp.int32, (LANES, width), 0)
    ex_c = lax.broadcasted_iota(jnp.int32, (LANES, width), 1)
    widen = (ex_r == lax.div(ex_c, head_dim)).astype(F32)

    def merge(r):
        s = slot_seq(r)
        for k in range(1, n):
            for which, (src, dst) in enumerate(((mix, mix_in), (stat, stat_in))):
                pltpu.make_async_remote_copy(
                    src_ref=src.at[0],
                    dst_ref=dst.at[k - 1, r],
                    send_sem=c_send.at[which, 0],
                    recv_sem=c_recv.at[which, k - 1, r],
                    device_id={"kv": lax.rem(me + k, n)},
                ).wait_recv()
        stats = jnp.concatenate([stat[s]] + [stat_in[k, r] for k in range(n - 1)], axis=0)
        totals = pltpu.roll(stats, LANES - heads, 1).reshape(n, props, LANES)
        tops = stats.reshape(n, props, LANES) + path_s[r][None]
        tops = jnp.where((lane_p < heads)[None], tops, LOW)
        ttop = jnp.where(lane_p < heads, tstat[r, 0], LOW)
        best = jnp.maximum(jnp.max(tops, axis=0), ttop)
        factors = jnp.exp(tops - best[None])
        tfactor = jnp.exp(ttop - best)
        denom = jnp.sum(factors * totals, axis=0) + tfactor * tstat[r, 1]
        packed = jnp.concatenate([factors.reshape(n * props, LANES), tfactor, denom], axis=0)
        wide = dot(packed, widen, HIGH)
        numer = wide[n * props : (n + 1) * props] * tmix[r] + wide[:props] * unfold(mix[s])
        for k in range(1, n):
            numer = numer + wide[k * props : (k + 1) * props] * unfold(mix_in[k - 1, r])
        att[s] = fold(numer / wide[(n + 1) * props :]).astype(BF16)
        for k in range(1, n):
            b_copy(r, k, att, d_send, d_recv).start()

    for r in range(slots):
        for_slot(r, functools.partial(project, r))
        if r > 0:
            for_slot(r - 1, functools.partial(merge, r - 1))
        for_slot(r, functools.partial(tree, r))
        lax.fori_loop(r * n, min((r + 1) * n, seqs), shard, 0)
    for_slot(slots - 1, functools.partial(merge, slots - 1))

    out_load.wait()
    block = rows // n_tp

    def e_copy(t):
        k = lax.rem(tp - t + n_tp, n_tp)
        return pltpu.make_async_remote_copy(
            src_ref=terms.at[t],
            dst_ref=terms_in.at[jnp.maximum(k - 1, 0)],
            send_sem=e_send.at[t],
            recv_sem=e_recv.at[jnp.maximum(k - 1, 0)],
            device_id={"tp": t},
        )

    arrived = 0
    for t in range(n_tp):
        first, last = t * block // props, ((t + 1) * block - 1) // props + 1
        for s in range(arrived, last):
            d = owner_of(s)

            @pl.when(d != me)
            def _(s=s, d=d):
                pltpu.make_async_remote_copy(
                    src_ref=att.at[s],
                    dst_ref=att.at[s],
                    send_sem=d_send.at[0, 0],
                    recv_sem=d_recv.at[s],
                    device_id={"kv": d},
                ).wait_recv()

        arrived = max(arrived, last)
        attended = jnp.concatenate([unfold(att[s]) for s in range(first, last)], axis=0)
        term = dot(attended.astype(BF16), out_w[...])
        begin = t * block - first * props
        terms[t] = term[begin : begin + block].astype(BF16)
        pl.when(tp != t)(e_copy(t).start)
    total = terms[tp].astype(F32)
    for k in range(1, n_tp):
        pltpu.make_async_remote_copy(
            src_ref=terms.at[0],
            dst_ref=terms_in.at[k - 1],
            send_sem=e_send.at[0],
            recv_sem=e_recv.at[k - 1],
            device_id={"tp": lax.rem(tp + k, n_tp)},
        ).wait_recv()
        total = total + terms_in[k - 1].astype(F32)
    out[...] = total.astype(BF16)

    for s in range(seqs):
        d = owner_of(s)
        for which in range(2):
            pl.when(crosses(s))(p_copy(s, which).wait_send)
            pl.when(passes(s))(a_copy(s, which).wait_send)
        for which, (src, dst) in enumerate(((mix, mix_in), (stat, stat_in))):
            _, copy = c_copy(s, which, src, dst)
            pl.when(d != me)(copy.wait_send)
    for r in range(slots):

        def drain(r=r):
            for k in range(1, n):
                b_copy(r, k, qbuf, b_send, b_recv).wait_send()
                b_copy(r, k, att, d_send, d_recv).wait_send()

        for_slot(r, drain)
    for t in range(n_tp):
        pl.when(tp != t)(e_copy(t).wait_send)


def solution(mesh):
    n, n_tp = mesh.shape["kv"], mesh.shape["tp"]

    def body(
        tokens,
        norm_gain,
        query_weight,
        key_weight,
        value_weight,
        gate_weight,
        gate_bias,
        out_weight,
        cache_keys,
        cache_values,
        cache_decay,
        lengths,
        parents,
    ):
        rows, depth = tokens.shape
        seqs, props = parents.shape
        heads = cache_decay.shape[1]
        pos_dev = cache_keys.shape[1]
        width = query_weight.shape[1]
        cols = out_weight.shape[1]
        slots = -(-seqs // n)
        block = rows // n_tp
        all_w = 2 * width + LANES
        folded = (2 * props, width // 2)
        vmem = pl.BlockSpec(memory_space=pltpu.VMEM)
        hbm = pl.BlockSpec(memory_space=pltpu.HBM)
        dma = pltpu.SemaphoreType.DMA
        return pl.pallas_call(
            functools.partial(kernel, n, n_tp),
            out_shape=jax.ShapeDtypeStruct((block, cols), BF16),
            in_specs=[hbm] * 13,
            out_specs=vmem,
            scratch_shapes=[
                pltpu.VMEM(tokens.shape, BF16),
                pltpu.VMEM((1, depth), F32),
                pltpu.VMEM(query_weight.shape, BF16),
                pltpu.VMEM(key_weight.shape, BF16),
                pltpu.VMEM(value_weight.shape, BF16),
                pltpu.VMEM((1, gate_bias.shape[0]), F32),
                pltpu.VMEM(cache_decay.shape, F32),
                pltpu.SMEM(lengths.shape, jnp.int32),
                pltpu.VMEM(parents.shape, jnp.int32),
                dma((9,)),
                pltpu.VMEM((seqs, props, all_w), F32),
                pltpu.VMEM((seqs,) + folded, BF16),
                pltpu.VMEM((seqs, props, all_w), F32),
                pltpu.VMEM((seqs,) + folded, BF16),
                pltpu.VMEM((n // 2 - 1, slots, props, all_w), F32),
                pltpu.VMEM((n // 2 - 1, slots) + folded, BF16),
                pltpu.VMEM((gate_weight.shape[1], depth), BF16),
                pltpu.VMEM(out_weight.shape, BF16),
                pltpu.VMEM(cache_keys.shape, BF16),
                pltpu.VMEM(cache_values.shape, BF16),
                pltpu.VMEM((seqs,) + folded, BF16),
                pltpu.VMEM((seqs,) + folded, BF16),
                pltpu.VMEM((seqs, props, LANES), F32),
                pltpu.VMEM((n - 1, slots) + folded, BF16),
                pltpu.VMEM((n - 1, slots, props, LANES), F32),
                pltpu.VMEM((seqs,) + folded, BF16),
                pltpu.VMEM((slots, props, LANES), F32),
                pltpu.VMEM((slots, props, LANES), F32),
                pltpu.VMEM((slots, props, width), F32),
                pltpu.VMEM((slots, 2, props, LANES), F32),
                pltpu.VMEM((slots, 2, LANES, width), F32),
                pltpu.VMEM((n_tp, block, cols), BF16),
                pltpu.VMEM((n_tp - 1, block, cols), BF16),
                pltpu.VMEM((-(-seqs // 8) * 8, LANES), jnp.int32),
                dma((2,)),
                dma((2, seqs)),
                dma((2, seqs)),
                dma((2, seqs)),
                dma((2, seqs)),
                dma((2, n // 2 - 1, slots)),
                dma((slots, n - 1)),
                dma((seqs,)),
                dma((2, seqs)),
                dma((2, n - 1, slots)),
                dma((slots, n - 1)),
                dma((seqs,)),
                dma((n_tp,)),
                dma((n_tp - 1,)),
            ],
            compiler_params=pltpu.CompilerParams(
                collective_id=0, has_side_effects=True, vmem_limit_bytes=67_043_328
            ),
        )(
            tokens,
            norm_gain.reshape(1, depth),
            query_weight,
            key_weight,
            value_weight,
            gate_weight.T,
            gate_bias.reshape(1, gate_bias.shape[0]),
            out_weight,
            cache_keys,
            cache_values,
            cache_decay,
            lengths,
            parents,
        )

    in_specs = (
        P(None, "kv"),
        P("kv"),
        P("kv", "tp"),
        P("kv", "tp"),
        P("kv", "tp"),
        P(),
        P(),
        P("tp", "kv"),
        P(None, "kv", "tp"),
        P(None, "kv", "tp"),
        P(None, "tp", "kv"),
        P(),
        P(),
    )
    out_specs = P("tp", "kv")
    return jax.shard_map(body, mesh=mesh, in_specs=in_specs, out_specs=out_specs, check_vma=False)
```

```python
import functools
import math

import jax
import jax.numpy as jnp
from jax import lax
from jax.experimental import pallas as pl
from jax.experimental.pallas import tpu as pltpu
from jax.sharding import PartitionSpec as P

F32 = jnp.float32
BF16 = jnp.bfloat16
LANES = 128
LOW = -1e30
NT = (((1,), (1,)), ((), ()))
HIGH = lax.Precision.HIGHEST


def dot(a, b, precision=None):
    return jnp.dot(a, b, preferred_element_type=F32, precision=precision)


def dot_nt(a, b, precision=None):
    return lax.dot_general(a, b, NT, preferred_element_type=F32, precision=precision)


def fold(x):
    half = x.shape[1] // 2
    return jnp.concatenate([x[:, :half], x[:, half:]], axis=0)


def unfold(x):
    rows = x.shape[0] // 2
    x = x.astype(F32)
    return jnp.concatenate([x[:rows], x[rows:]], axis=1)


def by_sequence(
    n,
    n_tp,
    tokens_hbm,
    gain_hbm,
    query_hbm,
    key_hbm,
    value_hbm,
    gate_hbm,
    bias_hbm,
    out_hbm,
    keys_hbm,
    values_hbm,
    decay_hbm,
    lengths_hbm,
    parents_hbm,
    out,
    tokens,
    gain,
    query_w,
    key_w,
    value_w,
    bias,
    decay,
    lengths,
    parents,
    small_sem,
    part,
    part_v,
    pair_in,
    pair_in_v,
    part_in,
    part_in_v,
    gate_w,
    out_w,
    keys,
    values,
    qbuf,
    mix,
    stat,
    mix_in,
    stat_in,
    att,
    anc,
    path_s,
    tmix,
    tstat,
    kvnew,
    terms,
    terms_in,
    par_pad,
    load_sem,
    cache_sem,
    p_send,
    p_recv,
    a_send,
    a_recv,
    b_send,
    b_recv,
    c_send,
    c_recv,
    d_send,
    d_recv,
    e_send,
    e_recv,
):
    me = lax.axis_index("kv")
    tp = lax.axis_index("tp")
    rows, depth = tokens.shape
    seqs, props = parents.shape
    heads = decay.shape[1]
    pos_dev = keys.shape[1]
    width = query_w.shape[1]
    head_dim = width // heads
    scale = head_dim ** (-0.5)
    slots = part_in.shape[1]
    parity = lax.rem(tp, 2)
    left_over = seqs % n
    hp = heads * props

    barrier = pltpu.get_barrier_semaphore()
    for k in range(1, n):
        pl.semaphore_signal(barrier, inc=1, device_id={"kv": lax.rem(me + k, n)})
    for k in range(1, n_tp):
        pl.semaphore_signal(barrier, inc=1, device_id={"tp": lax.rem(tp + k, n_tp)})

    pairs = (
        (tokens_hbm, tokens),
        (gain_hbm, gain),
        (query_hbm, query_w),
        (key_hbm, key_w),
        (value_hbm, value_w),
        (bias_hbm, bias),
        (parents_hbm, parents),
        (decay_hbm, decay),
        (lengths_hbm, lengths),
    )
    small_loads = [
        pltpu.make_async_copy(src, dst, small_sem.at[i]) for i, (src, dst) in enumerate(pairs)
    ]
    for load in small_loads:
        load.start()
    gate_load = pltpu.make_async_copy(
        gate_hbm.at[:, pl.ds(pl.multiple_of(me * depth, depth), depth)], gate_w, load_sem.at[0]
    )
    gate_load.start()
    cache_loads = []
    for s in range(seqs):
        k_load = pltpu.make_async_copy(keys_hbm.at[s], keys.at[s], cache_sem.at[0, s])
        v_load = pltpu.make_async_copy(values_hbm.at[s], values.at[s], cache_sem.at[1, s])
        k_load.start()
        v_load.start()
        cache_loads.append((k_load, v_load))
    out_load = pltpu.make_async_copy(out_hbm, out_w, load_sem.at[1])
    out_load.start()

    def owner_of(s):
        if isinstance(s, int):
            place = s % n
            shift = parity * left_over if s // n == seqs // n else 0
        else:
            place = lax.rem(s, n)
            shift = jnp.where(lax.div(s, n) == seqs // n, parity * left_over, 0)
        return lax.rem(place + shift, n)

    def slot_seq(r):
        shift = parity * left_over if r == seqs // n else 0
        return r * n + lax.rem(me + 2 * n - shift, n)

    def for_slot(r, f):
        if (r + 1) * n <= seqs:
            f()
        else:
            pl.when(slot_seq(r) < seqs)(f)

    for load in small_loads:
        load.wait()
    xf = tokens[...].astype(F32)
    squares = jnp.sum(xf * xf, axis=1, keepdims=True)
    normed = (xf * gain[...]).astype(BF16)
    sel_rows = lax.broadcasted_iota(jnp.int32, (bias.shape[1], LANES), 0)
    sel_cols = lax.broadcasted_iota(jnp.int32, (bias.shape[1], LANES), 1)
    select = ((sel_rows == sel_cols + tp * heads) & (sel_cols < heads)).astype(F32)
    for i, w in enumerate((query_w, key_w)):
        part[:, :, i * width : (i + 1) * width] = dot(normed, w[...]).reshape(seqs, props, width)
    value_part = dot(normed, value_w[...])
    for s in range(seqs):
        part_v[s] = fold(value_part[s * props : (s + 1) * props]).astype(BF16)
    gate_load.wait()
    gates_w = lax.dot_general(
        select.astype(BF16), gate_w[...], (((0,), (0,)), ((), ())), preferred_element_type=F32
    )
    gate_part = dot_nt(normed, gates_w.astype(BF16))
    lane = lax.broadcasted_iota(jnp.int32, (rows, LANES), 1)
    gate_part = jnp.where(lane == LANES // 2, squares, gate_part)
    part[:, :, 2 * width :] = gate_part.reshape(seqs, props, LANES)
    pl.semaphore_wait(barrier, n + n_tp - 2)

    side = lax.rem(me, 2)
    partner = me + 1 - 2 * side
    n_far = n // 2
    shares = ((part, pair_in, part_in), (part_v, pair_in_v, part_in_v))

    def p_copy(s, which):
        src, dst, _ = shares[which]
        return pltpu.make_async_remote_copy(
            src_ref=src.at[s],
            dst_ref=dst.at[s],
            send_sem=p_send.at[which, s],
            recv_sem=p_recv.at[which, s],
            device_id={"kv": partner},
        )

    def a_copy(s, which):
        src, _, dst = shares[which]
        d = owner_of(s)
        k = jnp.maximum(lax.rem(lax.div(me, 2) - lax.div(d, 2) + n_far, n_far) - 1, 0)
        return pltpu.make_async_remote_copy(
            src_ref=src.at[s],
            dst_ref=dst.at[k, s // n],
            send_sem=a_send.at[which, s],
            recv_sem=a_recv.at[which, k, s // n],
            device_id={"kv": d},
        )

    def crosses(s):
        return lax.rem(owner_of(s), 2) != side

    def passes(s):
        d = owner_of(s)
        return (lax.rem(d, 2) == side) & (d != me)

    for s in range(seqs):
        for which in range(2):
            pl.when(crosses(s))(p_copy(s, which).start)

    par_pad[...] = jnp.zeros(par_pad.shape, jnp.int32)
    par_pad[0:seqs, 0:props] = parents[...]
    r_i = lax.broadcasted_iota(jnp.int32, (LANES, LANES), 0)
    c_i = lax.broadcasted_iota(jnp.int32, (LANES, LANES), 1)
    eye = (r_i == c_i).astype(F32)
    bias_row = dot(jnp.broadcast_to(bias[...], (8, bias.shape[1])), select, HIGH)[0:1]

    def ancestry(r):
        s = slot_seq(r)
        row = par_pad[pl.ds(s, 1), :]
        link = jnp.maximum((row == r_i).astype(F32), eye).astype(BF16)
        for _ in range(props.bit_length()):
            link = jnp.minimum(dot(link, link), 1.0).astype(BF16)
        anc[r] = dot_nt(eye.astype(BF16), link)[:props]

    for r in range(slots):
        for_slot(r, functools.partial(ancestry, r))

    def pass_on(s):
        for which in range(2):
            p_copy(s, which).wait_recv()
        part[s] = part[s] + pair_in[s]
        part_v[s] = (part_v[s].astype(F32) + pair_in_v[s].astype(F32)).astype(BF16)
        for which in range(2):
            a_copy(s, which).start()

    for s in range(seqs):
        pl.when(passes(s))(functools.partial(pass_on, s))

    lane_p = lax.broadcasted_iota(jnp.int32, (props, LANES), 1)
    bd_row = lax.broadcasted_iota(jnp.int32, (heads, props, width), 0)
    bd_col = lax.broadcasted_iota(jnp.int32, (heads, props, width), 2)
    diag = (lax.div(bd_col, head_dim) == bd_row).reshape(hp, width)

    def spread(q):
        wide = jnp.broadcast_to(q[None], (heads, props, width)).reshape(hp, width)
        return jnp.where(diag, wide, 0.0).astype(BF16)

    def gather_diag(m):
        return jnp.sum(jnp.where(diag, m, 0.0).reshape(heads, props, width), axis=0)

    def to_lanes(col, first):
        acc = jnp.zeros((props, LANES), F32)
        for h in range(heads):
            acc = jnp.where(lane_p == h + first, col[h * props : (h + 1) * props], acc)
        return acc

    def b_copy(r, k, buf, send, recv):
        s = slot_seq(r)
        return pltpu.make_async_remote_copy(
            src_ref=buf.at[s],
            dst_ref=buf.at[s],
            send_sem=send.at[r, k - 1],
            recv_sem=recv.at[s],
            device_id={"kv": lax.rem(me + k, n)},
        )

    pad_rows = LANES - props

    def project(r):
        s = slot_seq(r)
        for which, (src, near, far) in enumerate(shares):
            pltpu.make_async_remote_copy(
                src_ref=src.at[0],
                dst_ref=near.at[s],
                send_sem=p_send.at[which, 0],
                recv_sem=p_recv.at[which, s],
                device_id={"kv": partner},
            ).wait_recv()
            for k in range(1, n_far):
                pltpu.make_async_remote_copy(
                    src_ref=src.at[0],
                    dst_ref=far.at[k - 1, r],
                    send_sem=a_send.at[which, 0],
                    recv_sem=a_recv.at[which, k - 1, r],
                    device_id={"kv": lax.rem(me + 2 * k, n)},
                ).wait_recv()
        total = part[s] + pair_in[s]
        total_v = unfold(part_v[s]) + unfold(pair_in_v[s])
        for k in range(1, n_far):
            total = total + part_in[k - 1, r]
            total_v = total_v + unfold(part_in_v[k - 1, r])
        tail = total[:, 2 * width :]
        square = jnp.sum(jnp.where(lane_p == LANES // 2, tail, 0.0), axis=1, keepdims=True)
        inverse = lax.rsqrt(square / (depth * n) + 1e-06)
        q = inverse * total[:, :width]
        qbuf[s] = fold(q).astype(BF16)
        for k in range(1, n):
            b_copy(r, k, qbuf, b_send, b_recv).start()
        kvnew[r, 0, 0:props] = inverse * total[:, width : 2 * width]
        kvnew[r, 1, 0:props] = inverse * total_v
        kvnew[r, :, props:] = jnp.zeros((2, pad_rows, width), F32)
        x = inverse * tail + bias_row
        log_gate = jnp.minimum(x, 0.0) - jnp.log1p(jnp.exp(-jnp.abs(x)))
        padded = jnp.concatenate([log_gate, jnp.zeros((pad_rows, LANES), F32)], axis=0)
        path_s[r] = dot(anc[r], padded, HIGH)

    def tree(r):
        s = slot_seq(r)
        path = path_s[r]
        q = spread(unfold(qbuf[s]))
        head_of = lax.broadcasted_iota(jnp.int32, (heads, props, LANES), 0)
        lane_of = lax.broadcasted_iota(jnp.int32, (heads, props, LANES), 2)
        pick = (head_of == lane_of).reshape(hp, LANES)
        tiled = jnp.broadcast_to(path[None], (heads, props, LANES)).reshape(hp, LANES)
        own = jnp.sum(jnp.where(pick, tiled, 0.0), axis=1, keepdims=True)
        padded = jnp.concatenate([path, jnp.zeros((pad_rows, LANES), F32)], axis=0)
        other = dot_nt(pick.astype(F32), padded, HIGH)
        scores = dot_nt(q, kvnew[r, 0].astype(BF16)) * scale + own - other
        live = jnp.broadcast_to(anc[r][None], (heads, props, LANES)).reshape(hp, LANES) > 0.5
        scores = jnp.where(live, scores, LOW)
        top = jnp.max(scores, axis=1, keepdims=True)
        w = jnp.where(live, jnp.exp(scores - top), 0.0)
        total = jnp.sum(w, axis=1, keepdims=True)
        tmix[r] = gather_diag(dot(w.astype(BF16), kvnew[r, 1].astype(BF16)))
        tstat[r, 0] = to_lanes(top, 0)
        tstat[r, 1] = to_lanes(total, 0)

    position = lax.broadcasted_iota(jnp.int32, (hp, pos_dev), 1) + me * pos_dev

    def c_copy(s, which, src, dst):
        d = owner_of(s)
        k = jnp.maximum(lax.rem(me - d + n, n) - 1, 0)
        slot = s // n if isinstance(s, int) else lax.div(s, n)
        return d, pltpu.make_async_remote_copy(
            src_ref=src.at[s],
            dst_ref=dst.at[k, slot],
            send_sem=c_send.at[which, s],
            recv_sem=c_recv.at[which, k, slot],
            device_id={"kv": d},
        )

    def shard(s, carry):
        d = owner_of(s)

        @pl.when(d != me)
        def _():
            pltpu.make_async_remote_copy(
                src_ref=qbuf.at[s],
                dst_ref=qbuf.at[s],
                send_sem=b_send.at[0, 0],
                recv_sem=b_recv.at[s],
                device_id={"kv": d},
            ).wait_recv()

        pltpu.make_async_copy(keys_hbm.at[s], keys.at[s], cache_sem.at[0, s]).wait()
        pltpu.make_async_copy(values_hbm.at[s], values.at[s], cache_sem.at[1, s]).wait()
        q = spread(unfold(qbuf[s]))
        fade = decay[s]
        fade = jnp.concatenate(
            [jnp.broadcast_to(fade[h : h + 1], (props, pos_dev)) for h in range(heads)], axis=0
        )
        scores = dot_nt(q, keys[s]) * scale + fade
        live = position < lengths[s]
        scores = jnp.where(live, scores, LOW)
        top = jnp.max(scores, axis=1, keepdims=True)
        w = jnp.where(live, jnp.exp(scores - top), 0.0)
        total = jnp.sum(w, axis=1, keepdims=True)
        mix[s] = fold(gather_diag(dot(w.astype(BF16), values[s]))).astype(BF16)
        stat[s] = to_lanes(top, 0) + to_lanes(total, heads)
        for which, (src, dst) in enumerate(((mix, mix_in), (stat, stat_in))):
            _, copy = c_copy(s, which, src, dst)
            pl.when(d != me)(copy.start)
        return carry

    ex_r = lax.broadcasted_iota(jnp.int32, (LANES, width), 0)
    ex_c = lax.broadcasted_iota(jnp.int32, (LANES, width), 1)
    widen = (ex_r == lax.div(ex_c, head_dim)).astype(F32)

    def merge(r):
        s = slot_seq(r)
        for k in range(1, n):
            for which, (src, dst) in enumerate(((mix, mix_in), (stat, stat_in))):
                pltpu.make_async_remote_copy(
                    src_ref=src.at[0],
                    dst_ref=dst.at[k - 1, r],
                    send_sem=c_send.at[which, 0],
                    recv_sem=c_recv.at[which, k - 1, r],
                    device_id={"kv": lax.rem(me + k, n)},
                ).wait_recv()
        stats = jnp.concatenate([stat[s]] + [stat_in[k, r] for k in range(n - 1)], axis=0)
        totals = pltpu.roll(stats, LANES - heads, 1).reshape(n, props, LANES)
        tops = stats.reshape(n, props, LANES) + path_s[r][None]
        tops = jnp.where((lane_p < heads)[None], tops, LOW)
        ttop = jnp.where(lane_p < heads, tstat[r, 0], LOW)
        best = jnp.maximum(jnp.max(tops, axis=0), ttop)
        factors = jnp.exp(tops - best[None])
        tfactor = jnp.exp(ttop - best)
        denom = jnp.sum(factors * totals, axis=0) + tfactor * tstat[r, 1]
        packed = jnp.concatenate([factors.reshape(n * props, LANES), tfactor, denom], axis=0)
        wide = dot(packed, widen, HIGH)
        numer = wide[n * props : (n + 1) * props] * tmix[r] + wide[:props] * unfold(mix[s])
        for k in range(1, n):
            numer = numer + wide[k * props : (k + 1) * props] * unfold(mix_in[k - 1, r])
        att[s] = fold(numer / wide[(n + 1) * props :]).astype(BF16)
        for k in range(1, n):
            b_copy(r, k, att, d_send, d_recv).start()

    for r in range(slots):
        for_slot(r, functools.partial(project, r))
        if r > 0:
            for_slot(r - 1, functools.partial(merge, r - 1))
        for_slot(r, functools.partial(tree, r))
        lax.fori_loop(r * n, min((r + 1) * n, seqs), shard, 0)
    for_slot(slots - 1, functools.partial(merge, slots - 1))

    out_load.wait()
    block = rows // n_tp

    def e_copy(t):
        k = lax.rem(tp - t + n_tp, n_tp)
        return pltpu.make_async_remote_copy(
            src_ref=terms.at[t],
            dst_ref=terms_in.at[jnp.maximum(k - 1, 0)],
            send_sem=e_send.at[t],
            recv_sem=e_recv.at[jnp.maximum(k - 1, 0)],
            device_id={"tp": t},
        )

    arrived = 0
    for t in range(n_tp):
        first, last = t * block // props, ((t + 1) * block - 1) // props + 1
        for s in range(arrived, last):
            d = owner_of(s)

            @pl.when(d != me)
            def _(s=s, d=d):
                pltpu.make_async_remote_copy(
                    src_ref=att.at[s],
                    dst_ref=att.at[s],
                    send_sem=d_send.at[0, 0],
                    recv_sem=d_recv.at[s],
                    device_id={"kv": d},
                ).wait_recv()

        arrived = max(arrived, last)
        attended = jnp.concatenate([unfold(att[s]) for s in range(first, last)], axis=0)
        term = dot(attended.astype(BF16), out_w[...])
        begin = t * block - first * props
        terms[t] = term[begin : begin + block].astype(BF16)
        pl.when(tp != t)(e_copy(t).start)
    total = terms[tp].astype(F32)
    for k in range(1, n_tp):
        pltpu.make_async_remote_copy(
            src_ref=terms.at[0],
            dst_ref=terms_in.at[k - 1],
            send_sem=e_send.at[0],
            recv_sem=e_recv.at[k - 1],
            device_id={"tp": lax.rem(tp + k, n_tp)},
        ).wait_recv()
        total = total + terms_in[k - 1].astype(F32)
    out[...] = total.astype(BF16)

    for s in range(seqs):
        d = owner_of(s)
        for which in range(2):
            pl.when(crosses(s))(p_copy(s, which).wait_send)
            pl.when(passes(s))(a_copy(s, which).wait_send)
        for which, (src, dst) in enumerate(((mix, mix_in), (stat, stat_in))):
            _, copy = c_copy(s, which, src, dst)
            pl.when(d != me)(copy.wait_send)
    for r in range(slots):

        def drain(r=r):
            for k in range(1, n):
                b_copy(r, k, qbuf, b_send, b_recv).wait_send()
                b_copy(r, k, att, d_send, d_recv).wait_send()

        for_slot(r, drain)
    for t in range(n_tp):
        pl.when(tp != t)(e_copy(t).wait_send)


def split3(x):
    high = x.astype(BF16)
    rest = x - high.astype(F32)
    mid = rest.astype(BF16)
    low = (rest - mid.astype(F32)).astype(BF16)
    return high, mid, low


def tile_rows(rows, total):
    return jnp.concatenate([rows, jnp.zeros((total - rows.shape[0], rows.shape[1]), rows.dtype)], axis=0)


def by_heads(
    n,
    n_tp,
    wave,
    tokens_hbm,
    gain_hbm,
    query_hbm,
    key_hbm,
    value_hbm,
    gate_hbm,
    bias_hbm,
    out_hbm,
    keys_hbm,
    values_hbm,
    decay_hbm,
    lengths_hbm,
    parents_hbm,
    out,
    tokens,
    gain,
    query_w,
    key_w,
    value_w,
    gate_w,
    bias,
    decay,
    lengths,
    parents,
    out_w,
    keys,
    values,
    feats,
    q_out,
    q_in,
    q_own,
    q_far,
    kv_out,
    kv_in,
    kv_own,
    kv_pass,
    kv_far,
    qbuf,
    mix,
    mix_in,
    stat,
    stat_in,
    att,
    terms,
    terms_in,
    par_pad,
    link_s,
    anc_s,
    path_s,
    inv_s,
    tmix,
    tstat,
    widen,
    load_sem,
    cache_sem,
    qx_send,
    qx_recv,
    kx_send,
    kx_recv,
    qz_send,
    qz_recv,
    kz_send,
    kz_recv,
    b_send,
    b_recv,
    c_send,
    c_recv,
    d_send,
    d_recv,
    e_send,
    e_recv,
):
    me = lax.axis_index("kv")
    tp = lax.axis_index("tp")
    side = lax.rem(me, 2)
    far = lax.div(me, 2)
    n_far = n // 2
    rows, depth = tokens.shape
    seqs, props = parents.shape
    heads = decay.shape[1]
    pos_dev = keys.shape[1]
    width = query_w.shape[1]
    head_dim = width // heads
    scale = head_dim ** (-0.5)
    exact_scale = math.frexp(scale)[0] == 0.5
    own_heads = heads // n_far
    cols = width // n_far
    half_seqs = seqs // 2
    half = rows // 2
    waves = half_seqs // wave
    wrows = wave * props
    sources = n - 1

    barrier = pltpu.get_barrier_semaphore()
    for k in range(1, n):
        pl.semaphore_signal(barrier, inc=1, device_id={"kv": lax.rem(me + k, n)})
    for k in range(1, n_tp):
        pl.semaphore_signal(barrier, inc=1, device_id={"tp": lax.rem(tp + k, n_tp)})

    pairs = (
        (tokens_hbm, tokens),
        (gain_hbm, gain),
        (gate_hbm.at[:, pl.ds(pl.multiple_of(me * depth, depth), depth)], gate_w),
        (query_hbm, query_w),
        (key_hbm, key_w),
        (value_hbm, value_w),
        (bias_hbm, bias),
        (parents_hbm, parents),
        (lengths_hbm, lengths),
        (decay_hbm, decay),
        (out_hbm, out_w),
    )
    loads = [pltpu.make_async_copy(src, dst, load_sem.at[i]) for i, (src, dst) in enumerate(pairs)]
    for load in loads:
        load.start()
    for s in range(seqs):
        pltpu.make_async_copy(keys_hbm.at[s], keys.at[s], cache_sem.at[0, s]).start()
        pltpu.make_async_copy(values_hbm.at[s], values.at[s], cache_sem.at[1, s]).start()
    load_of = dict(
        zip(("tokens", "gain", "gate", "q", "k", "v", "bias", "parents", "lengths", "decay", "out"), loads)
    )

    def iota(shape, dim):
        return lax.broadcasted_iota(jnp.int32, shape, dim)

    def far_id(d):
        return lax.rem(far + d, n_far)

    def near_id(z, x):
        return {"kv": z * 2 + x}

    own_half = pl.multiple_of(side * half, half)
    peer_half = pl.multiple_of((1 - side) * half, half)

    load_of["tokens"].wait()
    load_of["gain"].wait()
    xf = tokens[...].astype(F32)
    feats[:, :depth] = (xf * gain[...]).astype(BF16)
    square = xf * xf
    high = square.astype(BF16)
    feats[:, depth : 2 * depth] = high
    feats[:, 2 * depth :] = (square - high.astype(F32)).astype(BF16)

    load_of["gate"].wait()
    t_rows = n_far * 8
    p_row = iota((t_rows, gate_w.shape[0]), 0)
    p_col = iota((t_rows, gate_w.shape[0]), 1)
    p_in = lax.rem(p_row, 8)
    wanted = (p_in < own_heads) & (p_col == tp * heads + lax.div(p_row, 8) * own_heads + p_in)
    gates = dot(wanted.astype(BF16), gate_w[...]).astype(BF16)
    ones = (lax.rem(iota((t_rows, depth), 0), 8) == own_heads).astype(BF16)
    tails = jnp.concatenate([gates, ones, ones], axis=1)

    def project_q(base, dst):
        full = dot(feats[pl.ds(base, half), :depth], query_w[...])
        for i in range(waves):
            piece = full[i * wrows : (i + 1) * wrows]
            tail = dot_nt(tails, feats[pl.ds(base + i * wrows, wrows), :])
            tail = jnp.concatenate([tail, jnp.zeros((t_rows, LANES - wrows), F32)], axis=1)
            for f in range(n_far):
                dst[i, f, :wrows] = piece[:, f * cols : (f + 1) * cols]
                dst[i, f, wrows:] = tail[f * 8 : (f + 1) * 8]

    def project_kv(base, dst):
        for which, w in enumerate((key_w, value_w)):
            full = dot(feats[pl.ds(base, half), :depth], w[...])
            for i in range(waves):
                piece = full[i * wrows : (i + 1) * wrows].astype(dst.dtype)
                for f in range(n_far):
                    dst[i, f, which * wrows : (which + 1) * wrows] = piece[:, f * cols : (f + 1) * cols]

    def x_copy(i, src, dst, send, recv):
        return pltpu.make_async_remote_copy(
            src_ref=src.at[i],
            dst_ref=dst.at[i],
            send_sem=send.at[i],
            recv_sem=recv.at[i],
            device_id=near_id(far, 1 - side),
        )

    def z_copy(i, d, src, dst, send, recv):
        return pltpu.make_async_remote_copy(
            src_ref=src.at[i, far_id(d)],
            dst_ref=dst.at[d - 1, i],
            send_sem=send.at[d - 1, i],
            recv_sem=recv.at[d - 1, i],
            device_id=near_id(far_id(d), side),
        )

    load_of["q"].wait()
    project_q(peer_half, q_out)
    pl.semaphore_wait(barrier, n + n_tp - 2)
    for i in range(waves):
        x_copy(i, q_out, q_in, qx_send, qx_recv).start()
    load_of["k"].wait()
    load_of["v"].wait()
    project_kv(peer_half, kv_out)
    for i in range(waves):
        x_copy(i, kv_out, kv_in, kx_send, kx_recv).start()
    project_q(own_half, q_own)
    project_kv(own_half, kv_own)

    load_of["bias"].wait()
    load_of["parents"].wait()
    load_of["lengths"].wait()
    load_of["decay"].wait()
    par_pad[...] = jnp.zeros(par_pad.shape, jnp.int32)
    par_pad[0:seqs, 0:props] = parents[...]
    r_i = iota((LANES, LANES), 0)
    c_i = iota((LANES, LANES), 1)
    lane1 = iota((1, LANES), 1)
    eye = r_i == c_i
    for i in range(waves):
        row = jnp.full((1, LANES), -1, jnp.int32)
        for j in range(wave):
            of = par_pad[pl.ds(side * half_seqs + i * wave + j, 1), :]
            if j:
                of = pltpu.roll(jnp.broadcast_to(of, (8, LANES)), j * props, 1)[0:1]
            inside = (lane1 >= j * props) & (lane1 < (j + 1) * props)
            row = jnp.where(inside, of + j * props, row)
        link = ((row == r_i) | eye).astype(F32).astype(BF16)
        for _ in range(props.bit_length()):
            link = jnp.minimum(dot(link, link), 1.0).astype(BF16)
        link_s[i] = link
        anc_s[i] = dot_nt(eye.astype(F32).astype(BF16), link)
    w_row = lax.rem(iota(widen.shape, 0), LANES)
    w_col = iota(widen.shape, 1)
    w_src = lax.div(w_col, cols) * 8 + lax.div(lax.rem(w_col, cols), head_dim)
    widen[...] = (w_row == w_src).astype(F32).astype(BF16)
    b_shape = (8, bias.shape[1])
    b_row, b_col = iota(b_shape, 0), iota(b_shape, 1)
    mine = (b_row < own_heads) & (b_col == tp * heads + far * own_heads + b_row)
    bias_col = jnp.sum(jnp.where(mine, jnp.broadcast_to(bias[...], b_shape), 0.0), axis=1, keepdims=True)

    for i in range(waves):
        x_copy(i, q_out, q_in, qx_send, qx_recv).wait_recv()
        q_own[i] = q_own[i] + q_in[i]
        for d in range(1, n_far):
            z_copy(i, d, q_own, q_far, qz_send, qz_recv).start()

    targets = [(d, 0) for d in range(1, n_far)] + [(d, 1) for d in range(n_far)]

    def target_id(d, cross):
        return near_id(far_id(d), side if not cross else 1 - side)

    def spread_copy(i, t, buf, send, recv):
        d, cross = targets[t]
        block = side * waves + i
        return pltpu.make_async_remote_copy(
            src_ref=buf.at[block, far],
            dst_ref=buf.at[block, far],
            send_sem=send.at[t, i],
            recv_sem=recv.at[block, far],
            device_id=target_id(d, cross),
        )

    def spread_wait(i, t, buf, send, recv):
        d, cross = targets[t]
        block = (1 - side if cross else side) * waves + i
        pltpu.make_async_remote_copy(
            src_ref=buf.at[block, far_id(d)],
            dst_ref=buf.at[block, far_id(d)],
            send_sem=send.at[t, i],
            recv_sem=recv.at[block, far_id(d)],
            device_id=target_id(d, cross),
        ).wait_recv()

    lane8 = iota((8, LANES), 1)
    row8 = iota((8, LANES), 0)

    def owner_q(i):
        total = q_own[i, far]
        for d in range(1, n_far):
            z_copy(i, d, q_own, q_far, qz_send, qz_recv).wait_recv()
            total = total + q_far[d - 1, i]
        tail = total[wrows:]
        inverse = lax.rsqrt(tail / (depth * n) + 1e-06)
        column = tile_rows(inverse, LANES).T[:wrows, own_heads : own_heads + 1]
        inv_s[i] = jnp.broadcast_to(column, (wrows, cols))
        qbuf[side * waves + i, far] = (inv_s[i] * total[:wrows]).astype(BF16)
        for t in range(sources):
            spread_copy(i, t, qbuf, b_send, b_recv).start()
        inverse_row = jnp.broadcast_to(inverse[own_heads : own_heads + 1], (8, LANES))
        x = inverse_row * tail + bias_col
        log_gate = jnp.minimum(x, 0.0) - jnp.log1p(jnp.exp(-jnp.abs(x)))
        log_gate = jnp.where((row8 < own_heads) & (lane8 < wrows), log_gate, 0.0)
        parts = dot(jnp.concatenate(split3(log_gate), axis=0), link_s[i])
        path_s[i] = parts[:8] + parts[8:16] + parts[16:24]

    for i in range(waves):
        owner_q(i)

    for i in range(waves):
        x_copy(i, kv_out, kv_in, kx_send, kx_recv).wait_recv()
        kv_own[i] = kv_own[i] + kv_in[i].astype(F32)
        kv_pass[i] = kv_own[i].astype(BF16)
        for d in range(1, n_far):
            z_copy(i, d, kv_pass, kv_far, kz_send, kz_recv).start()

    group = min(heads, 256 // head_dim)
    gwidth = group * head_dim
    g_head = iota((group, props, gwidth), 0)
    g_col = lax.div(iota((group, props, gwidth), 2), head_dim)
    g_diag = (g_head == g_col).reshape(group * props, gwidth)
    lane_w = iota((wrows, LANES), 1)
    position = iota((heads, pos_dev), 1) + me * pos_dev

    def mix_copy(i, t, which, src, dst):
        d, cross = targets[t]
        block = (1 - side if cross else side) * waves + i
        return pltpu.make_async_remote_copy(
            src_ref=src.at[block, far_id(d)],
            dst_ref=dst.at[t, i],
            send_sem=c_send.at[which, t, i],
            recv_sem=c_recv.at[which, t, i],
            device_id=target_id(d, cross),
        )

    def attend(i, cross):
        place = 1 - side if cross else side
        block = place * waves + i
        for t in range(sources):
            if targets[t][1] == cross:
                spread_wait(i, t, qbuf, b_send, b_recv)
        q_wave = jnp.concatenate([qbuf[block, f] for f in range(n_far)], axis=1).astype(F32)
        if exact_scale:
            q_wave = q_wave * scale
        mixes, tops, totals = [], [], []
        for j in range(wave):
            s = place * half_seqs + i * wave + j
            pltpu.make_async_copy(keys_hbm.at[s], keys.at[s], cache_sem.at[0, s]).wait()
            pltpu.make_async_copy(values_hbm.at[s], values.at[s], cache_sem.at[1, s]).wait()
            fade = jnp.where(position < lengths[s], decay[s], LOW)
            m_parts, t_parts, n_parts = [], [], []
            for g in range(heads // group):
                q = q_wave[j * props : (j + 1) * props, g * gwidth : (g + 1) * gwidth]
                q = jnp.broadcast_to(q[None], (group, props, gwidth)).reshape(group * props, gwidth)
                q = jnp.where(g_diag, q, 0.0).astype(BF16)
                scores = dot_nt(q, keys[s, :, g * gwidth : (g + 1) * gwidth])
                if not exact_scale:
                    scores = scores * scale
                fades = [
                    jnp.broadcast_to(fade[h : h + 1], (props, pos_dev))
                    for h in range(g * group, (g + 1) * group)
                ]
                scores = scores + jnp.concatenate(fades, axis=0)
                top = jnp.max(scores, axis=1, keepdims=True)
                w = jnp.exp(scores - top)
                total = jnp.sum(w, axis=1, keepdims=True)
                m = dot(w.astype(BF16), values[s, :, g * gwidth : (g + 1) * gwidth])
                m = jnp.where(g_diag, m, 0.0).reshape(group, props, gwidth)
                m_parts.append(jnp.sum(m, axis=0))
                for h in range(group):
                    t_parts.append(top[h * props : (h + 1) * props])
                    n_parts.append(total[h * props : (h + 1) * props])
            mixes.append(jnp.concatenate(m_parts, axis=1))
            tops.append(t_parts)
            totals.append(n_parts)
        mixed = jnp.concatenate(mixes, axis=0).astype(BF16)
        for f in range(n_far):
            mix[block, f] = mixed[:, f * cols : (f + 1) * cols]
        acc = jnp.zeros((wrows, LANES), F32)
        for h in range(heads):
            f, k = divmod(h, own_heads)
            for at, cols_of in ((k, tops), (own_heads + k, totals)):
                col = jnp.concatenate([cols_of[j][h] for j in range(wave)], axis=0)
                acc = jnp.where(lane_w == f * 8 + at, col, acc)
        flat = tile_rows(acc, LANES).T
        for f in range(n_far):
            stat[block, f] = flat[f * 8 : (f + 1) * 8]
        for t in range(sources):
            if targets[t][1] == cross:
                mix_copy(i, t, 0, mix, mix_in).start()
                mix_copy(i, t, 1, stat, stat_in).start()

    own_head_of = lax.div(iota((wrows, cols), 1), head_dim)

    def tree(i):
        block = side * waves + i
        total = kv_own[i, far]
        for d in range(1, n_far):
            z_copy(i, d, kv_pass, kv_far, kz_send, kz_recv).wait_recv()
            total = total + kv_far[d - 1, i].astype(F32)
        new_k = tile_rows(inv_s[i] * total[:wrows], LANES).astype(BF16)
        new_v = tile_rows(inv_s[i] * total[wrows:], LANES).astype(BF16)
        q = qbuf[block, far].astype(F32)
        q = jnp.concatenate([jnp.where(own_head_of == h, q, 0.0) for h in range(own_heads)], axis=0)
        scores = dot_nt(q.astype(BF16), new_k) * scale
        path = path_s[i]
        path_cols = tile_rows(path, LANES).T[:wrows]
        shifts = [path_cols[:, h : h + 1] - path[h : h + 1] for h in range(own_heads)]
        scores = scores + jnp.concatenate(shifts, axis=0)
        live = jnp.concatenate([anc_s[i, :wrows]] * own_heads, axis=0) > 0.5
        scores = jnp.where(live, scores, LOW)
        top = jnp.max(scores, axis=1, keepdims=True)
        w = jnp.where(live, jnp.exp(scores - top), 0.0)
        total = jnp.sum(w, axis=1, keepdims=True)
        m = dot(w.astype(BF16), new_v)
        merged = jnp.zeros((wrows, cols), F32)
        acc = jnp.zeros((wrows, LANES), F32)
        for h in range(own_heads):
            part = slice(h * wrows, (h + 1) * wrows)
            merged = jnp.where(own_head_of == h, m[part], merged)
            acc = jnp.where(lane_w == h, top[part], acc)
            acc = jnp.where(lane_w == own_heads + h, total[part], acc)
        tmix[i] = merged
        tstat[i] = tile_rows(acc, LANES).T[:8]

    def merge(i):
        block = side * waves + i
        for t in range(sources):
            mix_copy(i, t, 0, mix, mix_in).wait_recv()
            mix_copy(i, t, 1, stat, stat_in).wait_recv()
        stats = [stat[block, far]] + [stat_in[t, i] for t in range(sources)]
        path = path_s[i]
        tops = [st + path for st in stats] + [tstat[i]]
        totals = [pltpu.roll(st, 8 - own_heads, 0) for st in stats + [tstat[i]]]
        best = functools.reduce(jnp.maximum, tops)
        factors = [jnp.exp(top - best) for top in tops]
        denom = functools.reduce(jnp.add, [f * t for f, t in zip(factors, totals)])
        factors = [jnp.where(row8 < own_heads, f / denom, 0.0) for f in factors]
        turned = tile_rows(jnp.concatenate(factors, axis=0), LANES).T[:wrows]
        high = turned.astype(BF16)
        low = (turned - high.astype(F32)).astype(BF16)
        wide = dot(jnp.concatenate([high, low], axis=1), widen[...])
        mixes = [mix[block, far]] + [mix_in[t, i] for t in range(sources)] + [tmix[i]]
        numer = jnp.zeros((wrows, cols), F32)
        for k, m in enumerate(mixes):
            numer = numer + wide[:, k * cols : (k + 1) * cols] * m.astype(F32)
        att[block, far] = numer.astype(BF16)
        for t in range(sources):
            spread_copy(i, t, att, d_send, d_recv).start()

    per_tp = seqs // n_tp

    def e_copy(s, t):
        k = jnp.maximum(lax.rem(tp - t + n_tp, n_tp) - 1, 0)
        return pltpu.make_async_remote_copy(
            src_ref=terms.at[s],
            dst_ref=terms_in.at[k, lax.rem(s, per_tp)],
            send_sem=e_send.at[s],
            recv_sem=e_recv.at[k, lax.rem(s, per_tp)],
            device_id={"tp": t},
        )

    def output(i, cross):
        place = 1 - side if cross else side
        block = place * waves + i
        for t in range(sources):
            if targets[t][1] == cross:
                spread_wait(i, t, att, d_send, d_recv)
        attended = jnp.concatenate([att[block, f] for f in range(n_far)], axis=1)
        term = dot(attended, out_w[...])
        for j in range(wave):
            s = place * half_seqs + i * wave + j
            terms[s] = fold(term[j * props : (j + 1) * props]).astype(BF16)
            t = lax.div(s, per_tp)
            pl.when(tp != t)(e_copy(s, t).start)

    for i in range(waves):
        for cross in range(2):
            attend(i, cross)
        if i > 0:
            merge(i - 1)
        tree(i)
    merge(waves - 1)
    load_of["out"].wait()
    for i in range(waves):
        for cross in range(2):
            output(i, cross)

    done = []
    for j in range(per_tp):
        total = unfold(terms[tp * per_tp + j])
        for k in range(1, n_tp):
            pltpu.make_async_remote_copy(
                src_ref=terms.at[0],
                dst_ref=terms_in.at[k - 1, j],
                send_sem=e_send.at[0],
                recv_sem=e_recv.at[k - 1, j],
                device_id={"tp": lax.rem(tp + k, n_tp)},
            ).wait_recv()
            total = total + unfold(terms_in[k - 1, j])
        done.append(total)
    out[...] = jnp.concatenate(done, axis=0).astype(BF16)

    for i in range(waves):
        x_copy(i, q_out, q_in, qx_send, qx_recv).wait_send()
        x_copy(i, kv_out, kv_in, kx_send, kx_recv).wait_send()
        for d in range(1, n_far):
            z_copy(i, d, q_own, q_far, qz_send, qz_recv).wait_send()
            z_copy(i, d, kv_pass, kv_far, kz_send, kz_recv).wait_send()
        for t in range(sources):
            spread_copy(i, t, qbuf, b_send, b_recv).wait_send()
            spread_copy(i, t, att, d_send, d_recv).wait_send()
            mix_copy(i, t, 0, mix, mix_in).wait_send()
            mix_copy(i, t, 1, stat, stat_in).wait_send()
    for s in range(seqs):
        t = s // per_tp
        pl.when(tp != t)(e_copy(s, t).wait_send)


def wave_size(n, n_tp, seqs, props, heads, width):
    n_far = n // 2
    if n % 2 or seqs % 2 or seqs % n_tp or heads % n_far or width % (n_far * LANES):
        return 0
    head_dim = width // heads
    own = heads // n_far
    if own > 4 or 8 * (n + 1) > LANES or (heads % min(heads, max(256 // head_dim, 1))):
        return 0
    for wave in range(1, seqs // 2 + 1):
        fits = wave * props % 16 == 0 and wave * props <= LANES
        if seqs // 2 % wave == 0 and fits and props % 8 == 0:
            return wave
    return 0


def solution(mesh):
    n, n_tp = mesh.shape["kv"], mesh.shape["tp"]

    def body(
        tokens,
        norm_gain,
        query_weight,
        key_weight,
        value_weight,
        gate_weight,
        gate_bias,
        out_weight,
        cache_keys,
        cache_values,
        cache_decay,
        lengths,
        parents,
    ):
        rows, depth = tokens.shape
        seqs, props = parents.shape
        heads = cache_decay.shape[1]
        pos_dev = cache_keys.shape[1]
        width = query_weight.shape[1]
        cols = out_weight.shape[1]
        slots = -(-seqs // n)
        block = rows // n_tp
        all_w = 2 * width + LANES
        folded = (2 * props, width // 2)
        vmem = pl.BlockSpec(memory_space=pltpu.VMEM)
        hbm = pl.BlockSpec(memory_space=pltpu.HBM)
        dma = pltpu.SemaphoreType.DMA
        wave = wave_size(n, n_tp, seqs, props, heads, width)
        if wave:
            n_far = n // 2
            waves = seqs // 2 // wave
            wrows = wave * props
            wcols = width // n_far
            per_tp = seqs // n_tp
            block_q = (n_far, wrows + 8, wcols)
            block_kv = (n_far, 2 * wrows, wcols)
            body_of = functools.partial(by_heads, n, n_tp, wave)
            scratch = [
                pltpu.VMEM(tokens.shape, BF16),
                pltpu.VMEM((1, depth), F32),
                pltpu.VMEM(query_weight.shape, BF16),
                pltpu.VMEM(key_weight.shape, BF16),
                pltpu.VMEM(value_weight.shape, BF16),
                pltpu.VMEM((gate_weight.shape[1], depth), BF16),
                pltpu.VMEM((1, gate_bias.shape[0]), F32),
                pltpu.VMEM(cache_decay.shape, F32),
                pltpu.SMEM(lengths.shape, jnp.int32),
                pltpu.VMEM(parents.shape, jnp.int32),
                pltpu.VMEM(out_weight.shape, BF16),
                pltpu.VMEM(cache_keys.shape, BF16),
                pltpu.VMEM(cache_values.shape, BF16),
                pltpu.VMEM((rows, 3 * depth), BF16),
                pltpu.VMEM((waves,) + block_q, F32),
                pltpu.VMEM((waves,) + block_q, F32),
                pltpu.VMEM((waves,) + block_q, F32),
                pltpu.VMEM((n_far - 1, waves) + block_q[1:], F32),
                pltpu.VMEM((waves,) + block_kv, BF16),
                pltpu.VMEM((waves,) + block_kv, BF16),
                pltpu.VMEM((waves,) + block_kv, F32),
                pltpu.VMEM((waves,) + block_kv, BF16),
                pltpu.VMEM((n_far - 1, waves) + block_kv[1:], BF16),
                pltpu.VMEM((2 * waves, n_far, wrows, wcols), BF16),
                pltpu.VMEM((2 * waves, n_far, wrows, wcols), BF16),
                pltpu.VMEM((n - 1, waves, wrows, wcols), BF16),
                pltpu.VMEM((2 * waves, n_far, 8, LANES), F32),
                pltpu.VMEM((n - 1, waves, 8, LANES), F32),
                pltpu.VMEM((2 * waves, n_far, wrows, wcols), BF16),
                pltpu.VMEM((seqs,) + folded, BF16),
                pltpu.VMEM((n_tp - 1, per_tp) + folded, BF16),
                pltpu.VMEM((-(-seqs // 8) * 8, LANES), jnp.int32),
                pltpu.VMEM((waves, LANES, LANES), BF16),
                pltpu.VMEM((waves, LANES, LANES), F32),
                pltpu.VMEM((waves, 8, LANES), F32),
                pltpu.VMEM((waves, wrows, wcols), F32),
                pltpu.VMEM((waves, wrows, wcols), F32),
                pltpu.VMEM((waves, 8, LANES), F32),
                pltpu.VMEM((2 * LANES, (n + 1) * wcols), BF16),
                dma((11,)),
                dma((2, seqs)),
                dma((waves,)),
                dma((waves,)),
                dma((waves,)),
                dma((waves,)),
                dma((n_far - 1, waves)),
                dma((n_far - 1, waves)),
                dma((n_far - 1, waves)),
                dma((n_far - 1, waves)),
                dma((n - 1, waves)),
                dma((2 * waves, n_far)),
                dma((2, n - 1, waves)),
                dma((2, n - 1, waves)),
                dma((n - 1, waves)),
                dma((2 * waves, n_far)),
                dma((seqs,)),
                dma((n_tp - 1, per_tp)),
            ]
        else:
            body_of = functools.partial(by_sequence, n, n_tp)
            scratch = [
                pltpu.VMEM(tokens.shape, BF16),
                pltpu.VMEM((1, depth), F32),
                pltpu.VMEM(query_weight.shape, BF16),
                pltpu.VMEM(key_weight.shape, BF16),
                pltpu.VMEM(value_weight.shape, BF16),
                pltpu.VMEM((1, gate_bias.shape[0]), F32),
                pltpu.VMEM(cache_decay.shape, F32),
                pltpu.SMEM(lengths.shape, jnp.int32),
                pltpu.VMEM(parents.shape, jnp.int32),
                dma((9,)),
                pltpu.VMEM((seqs, props, all_w), F32),
                pltpu.VMEM((seqs,) + folded, BF16),
                pltpu.VMEM((seqs, props, all_w), F32),
                pltpu.VMEM((seqs,) + folded, BF16),
                pltpu.VMEM((n // 2 - 1, slots, props, all_w), F32),
                pltpu.VMEM((n // 2 - 1, slots) + folded, BF16),
                pltpu.VMEM((gate_weight.shape[1], depth), BF16),
                pltpu.VMEM(out_weight.shape, BF16),
                pltpu.VMEM(cache_keys.shape, BF16),
                pltpu.VMEM(cache_values.shape, BF16),
                pltpu.VMEM((seqs,) + folded, BF16),
                pltpu.VMEM((seqs,) + folded, BF16),
                pltpu.VMEM((seqs, props, LANES), F32),
                pltpu.VMEM((n - 1, slots) + folded, BF16),
                pltpu.VMEM((n - 1, slots, props, LANES), F32),
                pltpu.VMEM((seqs,) + folded, BF16),
                pltpu.VMEM((slots, props, LANES), F32),
                pltpu.VMEM((slots, props, LANES), F32),
                pltpu.VMEM((slots, props, width), F32),
                pltpu.VMEM((slots, 2, props, LANES), F32),
                pltpu.VMEM((slots, 2, LANES, width), F32),
                pltpu.VMEM((n_tp, block, cols), BF16),
                pltpu.VMEM((n_tp - 1, block, cols), BF16),
                pltpu.VMEM((-(-seqs // 8) * 8, LANES), jnp.int32),
                dma((2,)),
                dma((2, seqs)),
                dma((2, seqs)),
                dma((2, seqs)),
                dma((2, seqs)),
                dma((2, n // 2 - 1, slots)),
                dma((slots, n - 1)),
                dma((seqs,)),
                dma((2, seqs)),
                dma((2, n - 1, slots)),
                dma((slots, n - 1)),
                dma((seqs,)),
                dma((n_tp,)),
                dma((n_tp - 1,)),
            ]
        return pl.pallas_call(
            body_of,
            out_shape=jax.ShapeDtypeStruct((block, cols), BF16),
            in_specs=[hbm] * 13,
            out_specs=vmem,
            scratch_shapes=scratch,
            compiler_params=pltpu.CompilerParams(
                collective_id=0, has_side_effects=True, vmem_limit_bytes=67_043_328
            ),
        )(
            tokens,
            norm_gain.reshape(1, depth),
            query_weight,
            key_weight,
            value_weight,
            gate_weight.T,
            gate_bias.reshape(1, gate_bias.shape[0]),
            out_weight,
            cache_keys,
            cache_values,
            cache_decay,
            lengths,
            parents,
        )

    in_specs = (
        P(None, "kv"),
        P("kv"),
        P("kv", "tp"),
        P("kv", "tp"),
        P("kv", "tp"),
        P(),
        P(),
        P("tp", "kv"),
        P(None, "kv", "tp"),
        P(None, "kv", "tp"),
        P(None, "tp", "kv"),
        P(),
        P(),
    )
    out_specs = P("tp", "kv")
    return jax.shard_map(body, mesh=mesh, in_specs=in_specs, out_specs=out_specs, check_vma=False)
```

```python
import functools
import math

import jax
import jax.numpy as jnp
from jax import lax
from jax.experimental import pallas as pl
from jax.experimental.pallas import tpu as pltpu
from jax.sharding import PartitionSpec as P

F32 = jnp.float32
BF16 = jnp.bfloat16
LANES = 128
LOW = -1e30
NT = (((1,), (1,)), ((), ()))
HIGH = lax.Precision.HIGHEST


def dot(a, b, precision=None):
    return jnp.dot(a, b, preferred_element_type=F32, precision=precision)


def dot_nt(a, b, precision=None):
    return lax.dot_general(a, b, NT, preferred_element_type=F32, precision=precision)


def fold(x):
    half = x.shape[1] // 2
    return jnp.concatenate([x[:, :half], x[:, half:]], axis=0)


def unfold(x):
    rows = x.shape[0] // 2
    x = x.astype(F32)
    return jnp.concatenate([x[:rows], x[rows:]], axis=1)


def by_sequence(
    n,
    n_tp,
    tokens_hbm,
    gain_hbm,
    query_hbm,
    key_hbm,
    value_hbm,
    gate_hbm,
    bias_hbm,
    out_hbm,
    keys_hbm,
    values_hbm,
    decay_hbm,
    lengths_hbm,
    parents_hbm,
    out,
    tokens,
    gain,
    query_w,
    key_w,
    value_w,
    bias,
    decay,
    lengths,
    parents,
    small_sem,
    part,
    part_v,
    pair_in,
    pair_in_v,
    part_in,
    part_in_v,
    gate_w,
    out_w,
    keys,
    values,
    qbuf,
    mix,
    stat,
    mix_in,
    stat_in,
    att,
    anc,
    path_s,
    tmix,
    tstat,
    kvnew,
    terms,
    terms_in,
    par_pad,
    load_sem,
    cache_sem,
    p_send,
    p_recv,
    a_send,
    a_recv,
    b_send,
    b_recv,
    c_send,
    c_recv,
    d_send,
    d_recv,
    e_send,
    e_recv,
):
    me = lax.axis_index("kv")
    tp = lax.axis_index("tp")
    rows, depth = tokens.shape
    seqs, props = parents.shape
    heads = decay.shape[1]
    pos_dev = keys.shape[1]
    width = query_w.shape[1]
    head_dim = width // heads
    scale = head_dim ** (-0.5)
    slots = part_in.shape[1]
    parity = lax.rem(tp, 2)
    left_over = seqs % n
    hp = heads * props

    barrier = pltpu.get_barrier_semaphore()
    for k in range(1, n):
        pl.semaphore_signal(barrier, inc=1, device_id={"kv": lax.rem(me + k, n)})
    for k in range(1, n_tp):
        pl.semaphore_signal(barrier, inc=1, device_id={"tp": lax.rem(tp + k, n_tp)})

    pairs = (
        (tokens_hbm, tokens),
        (gain_hbm, gain),
        (query_hbm, query_w),
        (key_hbm, key_w),
        (value_hbm, value_w),
        (bias_hbm, bias),
        (parents_hbm, parents),
        (decay_hbm, decay),
        (lengths_hbm, lengths),
    )
    small_loads = [
        pltpu.make_async_copy(src, dst, small_sem.at[i]) for i, (src, dst) in enumerate(pairs)
    ]
    for load in small_loads:
        load.start()
    gate_load = pltpu.make_async_copy(
        gate_hbm.at[:, pl.ds(pl.multiple_of(me * depth, depth), depth)], gate_w, load_sem.at[0]
    )
    gate_load.start()
    cache_loads = []
    for s in range(seqs):
        k_load = pltpu.make_async_copy(keys_hbm.at[s], keys.at[s], cache_sem.at[0, s])
        v_load = pltpu.make_async_copy(values_hbm.at[s], values.at[s], cache_sem.at[1, s])
        k_load.start()
        v_load.start()
        cache_loads.append((k_load, v_load))
    out_load = pltpu.make_async_copy(out_hbm, out_w, load_sem.at[1])
    out_load.start()

    def owner_of(s):
        if isinstance(s, int):
            place = s % n
            shift = parity * left_over if s // n == seqs // n else 0
        else:
            place = lax.rem(s, n)
            shift = jnp.where(lax.div(s, n) == seqs // n, parity * left_over, 0)
        return lax.rem(place + shift, n)

    def slot_seq(r):
        shift = parity * left_over if r == seqs // n else 0
        return r * n + lax.rem(me + 2 * n - shift, n)

    def for_slot(r, f):
        if (r + 1) * n <= seqs:
            f()
        else:
            pl.when(slot_seq(r) < seqs)(f)

    for load in small_loads:
        load.wait()
    xf = tokens[...].astype(F32)
    squares = jnp.sum(xf * xf, axis=1, keepdims=True)
    normed = (xf * gain[...]).astype(BF16)
    sel_rows = lax.broadcasted_iota(jnp.int32, (bias.shape[1], LANES), 0)
    sel_cols = lax.broadcasted_iota(jnp.int32, (bias.shape[1], LANES), 1)
    select = ((sel_rows == sel_cols + tp * heads) & (sel_cols < heads)).astype(F32)
    for i, w in enumerate((query_w, key_w)):
        part[:, :, i * width : (i + 1) * width] = dot(normed, w[...]).reshape(seqs, props, width)
    value_part = dot(normed, value_w[...])
    for s in range(seqs):
        part_v[s] = fold(value_part[s * props : (s + 1) * props]).astype(BF16)
    gate_load.wait()
    gates_w = lax.dot_general(
        select.astype(BF16), gate_w[...], (((0,), (0,)), ((), ())), preferred_element_type=F32
    )
    gate_part = dot_nt(normed, gates_w.astype(BF16))
    lane = lax.broadcasted_iota(jnp.int32, (rows, LANES), 1)
    gate_part = jnp.where(lane == LANES // 2, squares, gate_part)
    part[:, :, 2 * width :] = gate_part.reshape(seqs, props, LANES)
    pl.semaphore_wait(barrier, n + n_tp - 2)

    side = lax.rem(me, 2)
    partner = me + 1 - 2 * side
    n_far = n // 2
    shares = ((part, pair_in, part_in), (part_v, pair_in_v, part_in_v))

    def p_copy(s, which):
        src, dst, _ = shares[which]
        return pltpu.make_async_remote_copy(
            src_ref=src.at[s],
            dst_ref=dst.at[s],
            send_sem=p_send.at[which, s],
            recv_sem=p_recv.at[which, s],
            device_id={"kv": partner},
        )

    def a_copy(s, which):
        src, _, dst = shares[which]
        d = owner_of(s)
        k = jnp.maximum(lax.rem(lax.div(me, 2) - lax.div(d, 2) + n_far, n_far) - 1, 0)
        return pltpu.make_async_remote_copy(
            src_ref=src.at[s],
            dst_ref=dst.at[k, s // n],
            send_sem=a_send.at[which, s],
            recv_sem=a_recv.at[which, k, s // n],
            device_id={"kv": d},
        )

    def crosses(s):
        return lax.rem(owner_of(s), 2) != side

    def passes(s):
        d = owner_of(s)
        return (lax.rem(d, 2) == side) & (d != me)

    for s in range(seqs):
        for which in range(2):
            pl.when(crosses(s))(p_copy(s, which).start)

    par_pad[...] = jnp.zeros(par_pad.shape, jnp.int32)
    par_pad[0:seqs, 0:props] = parents[...]
    r_i = lax.broadcasted_iota(jnp.int32, (LANES, LANES), 0)
    c_i = lax.broadcasted_iota(jnp.int32, (LANES, LANES), 1)
    eye = (r_i == c_i).astype(F32)
    bias_row = dot(jnp.broadcast_to(bias[...], (8, bias.shape[1])), select, HIGH)[0:1]

    def ancestry(r):
        s = slot_seq(r)
        row = par_pad[pl.ds(s, 1), :]
        link = jnp.maximum((row == r_i).astype(F32), eye).astype(BF16)
        for _ in range(props.bit_length()):
            link = jnp.minimum(dot(link, link), 1.0).astype(BF16)
        anc[r] = dot_nt(eye.astype(BF16), link)[:props]

    for r in range(slots):
        for_slot(r, functools.partial(ancestry, r))

    def pass_on(s):
        for which in range(2):
            p_copy(s, which).wait_recv()
        part[s] = part[s] + pair_in[s]
        part_v[s] = (part_v[s].astype(F32) + pair_in_v[s].astype(F32)).astype(BF16)
        for which in range(2):
            a_copy(s, which).start()

    for s in range(seqs):
        pl.when(passes(s))(functools.partial(pass_on, s))

    lane_p = lax.broadcasted_iota(jnp.int32, (props, LANES), 1)
    bd_row = lax.broadcasted_iota(jnp.int32, (heads, props, width), 0)
    bd_col = lax.broadcasted_iota(jnp.int32, (heads, props, width), 2)
    diag = (lax.div(bd_col, head_dim) == bd_row).reshape(hp, width)

    def spread(q):
        wide = jnp.broadcast_to(q[None], (heads, props, width)).reshape(hp, width)
        return jnp.where(diag, wide, 0.0).astype(BF16)

    def gather_diag(m):
        return jnp.sum(jnp.where(diag, m, 0.0).reshape(heads, props, width), axis=0)

    def to_lanes(col, first):
        acc = jnp.zeros((props, LANES), F32)
        for h in range(heads):
            acc = jnp.where(lane_p == h + first, col[h * props : (h + 1) * props], acc)
        return acc

    def b_copy(r, k, buf, send, recv):
        s = slot_seq(r)
        return pltpu.make_async_remote_copy(
            src_ref=buf.at[s],
            dst_ref=buf.at[s],
            send_sem=send.at[r, k - 1],
            recv_sem=recv.at[s],
            device_id={"kv": lax.rem(me + k, n)},
        )

    pad_rows = LANES - props

    def project(r):
        s = slot_seq(r)
        for which, (src, near, far) in enumerate(shares):
            pltpu.make_async_remote_copy(
                src_ref=src.at[0],
                dst_ref=near.at[s],
                send_sem=p_send.at[which, 0],
                recv_sem=p_recv.at[which, s],
                device_id={"kv": partner},
            ).wait_recv()
            for k in range(1, n_far):
                pltpu.make_async_remote_copy(
                    src_ref=src.at[0],
                    dst_ref=far.at[k - 1, r],
                    send_sem=a_send.at[which, 0],
                    recv_sem=a_recv.at[which, k - 1, r],
                    device_id={"kv": lax.rem(me + 2 * k, n)},
                ).wait_recv()
        total = part[s] + pair_in[s]
        total_v = unfold(part_v[s]) + unfold(pair_in_v[s])
        for k in range(1, n_far):
            total = total + part_in[k - 1, r]
            total_v = total_v + unfold(part_in_v[k - 1, r])
        tail = total[:, 2 * width :]
        square = jnp.sum(jnp.where(lane_p == LANES // 2, tail, 0.0), axis=1, keepdims=True)
        inverse = lax.rsqrt(square / (depth * n) + 1e-06)
        q = inverse * total[:, :width]
        qbuf[s] = fold(q).astype(BF16)
        for k in range(1, n):
            b_copy(r, k, qbuf, b_send, b_recv).start()
        kvnew[r, 0, 0:props] = inverse * total[:, width : 2 * width]
        kvnew[r, 1, 0:props] = inverse * total_v
        kvnew[r, :, props:] = jnp.zeros((2, pad_rows, width), F32)
        x = inverse * tail + bias_row
        log_gate = jnp.minimum(x, 0.0) - jnp.log1p(jnp.exp(-jnp.abs(x)))
        padded = jnp.concatenate([log_gate, jnp.zeros((pad_rows, LANES), F32)], axis=0)
        path_s[r] = dot(anc[r], padded, HIGH)

    def tree(r):
        s = slot_seq(r)
        path = path_s[r]
        q = spread(unfold(qbuf[s]))
        head_of = lax.broadcasted_iota(jnp.int32, (heads, props, LANES), 0)
        lane_of = lax.broadcasted_iota(jnp.int32, (heads, props, LANES), 2)
        pick = (head_of == lane_of).reshape(hp, LANES)
        tiled = jnp.broadcast_to(path[None], (heads, props, LANES)).reshape(hp, LANES)
        own = jnp.sum(jnp.where(pick, tiled, 0.0), axis=1, keepdims=True)
        padded = jnp.concatenate([path, jnp.zeros((pad_rows, LANES), F32)], axis=0)
        other = dot_nt(pick.astype(F32), padded, HIGH)
        scores = dot_nt(q, kvnew[r, 0].astype(BF16)) * scale + own - other
        live = jnp.broadcast_to(anc[r][None], (heads, props, LANES)).reshape(hp, LANES) > 0.5
        scores = jnp.where(live, scores, LOW)
        top = jnp.max(scores, axis=1, keepdims=True)
        w = jnp.where(live, jnp.exp(scores - top), 0.0)
        total = jnp.sum(w, axis=1, keepdims=True)
        tmix[r] = gather_diag(dot(w.astype(BF16), kvnew[r, 1].astype(BF16)))
        tstat[r, 0] = to_lanes(top, 0)
        tstat[r, 1] = to_lanes(total, 0)

    position = lax.broadcasted_iota(jnp.int32, (hp, pos_dev), 1) + me * pos_dev

    def c_copy(s, which, src, dst):
        d = owner_of(s)
        k = jnp.maximum(lax.rem(me - d + n, n) - 1, 0)
        slot = s // n if isinstance(s, int) else lax.div(s, n)
        return d, pltpu.make_async_remote_copy(
            src_ref=src.at[s],
            dst_ref=dst.at[k, slot],
            send_sem=c_send.at[which, s],
            recv_sem=c_recv.at[which, k, slot],
            device_id={"kv": d},
        )

    def shard(s, carry):
        d = owner_of(s)

        @pl.when(d != me)
        def _():
            pltpu.make_async_remote_copy(
                src_ref=qbuf.at[s],
                dst_ref=qbuf.at[s],
                send_sem=b_send.at[0, 0],
                recv_sem=b_recv.at[s],
                device_id={"kv": d},
            ).wait_recv()

        pltpu.make_async_copy(keys_hbm.at[s], keys.at[s], cache_sem.at[0, s]).wait()
        pltpu.make_async_copy(values_hbm.at[s], values.at[s], cache_sem.at[1, s]).wait()
        q = spread(unfold(qbuf[s]))
        fade = decay[s]
        fade = jnp.concatenate(
            [jnp.broadcast_to(fade[h : h + 1], (props, pos_dev)) for h in range(heads)], axis=0
        )
        scores = dot_nt(q, keys[s]) * scale + fade
        live = position < lengths[s]
        scores = jnp.where(live, scores, LOW)
        top = jnp.max(scores, axis=1, keepdims=True)
        w = jnp.where(live, jnp.exp(scores - top), 0.0)
        total = jnp.sum(w, axis=1, keepdims=True)
        mix[s] = fold(gather_diag(dot(w.astype(BF16), values[s]))).astype(BF16)
        stat[s] = to_lanes(top, 0) + to_lanes(total, heads)
        for which, (src, dst) in enumerate(((mix, mix_in), (stat, stat_in))):
            _, copy = c_copy(s, which, src, dst)
            pl.when(d != me)(copy.start)
        return carry

    ex_r = lax.broadcasted_iota(jnp.int32, (LANES, width), 0)
    ex_c = lax.broadcasted_iota(jnp.int32, (LANES, width), 1)
    widen = (ex_r == lax.div(ex_c, head_dim)).astype(F32)

    def merge(r):
        s = slot_seq(r)
        for k in range(1, n):
            for which, (src, dst) in enumerate(((mix, mix_in), (stat, stat_in))):
                pltpu.make_async_remote_copy(
                    src_ref=src.at[0],
                    dst_ref=dst.at[k - 1, r],
                    send_sem=c_send.at[which, 0],
                    recv_sem=c_recv.at[which, k - 1, r],
                    device_id={"kv": lax.rem(me + k, n)},
                ).wait_recv()
        stats = jnp.concatenate([stat[s]] + [stat_in[k, r] for k in range(n - 1)], axis=0)
        totals = pltpu.roll(stats, LANES - heads, 1).reshape(n, props, LANES)
        tops = stats.reshape(n, props, LANES) + path_s[r][None]
        tops = jnp.where((lane_p < heads)[None], tops, LOW)
        ttop = jnp.where(lane_p < heads, tstat[r, 0], LOW)
        best = jnp.maximum(jnp.max(tops, axis=0), ttop)
        factors = jnp.exp(tops - best[None])
        tfactor = jnp.exp(ttop - best)
        denom = jnp.sum(factors * totals, axis=0) + tfactor * tstat[r, 1]
        packed = jnp.concatenate([factors.reshape(n * props, LANES), tfactor, denom], axis=0)
        wide = dot(packed, widen, HIGH)
        numer = wide[n * props : (n + 1) * props] * tmix[r] + wide[:props] * unfold(mix[s])
        for k in range(1, n):
            numer = numer + wide[k * props : (k + 1) * props] * unfold(mix_in[k - 1, r])
        att[s] = fold(numer / wide[(n + 1) * props :]).astype(BF16)
        for k in range(1, n):
            b_copy(r, k, att, d_send, d_recv).start()

    for r in range(slots):
        for_slot(r, functools.partial(project, r))
        if r > 0:
            for_slot(r - 1, functools.partial(merge, r - 1))
        for_slot(r, functools.partial(tree, r))
        lax.fori_loop(r * n, min((r + 1) * n, seqs), shard, 0)
    for_slot(slots - 1, functools.partial(merge, slots - 1))

    out_load.wait()
    block = rows // n_tp

    def e_copy(t):
        k = lax.rem(tp - t + n_tp, n_tp)
        return pltpu.make_async_remote_copy(
            src_ref=terms.at[t],
            dst_ref=terms_in.at[jnp.maximum(k - 1, 0)],
            send_sem=e_send.at[t],
            recv_sem=e_recv.at[jnp.maximum(k - 1, 0)],
            device_id={"tp": t},
        )

    arrived = 0
    for t in range(n_tp):
        first, last = t * block // props, ((t + 1) * block - 1) // props + 1
        for s in range(arrived, last):
            d = owner_of(s)

            @pl.when(d != me)
            def _(s=s, d=d):
                pltpu.make_async_remote_copy(
                    src_ref=att.at[s],
                    dst_ref=att.at[s],
                    send_sem=d_send.at[0, 0],
                    recv_sem=d_recv.at[s],
                    device_id={"kv": d},
                ).wait_recv()

        arrived = max(arrived, last)
        attended = jnp.concatenate([unfold(att[s]) for s in range(first, last)], axis=0)
        term = dot(attended.astype(BF16), out_w[...])
        begin = t * block - first * props
        terms[t] = term[begin : begin + block].astype(BF16)
        pl.when(tp != t)(e_copy(t).start)
    total = terms[tp].astype(F32)
    for k in range(1, n_tp):
        pltpu.make_async_remote_copy(
            src_ref=terms.at[0],
            dst_ref=terms_in.at[k - 1],
            send_sem=e_send.at[0],
            recv_sem=e_recv.at[k - 1],
            device_id={"tp": lax.rem(tp + k, n_tp)},
        ).wait_recv()
        total = total + terms_in[k - 1].astype(F32)
    out[...] = total.astype(BF16)

    for s in range(seqs):
        d = owner_of(s)
        for which in range(2):
            pl.when(crosses(s))(p_copy(s, which).wait_send)
            pl.when(passes(s))(a_copy(s, which).wait_send)
        for which, (src, dst) in enumerate(((mix, mix_in), (stat, stat_in))):
            _, copy = c_copy(s, which, src, dst)
            pl.when(d != me)(copy.wait_send)
    for r in range(slots):

        def drain(r=r):
            for k in range(1, n):
                b_copy(r, k, qbuf, b_send, b_recv).wait_send()
                b_copy(r, k, att, d_send, d_recv).wait_send()

        for_slot(r, drain)
    for t in range(n_tp):
        pl.when(tp != t)(e_copy(t).wait_send)


def split3(x):
    high = x.astype(BF16)
    rest = x - high.astype(F32)
    mid = rest.astype(BF16)
    low = (rest - mid.astype(F32)).astype(BF16)
    return high, mid, low


def tile_rows(rows, total):
    return jnp.concatenate([rows, jnp.zeros((total - rows.shape[0], rows.shape[1]), rows.dtype)], axis=0)


def by_heads(
    n,
    n_tp,
    wave,
    tokens_hbm,
    gain_hbm,
    query_hbm,
    key_hbm,
    value_hbm,
    gate_hbm,
    bias_hbm,
    out_hbm,
    keys_hbm,
    values_hbm,
    decay_hbm,
    lengths_hbm,
    parents_hbm,
    out,
    tokens,
    gain,
    query_w,
    key_w,
    value_w,
    gate_w,
    bias,
    decay,
    lengths,
    parents,
    out_w,
    keys,
    values,
    feats,
    q_out,
    q_in,
    q_own,
    q_far,
    q_last,
    q_last_in,
    q_cross,
    kv_out,
    kv_in,
    kv_own,
    kv_pass,
    kv_far,
    qbuf,
    mix,
    mix_in,
    stat,
    stat_in,
    att,
    terms,
    terms_in,
    par_pad,
    link_s,
    anc_s,
    path_s,
    inv_s,
    tmix,
    tstat,
    widen,
    load_sem,
    cache_sem,
    qx_send,
    qx_recv,
    kx_send,
    kx_recv,
    qz_send,
    qz_recv,
    kz_send,
    kz_recv,
    b_send,
    b_recv,
    c_send,
    c_recv,
    d_send,
    d_recv,
    e_send,
    e_recv,
    qr_send,
    qr_recv,
    ar_send,
    ar_recv,
    l_send,
    l_recv,
):
    me = lax.axis_index("kv")
    tp = lax.axis_index("tp")
    side = lax.rem(me, 2)
    far = lax.div(me, 2)
    n_far = n // 2
    rows, depth = tokens.shape
    seqs, props = parents.shape
    heads = decay.shape[1]
    pos_dev = keys.shape[1]
    width = query_w.shape[1]
    head_dim = width // heads
    scale = head_dim ** (-0.5)
    exact_scale = math.frexp(scale)[0] == 0.5
    own_heads = heads // n_far
    cols = width // n_far
    half_seqs = seqs // 2
    half = rows // 2
    waves = half_seqs // wave
    wrows = wave * props
    sources = n - 1

    pairs = (
        (tokens_hbm, tokens),
        (gain_hbm, gain),
        (gate_hbm.at[:, pl.ds(pl.multiple_of(me * depth, depth), depth)], gate_w),
        (query_hbm, query_w),
        (key_hbm, key_w),
        (value_hbm, value_w),
        (bias_hbm, bias),
        (parents_hbm, parents),
        (lengths_hbm, lengths),
        (decay_hbm, decay),
        (out_hbm, out_w),
    )
    loads = [pltpu.make_async_copy(src, dst, load_sem.at[i]) for i, (src, dst) in enumerate(pairs)]
    load_of = dict(
        zip(("tokens", "gain", "gate", "q", "k", "v", "bias", "parents", "lengths", "decay", "out"), loads)
    )
    for load in loads[:6]:
        load.start()
    barrier = pltpu.get_barrier_semaphore()
    for k in range(1, n):
        pl.semaphore_signal(barrier, inc=1, device_id={"kv": lax.rem(me + k, n)})
    for k in range(1, n_tp):
        pl.semaphore_signal(barrier, inc=1, device_id={"tp": lax.rem(tp + k, n_tp)})

    def iota(shape, dim):
        return lax.broadcasted_iota(jnp.int32, shape, dim)

    def far_id(d):
        return lax.rem(far + d, n_far)

    def near_id(z, x):
        return {"kv": z * 2 + x}

    own_half = pl.multiple_of(side * half, half)
    peer_half = pl.multiple_of((1 - side) * half, half)

    load_of["tokens"].wait()
    load_of["gain"].wait()
    for load in loads[6:]:
        load.start()
    for s in range(seqs):
        pltpu.make_async_copy(keys_hbm.at[s], keys.at[s], cache_sem.at[0, s]).start()
        pltpu.make_async_copy(values_hbm.at[s], values.at[s], cache_sem.at[1, s]).start()
    xf = tokens[...].astype(F32)
    feats[:, :depth] = (xf * gain[...]).astype(BF16)
    square = xf * xf
    high = square.astype(BF16)
    feats[:, depth : 2 * depth] = high
    feats[:, 2 * depth :] = (square - high.astype(F32)).astype(BF16)

    load_of["gate"].wait()
    t_rows = n_far * 8
    p_row = iota((t_rows, gate_w.shape[0]), 0)
    p_col = iota((t_rows, gate_w.shape[0]), 1)
    p_in = lax.rem(p_row, 8)
    wanted = (p_in < own_heads) & (p_col == tp * heads + lax.div(p_row, 8) * own_heads + p_in)
    gates = dot(wanted.astype(BF16), gate_w[...]).astype(BF16)
    ones = (lax.rem(iota((t_rows, depth), 0), 8) == own_heads).astype(BF16)
    tails = jnp.concatenate([gates, ones, ones], axis=1)

    def project_q(base, dst, which):
        full = dot(feats[pl.ds(base, half), :depth], query_w[...])
        for i in range(waves):
            piece = full[i * wrows : (i + 1) * wrows]
            tail = dot_nt(tails, feats[pl.ds(base + i * wrows, wrows), :])
            tail = jnp.concatenate([tail, jnp.zeros((t_rows, LANES - wrows), F32)], axis=1)
            for f in range(n_far):
                for at, rows_of in (
                    (slice(0, wrows), piece[:, f * cols : (f + 1) * cols]),
                    (slice(wrows, wrows + 8), tail[f * 8 : (f + 1) * 8]),
                ):
                    if i < waves - 1:
                        dst[i, f, at] = rows_of
                    else:
                        q_last[f, which, at] = rows_of

    def project_kv(base, dst):
        for which, w in enumerate((key_w, value_w)):
            full = dot(feats[pl.ds(base, half), :depth], w[...])
            for i in range(waves):
                piece = full[i * wrows : (i + 1) * wrows].astype(dst.dtype)
                for f in range(n_far):
                    dst[i, f, which * wrows : (which + 1) * wrows] = piece[:, f * cols : (f + 1) * cols]

    def x_copy(i, src, dst, send, recv):
        return pltpu.make_async_remote_copy(
            src_ref=src.at[i],
            dst_ref=dst.at[i],
            send_sem=send.at[i],
            recv_sem=recv.at[i],
            device_id=near_id(far, 1 - side),
        )

    def z_copy(i, d, src, dst, send, recv):
        return pltpu.make_async_remote_copy(
            src_ref=src.at[i, far_id(d)],
            dst_ref=dst.at[d - 1, i],
            send_sem=send.at[d - 1, i],
            recv_sem=recv.at[d - 1, i],
            device_id=near_id(far_id(d), side),
        )

    def last_copy(d):
        return pltpu.make_async_remote_copy(
            src_ref=q_last.at[far_id(d)],
            dst_ref=q_last_in.at[d - 1],
            send_sem=l_send.at[d - 1],
            recv_sem=l_recv.at[d - 1],
            device_id=near_id(far_id(d), side),
        )

    def last_cross():
        return pltpu.make_async_remote_copy(
            src_ref=q_last.at[far, 1],
            dst_ref=q_cross,
            send_sem=l_send.at[n_far - 1],
            recv_sem=l_recv.at[n_far - 1],
            device_id=near_id(far, 1 - side),
        )

    load_of["q"].wait()
    project_q(peer_half, q_out, 1)
    pl.semaphore_wait(barrier, n + n_tp - 2)
    for i in range(waves - 1):
        x_copy(i, q_out, q_in, qx_send, qx_recv).start()
    project_q(own_half, q_own, 0)
    for d in range(1, n_far):
        last_copy(d).start()
    load_of["k"].wait()
    load_of["v"].wait()
    project_kv(peer_half, kv_out)
    for i in range(waves):
        x_copy(i, kv_out, kv_in, kx_send, kx_recv).start()
    project_kv(own_half, kv_own)

    load_of["bias"].wait()
    load_of["parents"].wait()
    load_of["lengths"].wait()
    load_of["decay"].wait()
    par_pad[...] = jnp.zeros(par_pad.shape, jnp.int32)
    par_pad[0:seqs, 0:props] = parents[...]
    r_i = iota((LANES, LANES), 0)
    c_i = iota((LANES, LANES), 1)
    lane1 = iota((1, LANES), 1)
    eye = r_i == c_i
    for i in range(waves):
        row = jnp.full((1, LANES), -1, jnp.int32)
        for j in range(wave):
            of = par_pad[pl.ds(side * half_seqs + i * wave + j, 1), :]
            if j:
                of = pltpu.roll(jnp.broadcast_to(of, (8, LANES)), j * props, 1)[0:1]
            inside = (lane1 >= j * props) & (lane1 < (j + 1) * props)
            row = jnp.where(inside, of + j * props, row)
        link = ((row == r_i) | eye).astype(F32).astype(BF16)
        for _ in range(props.bit_length()):
            link = jnp.minimum(dot(link, link), 1.0).astype(BF16)
        link_s[i] = link
        anc_s[i] = dot_nt(eye.astype(F32).astype(BF16), link)
    w_row = lax.rem(iota(widen.shape, 0), LANES)
    w_col = iota(widen.shape, 1)
    w_src = lax.div(w_col, cols) * 8 + lax.div(lax.rem(w_col, cols), head_dim)
    widen[...] = (w_row == w_src).astype(F32).astype(BF16)
    b_shape = (8, bias.shape[1])
    b_row, b_col = iota(b_shape, 0), iota(b_shape, 1)
    mine = (b_row < own_heads) & (b_col == tp * heads + far * own_heads + b_row)
    bias_col = jnp.sum(jnp.where(mine, jnp.broadcast_to(bias[...], b_shape), 0.0), axis=1, keepdims=True)

    for i in range(waves - 1):
        x_copy(i, q_out, q_in, qx_send, qx_recv).wait_recv()
        q_own[i] = q_own[i] + q_in[i]
        for d in range(1, n_far):
            z_copy(i, d, q_own, q_far, qz_send, qz_recv).start()
    for d in range(1, n_far):
        last_copy(d).wait_recv()
    q_last[far] = q_last[far] + functools.reduce(jnp.add, [q_last_in[d] for d in range(n_far - 1)])
    last_cross().start()

    targets = [(d, 0) for d in range(1, n_far)] + [(d, 1) for d in range(n_far)]

    def target_id(d, cross):
        return near_id(far_id(d), side if not cross else 1 - side)

    def spread_copy(i, t, buf, send, recv):
        d, cross = targets[t]
        block = side * waves + i
        return pltpu.make_async_remote_copy(
            src_ref=buf.at[block, far],
            dst_ref=buf.at[block, far],
            send_sem=send.at[t, i],
            recv_sem=recv.at[block, far],
            device_id=target_id(d, cross),
        )

    def relay_copy(i, buf, send, recv):
        block = side * waves + i
        return pltpu.make_async_remote_copy(
            src_ref=buf.at[block],
            dst_ref=buf.at[block],
            send_sem=send.at[i],
            recv_sem=recv.at[i],
            device_id=near_id(far, 1 - side),
        )

    def spread(i, direct, buf, send, recv):
        for t in range(sources if direct else n_far - 1):
            spread_copy(i, t, buf, send, recv).start()

    def sent(i, direct, buf, send, recv, r_send, r_recv):
        for t in range(sources if direct else n_far - 1):
            spread_copy(i, t, buf, send, recv).wait_send()
        if not direct:
            relay_copy(i, buf, r_send, r_recv).wait_send()

    def spread_wait(i, t, buf, send, recv):
        d, cross = targets[t]
        block = (1 - side if cross else side) * waves + i
        pltpu.make_async_remote_copy(
            src_ref=buf.at[block, far_id(d)],
            dst_ref=buf.at[block, far_id(d)],
            send_sem=send.at[t, i],
            recv_sem=recv.at[block, far_id(d)],
            device_id=target_id(d, cross),
        ).wait_recv()

    def pass_on(i, direct, buf, send, recv, r_send, r_recv):
        for t in range(n_far - 1):
            spread_wait(i, t, buf, send, recv)
        if not direct:
            relay_copy(i, buf, r_send, r_recv).start()

    def crossed(i, direct, buf, send, recv, r_send, r_recv):
        if not direct:
            relay_copy(i, buf, r_send, r_recv).wait_recv()
            return
        for t in range(n_far - 1, sources):
            spread_wait(i, t, buf, send, recv)

    q_route = (qbuf, b_send, b_recv, qr_send, qr_recv)
    a_route = (att, d_send, d_recv, ar_send, ar_recv)
    q_direct = [False] * waves
    a_direct = [i > 0 for i in range(waves)]

    lane8 = iota((8, LANES), 1)
    row8 = iota((8, LANES), 0)

    def owner_q(i):
        if i < waves - 1:
            total = q_own[i, far]
            for d in range(1, n_far):
                z_copy(i, d, q_own, q_far, qz_send, qz_recv).wait_recv()
                total = total + q_far[d - 1, i]
        else:
            last_cross().wait_recv()
            total = q_last[far, 0] + q_cross[...]
        tail = total[wrows:]
        inverse = lax.rsqrt(tail / (depth * n) + 1e-06)
        column = tile_rows(inverse, LANES).T[:wrows, own_heads : own_heads + 1]
        inv_s[i] = jnp.broadcast_to(column, (wrows, cols))
        qbuf[side * waves + i, far] = (inv_s[i] * total[:wrows]).astype(BF16)
        spread(i, q_direct[i], qbuf, b_send, b_recv)
        inverse_row = jnp.broadcast_to(inverse[own_heads : own_heads + 1], (8, LANES))
        x = inverse_row * tail + bias_col
        log_gate = jnp.minimum(x, 0.0) - jnp.log1p(jnp.exp(-jnp.abs(x)))
        log_gate = jnp.where((row8 < own_heads) & (lane8 < wrows), log_gate, 0.0)
        parts = dot(jnp.concatenate(split3(log_gate), axis=0), link_s[i])
        path_s[i] = parts[:8] + parts[8:16] + parts[16:24]

    for i in range(waves):
        owner_q(i)

    strides = [1 << b for b in range(n_far.bit_length() - 1)]

    def halve_copy(i, st, m):
        slot = sum(n_far // (2 * x) for x in strides if x < st) + m
        partner = far + st - 2 * st * lax.rem(lax.div(far, st), 2)
        return pltpu.make_async_remote_copy(
            src_ref=kv_pass.at[i, lax.rem(partner, 2 * st) + 2 * st * m],
            dst_ref=kv_far.at[slot, i],
            send_sem=kz_send.at[slot, i],
            recv_sem=kz_recv.at[slot, i],
            device_id=near_id(partner, side),
        )

    def halve_start(i, st):
        partner = far + st - 2 * st * lax.rem(lax.div(far, st), 2)
        for m in range(n_far // (2 * st)):
            f = lax.rem(partner, 2 * st) + 2 * st * m
            kv_pass[i, f] = kv_own[i, f].astype(BF16)
            halve_copy(i, st, m).start()

    def halve_wait(i, st):
        for m in range(n_far // (2 * st)):
            halve_copy(i, st, m).wait_recv()
            f = lax.rem(far, 2 * st) + 2 * st * m
            slot = sum(n_far // (2 * x) for x in strides if x < st) + m
            kv_own[i, f] = kv_own[i, f] + kv_far[slot, i].astype(F32)

    def pass_kv(i, step):
        if step:
            halve_wait(i, strides[step - 1])
        else:
            x_copy(i, kv_out, kv_in, kx_send, kx_recv).wait_recv()
            kv_own[i] = kv_own[i] + kv_in[i].astype(F32)
        if step < len(strides):
            halve_start(i, strides[step])

    group = min(heads, 256 // head_dim)
    gwidth = group * head_dim
    g_head = iota((group, props, gwidth), 0)
    g_col = lax.div(iota((group, props, gwidth), 2), head_dim)
    g_diag = (g_head == g_col).reshape(group * props, gwidth)
    lane_w = iota((wrows, LANES), 1)
    position = iota((heads, pos_dev), 1) + me * pos_dev

    def mix_copy(i, t, which, src, dst):
        d, cross = targets[t]
        block = (1 - side if cross else side) * waves + i
        return pltpu.make_async_remote_copy(
            src_ref=src.at[block, far_id(d)],
            dst_ref=dst.at[t, i],
            send_sem=c_send.at[which, t, i],
            recv_sem=c_recv.at[which, t, i],
            device_id=target_id(d, cross),
        )

    def attend(i, cross):
        place = 1 - side if cross else side
        block = place * waves + i
        if cross:
            crossed(i, q_direct[i], *q_route)
        first = place * half_seqs + i * wave
        for j in range(wave):
            s = first + j
            pltpu.make_async_copy(keys_hbm.at[s], keys.at[s], cache_sem.at[0, s]).wait()
            pltpu.make_async_copy(values_hbm.at[s], values.at[s], cache_sem.at[1, s]).wait()
        q_wave = jnp.concatenate([qbuf[block, f] for f in range(n_far)], axis=1).astype(F32)
        if exact_scale:
            q_wave = q_wave * scale
        chains = [(j, g) for j in range(wave) for g in range(heads // group)]
        scores_of, w_of, tops, totals, parts = {}, {}, {}, {}, {}
        for j in range(wave):
            s = first + j
            fade = jnp.where(position < lengths[s], decay[s], LOW)
            for g in range(heads // group):
                q = q_wave[j * props : (j + 1) * props, g * gwidth : (g + 1) * gwidth]
                q = jnp.broadcast_to(q[None], (group, props, gwidth)).reshape(group * props, gwidth)
                q = jnp.where(g_diag, q, 0.0).astype(BF16)
                scores = dot_nt(q, keys[s, :, g * gwidth : (g + 1) * gwidth])
                if not exact_scale:
                    scores = scores * scale
                fades = [
                    jnp.broadcast_to(fade[h : h + 1], (props, pos_dev))
                    for h in range(g * group, (g + 1) * group)
                ]
                scores_of[j, g] = scores + jnp.concatenate(fades, axis=0)
        for j, g in chains:
            top = jnp.max(scores_of[j, g], axis=1, keepdims=True)
            w = jnp.exp(scores_of[j, g] - top)
            total = jnp.sum(w, axis=1, keepdims=True)
            w_of[j, g] = w.astype(BF16)
            for h in range(group):
                tops[j, g * group + h] = top[h * props : (h + 1) * props]
                totals[j, g * group + h] = total[h * props : (h + 1) * props]
        for j, g in chains:
            m = dot(w_of[j, g], values[first + j, :, g * gwidth : (g + 1) * gwidth])
            m = jnp.where(g_diag, m, 0.0).reshape(group, props, gwidth)
            parts[j, g] = jnp.sum(m, axis=0)
        mixes = [
            jnp.concatenate([parts[j, g] for g in range(heads // group)], axis=1) for j in range(wave)
        ]
        mixed = jnp.concatenate(mixes, axis=0).astype(BF16)
        for f in range(n_far):
            mix[block, f] = mixed[:, f * cols : (f + 1) * cols]
        acc = jnp.zeros((wrows, LANES), F32)
        for h in range(heads):
            f, k = divmod(h, own_heads)
            for at, cols_of in ((k, tops), (own_heads + k, totals)):
                col = jnp.concatenate([cols_of[j, h] for j in range(wave)], axis=0)
                acc = jnp.where(lane_w == f * 8 + at, col, acc)
        flat = tile_rows(acc, LANES).T
        for f in range(n_far):
            stat[block, f] = flat[f * 8 : f * 8 + stat.shape[2]]
        for t in range(sources):
            if targets[t][1] == cross:
                mix_copy(i, t, 0, mix, mix_in).start()
                mix_copy(i, t, 1, stat, stat_in).start()

    own_head_of = lax.div(iota((wrows, cols), 1), head_dim)

    def tree(i):
        block = side * waves + i
        pass_kv(i, len(strides))
        total = kv_own[i, far]
        new_k = tile_rows(inv_s[i] * total[:wrows], LANES).astype(BF16)
        new_v = tile_rows(inv_s[i] * total[wrows:], LANES).astype(BF16)
        q = qbuf[block, far].astype(F32)
        q = jnp.concatenate([jnp.where(own_head_of == h, q, 0.0) for h in range(own_heads)], axis=0)
        scores = dot_nt(q.astype(BF16), new_k) * scale
        path = path_s[i]
        path_cols = tile_rows(path, LANES).T[:wrows]
        shifts = [path_cols[:, h : h + 1] - path[h : h + 1] for h in range(own_heads)]
        scores = scores + jnp.concatenate(shifts, axis=0)
        live = jnp.concatenate([anc_s[i, :wrows]] * own_heads, axis=0) > 0.5
        scores = jnp.where(live, scores, LOW)
        top = jnp.max(scores, axis=1, keepdims=True)
        w = jnp.where(live, jnp.exp(scores - top), 0.0)
        total = jnp.sum(w, axis=1, keepdims=True)
        m = dot(w.astype(BF16), new_v)
        merged = jnp.zeros((wrows, cols), F32)
        acc = jnp.zeros((wrows, LANES), F32)
        for h in range(own_heads):
            part = slice(h * wrows, (h + 1) * wrows)
            merged = jnp.where(own_head_of == h, m[part], merged)
            acc = jnp.where(lane_w == h, top[part], acc)
            acc = jnp.where(lane_w == own_heads + h, total[part], acc)
        tmix[i] = merged
        tstat[i] = tile_rows(acc, LANES).T[:8]

    def merge(i):
        block = side * waves + i
        for t in range(sources):
            mix_copy(i, t, 0, mix, mix_in).wait_recv()
            mix_copy(i, t, 1, stat, stat_in).wait_recv()
        stats = [stat[block, far]] + [stat_in[t, i] for t in range(sources)]
        stats = [tile_rows(st, 8) for st in stats]
        path = path_s[i]
        tops = [st + path for st in stats] + [tstat[i]]
        totals = [pltpu.roll(st, 8 - own_heads, 0) for st in stats + [tstat[i]]]
        best = functools.reduce(jnp.maximum, tops)
        factors = [jnp.exp(top - best) for top in tops]
        denom = functools.reduce(jnp.add, [f * t for f, t in zip(factors, totals)])
        factors = [jnp.where(row8 < own_heads, f / denom, 0.0) for f in factors]
        turned = tile_rows(jnp.concatenate(factors, axis=0), LANES).T[:wrows]
        high = turned.astype(BF16)
        low = (turned - high.astype(F32)).astype(BF16)
        wide = dot(jnp.concatenate([high, low], axis=1), widen[...])
        mixes = [mix[block, far]] + [mix_in[t, i] for t in range(sources)] + [tmix[i]]
        numer = jnp.zeros((wrows, cols), F32)
        for k, m in enumerate(mixes):
            numer = numer + wide[:, k * cols : (k + 1) * cols] * m.astype(F32)
        att[block, far] = numer.astype(BF16)
        spread(i, a_direct[i], att, d_send, d_recv)

    per_tp = seqs // n_tp

    def e_copy(s, t):
        k = jnp.maximum(lax.rem(tp - t + n_tp, n_tp) - 1, 0)
        return pltpu.make_async_remote_copy(
            src_ref=terms.at[s],
            dst_ref=terms_in.at[k, lax.rem(s, per_tp)],
            send_sem=e_send.at[s],
            recv_sem=e_recv.at[k, lax.rem(s, per_tp)],
            device_id={"tp": t},
        )

    def output(i, cross):
        place = 1 - side if cross else side
        block = place * waves + i
        if cross:
            crossed(i, a_direct[i], *a_route)
        attended = jnp.concatenate([att[block, f] for f in range(n_far)], axis=1)
        term = dot(attended, out_w[...])
        for j in range(wave):
            s = place * half_seqs + i * wave + j
            terms[s] = fold(term[j * props : (j + 1) * props]).astype(BF16)
            t = lax.div(s, per_tp)
            pl.when(tp != t)(e_copy(s, t).start)

    for i in range(waves):
        pass_kv(i, 0)
    pass_on(0, q_direct[0], *q_route)
    attend(0, 0)
    for i in range(waves):
        if i + 1 < waves:
            pass_on(i + 1, q_direct[i + 1], *q_route)
            attend(i + 1, 0)
        for step in range(1, len(strides)):
            if 0 <= i - step + 1:
                pass_kv(i - step + 1, step)
        attend(i, 1)
    for step in range(1, len(strides)):
        for i in range(max(waves - step + 1, 0), waves):
            pass_kv(i, step)
    load_of["out"].wait()
    for i in range(waves):
        tree(i)
        if i >= 2:
            pass_on(i - 2, a_direct[i - 2], *a_route)
        merge(i)
    if waves >= 2:
        pass_on(waves - 2, a_direct[waves - 2], *a_route)
    for i in range(waves):
        if i == waves - 1:
            pass_on(i, a_direct[i], *a_route)
        output(i, 0)
        output(i, 1)

    done = []
    for j in range(per_tp):
        total = unfold(terms[tp * per_tp + j])
        for k in range(1, n_tp):
            pltpu.make_async_remote_copy(
                src_ref=terms.at[0],
                dst_ref=terms_in.at[k - 1, j],
                send_sem=e_send.at[0],
                recv_sem=e_recv.at[k - 1, j],
                device_id={"tp": lax.rem(tp + k, n_tp)},
            ).wait_recv()
            total = total + unfold(terms_in[k - 1, j])
        done.append(total)
    out[...] = jnp.concatenate(done, axis=0).astype(BF16)

    for i in range(waves):
        if i < waves - 1:
            x_copy(i, q_out, q_in, qx_send, qx_recv).wait_send()
            for d in range(1, n_far):
                z_copy(i, d, q_own, q_far, qz_send, qz_recv).wait_send()
        x_copy(i, kv_out, kv_in, kx_send, kx_recv).wait_send()
        for st in strides:
            for m in range(n_far // (2 * st)):
                halve_copy(i, st, m).wait_send()
        sent(i, q_direct[i], *q_route)
        sent(i, a_direct[i], *a_route)
        for t in range(sources):
            mix_copy(i, t, 0, mix, mix_in).wait_send()
            mix_copy(i, t, 1, stat, stat_in).wait_send()
    for d in range(1, n_far):
        last_copy(d).wait_send()
    last_cross().wait_send()
    for s in range(seqs):
        t = s // per_tp
        pl.when(tp != t)(e_copy(s, t).wait_send)


def wave_size(n, n_tp, seqs, props, heads, width):
    n_far = n // 2
    if n < 4 or n & (n - 1) or seqs % 2 or seqs % n_tp or heads % n_far or width % (n_far * LANES):
        return 0
    head_dim = width // heads
    own = heads // n_far
    if own > 4 or 8 * (n + 1) > LANES or (heads % min(heads, max(256 // head_dim, 1))):
        return 0
    for wave in range(1, seqs // 2 + 1):
        fits = wave * props % 16 == 0 and wave * props <= LANES
        if seqs // 2 % wave == 0 and fits and props % 8 == 0:
            return wave
    return 0


def solution(mesh):
    n, n_tp = mesh.shape["kv"], mesh.shape["tp"]

    def body(
        tokens,
        norm_gain,
        query_weight,
        key_weight,
        value_weight,
        gate_weight,
        gate_bias,
        out_weight,
        cache_keys,
        cache_values,
        cache_decay,
        lengths,
        parents,
    ):
        rows, depth = tokens.shape
        seqs, props = parents.shape
        heads = cache_decay.shape[1]
        pos_dev = cache_keys.shape[1]
        width = query_weight.shape[1]
        cols = out_weight.shape[1]
        slots = -(-seqs // n)
        block = rows // n_tp
        all_w = 2 * width + LANES
        folded = (2 * props, width // 2)
        vmem = pl.BlockSpec(memory_space=pltpu.VMEM)
        hbm = pl.BlockSpec(memory_space=pltpu.HBM)
        dma = pltpu.SemaphoreType.DMA
        wave = wave_size(n, n_tp, seqs, props, heads, width)
        if wave:
            n_far = n // 2
            waves = seqs // 2 // wave
            q_waves = max(waves - 1, 1)
            wrows = wave * props
            wcols = width // n_far
            per_tp = seqs // n_tp
            s_rows = max(4, 2 * (heads // n_far))
            block_q = (n_far, wrows + 8, wcols)
            block_kv = (n_far, 2 * wrows, wcols)
            body_of = functools.partial(by_heads, n, n_tp, wave)
            scratch = [
                pltpu.VMEM(tokens.shape, BF16),
                pltpu.VMEM((1, depth), F32),
                pltpu.VMEM(query_weight.shape, BF16),
                pltpu.VMEM(key_weight.shape, BF16),
                pltpu.VMEM(value_weight.shape, BF16),
                pltpu.VMEM((gate_weight.shape[1], depth), BF16),
                pltpu.VMEM((1, gate_bias.shape[0]), F32),
                pltpu.VMEM(cache_decay.shape, F32),
                pltpu.SMEM(lengths.shape, jnp.int32),
                pltpu.VMEM(parents.shape, jnp.int32),
                pltpu.VMEM(out_weight.shape, BF16),
                pltpu.VMEM(cache_keys.shape, BF16),
                pltpu.VMEM(cache_values.shape, BF16),
                pltpu.VMEM((rows, 3 * depth), BF16),
                pltpu.VMEM((q_waves,) + block_q, F32),
                pltpu.VMEM((q_waves,) + block_q, F32),
                pltpu.VMEM((q_waves,) + block_q, F32),
                pltpu.VMEM((n_far - 1, q_waves) + block_q[1:], F32),
                pltpu.VMEM((n_far, 2) + block_q[1:], F32),
                pltpu.VMEM((n_far - 1, 2) + block_q[1:], F32),
                pltpu.VMEM(block_q[1:], F32),
                pltpu.VMEM((waves,) + block_kv, BF16),
                pltpu.VMEM((waves,) + block_kv, BF16),
                pltpu.VMEM((waves,) + block_kv, F32),
                pltpu.VMEM((waves,) + block_kv, BF16),
                pltpu.VMEM((n_far - 1, waves) + block_kv[1:], BF16),
                pltpu.VMEM((2 * waves, n_far, wrows, wcols), BF16),
                pltpu.VMEM((2 * waves, n_far, wrows, wcols), BF16),
                pltpu.VMEM((n - 1, waves, wrows, wcols), BF16),
                pltpu.VMEM((2 * waves, n_far, s_rows, LANES), F32),
                pltpu.VMEM((n - 1, waves, s_rows, LANES), F32),
                pltpu.VMEM((2 * waves, n_far, wrows, wcols), BF16),
                pltpu.VMEM((seqs,) + folded, BF16),
                pltpu.VMEM((n_tp - 1, per_tp) + folded, BF16),
                pltpu.VMEM((-(-seqs // 8) * 8, LANES), jnp.int32),
                pltpu.VMEM((waves, LANES, LANES), BF16),
                pltpu.VMEM((waves, LANES, LANES), F32),
                pltpu.VMEM((waves, 8, LANES), F32),
                pltpu.VMEM((waves, wrows, wcols), F32),
                pltpu.VMEM((waves, wrows, wcols), F32),
                pltpu.VMEM((waves, 8, LANES), F32),
                pltpu.VMEM((2 * LANES, (n + 1) * wcols), BF16),
                dma((11,)),
                dma((2, seqs)),
                dma((waves,)),
                dma((waves,)),
                dma((waves,)),
                dma((waves,)),
                dma((n_far - 1, waves)),
                dma((n_far - 1, waves)),
                dma((n_far - 1, waves)),
                dma((n_far - 1, waves)),
                dma((n - 1, waves)),
                dma((2 * waves, n_far)),
                dma((2, n - 1, waves)),
                dma((2, n - 1, waves)),
                dma((n - 1, waves)),
                dma((2 * waves, n_far)),
                dma((seqs,)),
                dma((n_tp - 1, per_tp)),
                dma((waves,)),
                dma((waves,)),
                dma((waves,)),
                dma((waves,)),
                dma((n_far,)),
                dma((n_far,)),
            ]
        else:
            body_of = functools.partial(by_sequence, n, n_tp)
            scratch = [
                pltpu.VMEM(tokens.shape, BF16),
                pltpu.VMEM((1, depth), F32),
                pltpu.VMEM(query_weight.shape, BF16),
                pltpu.VMEM(key_weight.shape, BF16),
                pltpu.VMEM(value_weight.shape, BF16),
                pltpu.VMEM((1, gate_bias.shape[0]), F32),
                pltpu.VMEM(cache_decay.shape, F32),
                pltpu.SMEM(lengths.shape, jnp.int32),
                pltpu.VMEM(parents.shape, jnp.int32),
                dma((9,)),
                pltpu.VMEM((seqs, props, all_w), F32),
                pltpu.VMEM((seqs,) + folded, BF16),
                pltpu.VMEM((seqs, props, all_w), F32),
                pltpu.VMEM((seqs,) + folded, BF16),
                pltpu.VMEM((n // 2 - 1, slots, props, all_w), F32),
                pltpu.VMEM((n // 2 - 1, slots) + folded, BF16),
                pltpu.VMEM((gate_weight.shape[1], depth), BF16),
                pltpu.VMEM(out_weight.shape, BF16),
                pltpu.VMEM(cache_keys.shape, BF16),
                pltpu.VMEM(cache_values.shape, BF16),
                pltpu.VMEM((seqs,) + folded, BF16),
                pltpu.VMEM((seqs,) + folded, BF16),
                pltpu.VMEM((seqs, props, LANES), F32),
                pltpu.VMEM((n - 1, slots) + folded, BF16),
                pltpu.VMEM((n - 1, slots, props, LANES), F32),
                pltpu.VMEM((seqs,) + folded, BF16),
                pltpu.VMEM((slots, props, LANES), F32),
                pltpu.VMEM((slots, props, LANES), F32),
                pltpu.VMEM((slots, props, width), F32),
                pltpu.VMEM((slots, 2, props, LANES), F32),
                pltpu.VMEM((slots, 2, LANES, width), F32),
                pltpu.VMEM((n_tp, block, cols), BF16),
                pltpu.VMEM((n_tp - 1, block, cols), BF16),
                pltpu.VMEM((-(-seqs // 8) * 8, LANES), jnp.int32),
                dma((2,)),
                dma((2, seqs)),
                dma((2, seqs)),
                dma((2, seqs)),
                dma((2, seqs)),
                dma((2, n // 2 - 1, slots)),
                dma((slots, n - 1)),
                dma((seqs,)),
                dma((2, seqs)),
                dma((2, n - 1, slots)),
                dma((slots, n - 1)),
                dma((seqs,)),
                dma((n_tp,)),
                dma((n_tp - 1,)),
            ]
        return pl.pallas_call(
            body_of,
            out_shape=pltpu.VMEM((block, cols), BF16),
            in_specs=[hbm] * 13,
            out_specs=vmem,
            scratch_shapes=scratch,
            compiler_params=pltpu.CompilerParams(
                collective_id=0, has_side_effects=True, vmem_limit_bytes=67_043_328 - 131072
            ),
        )(
            tokens,
            norm_gain.reshape(1, depth),
            query_weight,
            key_weight,
            value_weight,
            gate_weight.T,
            gate_bias.reshape(1, gate_bias.shape[0]),
            out_weight,
            cache_keys,
            cache_values,
            cache_decay,
            lengths,
            parents,
        )

    in_specs = (
        P(None, "kv"),
        P("kv"),
        P("kv", "tp"),
        P("kv", "tp"),
        P("kv", "tp"),
        P(),
        P(),
        P("tp", "kv"),
        P(None, "kv", "tp"),
        P(None, "kv", "tp"),
        P(None, "tp", "kv"),
        P(),
        P(),
    )
    out_specs = P("tp", "kv")
    return jax.shard_map(body, mesh=mesh, in_specs=in_specs, out_specs=out_specs, check_vma=False)
```

```python
import functools
import math

import jax
import jax.numpy as jnp
from jax import lax
from jax.experimental import pallas as pl
from jax.experimental.pallas import tpu as pltpu
from jax.sharding import PartitionSpec as P

F32 = jnp.float32
BF16 = jnp.bfloat16
LANES = 128
LOW = -1e30
NT = (((1,), (1,)), ((), ()))
HIGH = lax.Precision.HIGHEST


def dot(a, b, precision=None):
    return jnp.dot(a, b, preferred_element_type=F32, precision=precision)


def dot_nt(a, b, precision=None):
    return lax.dot_general(a, b, NT, preferred_element_type=F32, precision=precision)


def fold(x):
    half = x.shape[1] // 2
    return jnp.concatenate([x[:, :half], x[:, half:]], axis=0)


def unfold(x):
    rows = x.shape[0] // 2
    x = x.astype(F32)
    return jnp.concatenate([x[:rows], x[rows:]], axis=1)


def by_sequence(
    n,
    n_tp,
    tokens_hbm,
    gain_hbm,
    query_hbm,
    key_hbm,
    value_hbm,
    gate_hbm,
    bias_hbm,
    out_hbm,
    keys_hbm,
    values_hbm,
    decay_hbm,
    lengths_hbm,
    parents_hbm,
    out,
    tokens,
    gain,
    query_w,
    key_w,
    value_w,
    bias,
    decay,
    lengths,
    parents,
    small_sem,
    part,
    part_v,
    pair_in,
    pair_in_v,
    part_in,
    part_in_v,
    gate_w,
    out_w,
    keys,
    values,
    qbuf,
    mix,
    stat,
    mix_in,
    stat_in,
    att,
    anc,
    path_s,
    tmix,
    tstat,
    kvnew,
    terms,
    terms_in,
    par_pad,
    load_sem,
    cache_sem,
    p_send,
    p_recv,
    a_send,
    a_recv,
    b_send,
    b_recv,
    c_send,
    c_recv,
    d_send,
    d_recv,
    e_send,
    e_recv,
):
    me = lax.axis_index("kv")
    tp = lax.axis_index("tp")
    rows, depth = tokens.shape
    seqs, props = parents.shape
    heads = decay.shape[1]
    pos_dev = keys.shape[1]
    width = query_w.shape[1]
    head_dim = width // heads
    scale = head_dim ** (-0.5)
    slots = part_in.shape[1]
    parity = lax.rem(tp, 2)
    left_over = seqs % n
    hp = heads * props

    barrier = pltpu.get_barrier_semaphore()
    for k in range(1, n):
        pl.semaphore_signal(barrier, inc=1, device_id={"kv": lax.rem(me + k, n)})
    for k in range(1, n_tp):
        pl.semaphore_signal(barrier, inc=1, device_id={"tp": lax.rem(tp + k, n_tp)})

    pairs = (
        (tokens_hbm, tokens),
        (gain_hbm, gain),
        (query_hbm, query_w),
        (key_hbm, key_w),
        (value_hbm, value_w),
        (bias_hbm, bias),
        (parents_hbm, parents),
        (decay_hbm, decay),
        (lengths_hbm, lengths),
    )
    small_loads = [
        pltpu.make_async_copy(src, dst, small_sem.at[i]) for i, (src, dst) in enumerate(pairs)
    ]
    for load in small_loads:
        load.start()
    gate_load = pltpu.make_async_copy(
        gate_hbm.at[:, pl.ds(pl.multiple_of(me * depth, depth), depth)], gate_w, load_sem.at[0]
    )
    gate_load.start()
    cache_loads = []
    for s in range(seqs):
        k_load = pltpu.make_async_copy(keys_hbm.at[s], keys.at[s], cache_sem.at[0, s])
        v_load = pltpu.make_async_copy(values_hbm.at[s], values.at[s], cache_sem.at[1, s])
        k_load.start()
        v_load.start()
        cache_loads.append((k_load, v_load))
    out_load = pltpu.make_async_copy(out_hbm, out_w, load_sem.at[1])
    out_load.start()

    def owner_of(s):
        if isinstance(s, int):
            place = s % n
            shift = parity * left_over if s // n == seqs // n else 0
        else:
            place = lax.rem(s, n)
            shift = jnp.where(lax.div(s, n) == seqs // n, parity * left_over, 0)
        return lax.rem(place + shift, n)

    def slot_seq(r):
        shift = parity * left_over if r == seqs // n else 0
        return r * n + lax.rem(me + 2 * n - shift, n)

    def for_slot(r, f):
        if (r + 1) * n <= seqs:
            f()
        else:
            pl.when(slot_seq(r) < seqs)(f)

    for load in small_loads:
        load.wait()
    xf = tokens[...].astype(F32)
    squares = jnp.sum(xf * xf, axis=1, keepdims=True)
    normed = (xf * gain[...]).astype(BF16)
    sel_rows = lax.broadcasted_iota(jnp.int32, (bias.shape[1], LANES), 0)
    sel_cols = lax.broadcasted_iota(jnp.int32, (bias.shape[1], LANES), 1)
    select = ((sel_rows == sel_cols + tp * heads) & (sel_cols < heads)).astype(F32)
    for i, w in enumerate((query_w, key_w)):
        part[:, :, i * width : (i + 1) * width] = dot(normed, w[...]).reshape(seqs, props, width)
    value_part = dot(normed, value_w[...])
    for s in range(seqs):
        part_v[s] = fold(value_part[s * props : (s + 1) * props]).astype(BF16)
    gate_load.wait()
    gates_w = lax.dot_general(
        select.astype(BF16), gate_w[...], (((0,), (0,)), ((), ())), preferred_element_type=F32
    )
    gate_part = dot_nt(normed, gates_w.astype(BF16))
    lane = lax.broadcasted_iota(jnp.int32, (rows, LANES), 1)
    gate_part = jnp.where(lane == LANES // 2, squares, gate_part)
    part[:, :, 2 * width :] = gate_part.reshape(seqs, props, LANES)
    pl.semaphore_wait(barrier, n + n_tp - 2)

    side = lax.rem(me, 2)
    partner = me + 1 - 2 * side
    n_far = n // 2
    shares = ((part, pair_in, part_in), (part_v, pair_in_v, part_in_v))

    def p_copy(s, which):
        src, dst, _ = shares[which]
        return pltpu.make_async_remote_copy(
            src_ref=src.at[s],
            dst_ref=dst.at[s],
            send_sem=p_send.at[which, s],
            recv_sem=p_recv.at[which, s],
            device_id={"kv": partner},
        )

    def a_copy(s, which):
        src, _, dst = shares[which]
        d = owner_of(s)
        k = jnp.maximum(lax.rem(lax.div(me, 2) - lax.div(d, 2) + n_far, n_far) - 1, 0)
        return pltpu.make_async_remote_copy(
            src_ref=src.at[s],
            dst_ref=dst.at[k, s // n],
            send_sem=a_send.at[which, s],
            recv_sem=a_recv.at[which, k, s // n],
            device_id={"kv": d},
        )

    def crosses(s):
        return lax.rem(owner_of(s), 2) != side

    def passes(s):
        d = owner_of(s)
        return (lax.rem(d, 2) == side) & (d != me)

    for s in range(seqs):
        for which in range(2):
            pl.when(crosses(s))(p_copy(s, which).start)

    par_pad[...] = jnp.zeros(par_pad.shape, jnp.int32)
    par_pad[0:seqs, 0:props] = parents[...]
    r_i = lax.broadcasted_iota(jnp.int32, (LANES, LANES), 0)
    c_i = lax.broadcasted_iota(jnp.int32, (LANES, LANES), 1)
    eye = (r_i == c_i).astype(F32)
    bias_row = dot(jnp.broadcast_to(bias[...], (8, bias.shape[1])), select, HIGH)[0:1]

    def ancestry(r):
        s = slot_seq(r)
        row = par_pad[pl.ds(s, 1), :]
        link = jnp.maximum((row == r_i).astype(F32), eye).astype(BF16)
        for _ in range(props.bit_length()):
            link = jnp.minimum(dot(link, link), 1.0).astype(BF16)
        anc[r] = dot_nt(eye.astype(BF16), link)[:props]

    for r in range(slots):
        for_slot(r, functools.partial(ancestry, r))

    def pass_on(s):
        for which in range(2):
            p_copy(s, which).wait_recv()
        part[s] = part[s] + pair_in[s]
        part_v[s] = (part_v[s].astype(F32) + pair_in_v[s].astype(F32)).astype(BF16)
        for which in range(2):
            a_copy(s, which).start()

    for s in range(seqs):
        pl.when(passes(s))(functools.partial(pass_on, s))

    lane_p = lax.broadcasted_iota(jnp.int32, (props, LANES), 1)
    bd_row = lax.broadcasted_iota(jnp.int32, (heads, props, width), 0)
    bd_col = lax.broadcasted_iota(jnp.int32, (heads, props, width), 2)
    diag = (lax.div(bd_col, head_dim) == bd_row).reshape(hp, width)

    def spread(q):
        wide = jnp.broadcast_to(q[None], (heads, props, width)).reshape(hp, width)
        return jnp.where(diag, wide, 0.0).astype(BF16)

    def gather_diag(m):
        return jnp.sum(jnp.where(diag, m, 0.0).reshape(heads, props, width), axis=0)

    def to_lanes(col, first):
        acc = jnp.zeros((props, LANES), F32)
        for h in range(heads):
            acc = jnp.where(lane_p == h + first, col[h * props : (h + 1) * props], acc)
        return acc

    def b_copy(r, k, buf, send, recv):
        s = slot_seq(r)
        return pltpu.make_async_remote_copy(
            src_ref=buf.at[s],
            dst_ref=buf.at[s],
            send_sem=send.at[r, k - 1],
            recv_sem=recv.at[s],
            device_id={"kv": lax.rem(me + k, n)},
        )

    pad_rows = LANES - props

    def project(r):
        s = slot_seq(r)
        for which, (src, near, far) in enumerate(shares):
            pltpu.make_async_remote_copy(
                src_ref=src.at[0],
                dst_ref=near.at[s],
                send_sem=p_send.at[which, 0],
                recv_sem=p_recv.at[which, s],
                device_id={"kv": partner},
            ).wait_recv()
            for k in range(1, n_far):
                pltpu.make_async_remote_copy(
                    src_ref=src.at[0],
                    dst_ref=far.at[k - 1, r],
                    send_sem=a_send.at[which, 0],
                    recv_sem=a_recv.at[which, k - 1, r],
                    device_id={"kv": lax.rem(me + 2 * k, n)},
                ).wait_recv()
        total = part[s] + pair_in[s]
        total_v = unfold(part_v[s]) + unfold(pair_in_v[s])
        for k in range(1, n_far):
            total = total + part_in[k - 1, r]
            total_v = total_v + unfold(part_in_v[k - 1, r])
        tail = total[:, 2 * width :]
        square = jnp.sum(jnp.where(lane_p == LANES // 2, tail, 0.0), axis=1, keepdims=True)
        inverse = lax.rsqrt(square / (depth * n) + 1e-06)
        q = inverse * total[:, :width]
        qbuf[s] = fold(q).astype(BF16)
        for k in range(1, n):
            b_copy(r, k, qbuf, b_send, b_recv).start()
        kvnew[r, 0, 0:props] = inverse * total[:, width : 2 * width]
        kvnew[r, 1, 0:props] = inverse * total_v
        kvnew[r, :, props:] = jnp.zeros((2, pad_rows, width), F32)
        x = inverse * tail + bias_row
        log_gate = jnp.minimum(x, 0.0) - jnp.log1p(jnp.exp(-jnp.abs(x)))
        padded = jnp.concatenate([log_gate, jnp.zeros((pad_rows, LANES), F32)], axis=0)
        path_s[r] = dot(anc[r], padded, HIGH)

    def tree(r):
        s = slot_seq(r)
        path = path_s[r]
        q = spread(unfold(qbuf[s]))
        head_of = lax.broadcasted_iota(jnp.int32, (heads, props, LANES), 0)
        lane_of = lax.broadcasted_iota(jnp.int32, (heads, props, LANES), 2)
        pick = (head_of == lane_of).reshape(hp, LANES)
        tiled = jnp.broadcast_to(path[None], (heads, props, LANES)).reshape(hp, LANES)
        own = jnp.sum(jnp.where(pick, tiled, 0.0), axis=1, keepdims=True)
        padded = jnp.concatenate([path, jnp.zeros((pad_rows, LANES), F32)], axis=0)
        other = dot_nt(pick.astype(F32), padded, HIGH)
        scores = dot_nt(q, kvnew[r, 0].astype(BF16)) * scale + own - other
        live = jnp.broadcast_to(anc[r][None], (heads, props, LANES)).reshape(hp, LANES) > 0.5
        scores = jnp.where(live, scores, LOW)
        top = jnp.max(scores, axis=1, keepdims=True)
        w = jnp.where(live, jnp.exp(scores - top), 0.0)
        total = jnp.sum(w, axis=1, keepdims=True)
        tmix[r] = gather_diag(dot(w.astype(BF16), kvnew[r, 1].astype(BF16)))
        tstat[r, 0] = to_lanes(top, 0)
        tstat[r, 1] = to_lanes(total, 0)

    position = lax.broadcasted_iota(jnp.int32, (hp, pos_dev), 1) + me * pos_dev

    def c_copy(s, which, src, dst):
        d = owner_of(s)
        k = jnp.maximum(lax.rem(me - d + n, n) - 1, 0)
        slot = s // n if isinstance(s, int) else lax.div(s, n)
        return d, pltpu.make_async_remote_copy(
            src_ref=src.at[s],
            dst_ref=dst.at[k, slot],
            send_sem=c_send.at[which, s],
            recv_sem=c_recv.at[which, k, slot],
            device_id={"kv": d},
        )

    def shard(s, carry):
        d = owner_of(s)

        @pl.when(d != me)
        def _():
            pltpu.make_async_remote_copy(
                src_ref=qbuf.at[s],
                dst_ref=qbuf.at[s],
                send_sem=b_send.at[0, 0],
                recv_sem=b_recv.at[s],
                device_id={"kv": d},
            ).wait_recv()

        pltpu.make_async_copy(keys_hbm.at[s], keys.at[s], cache_sem.at[0, s]).wait()
        pltpu.make_async_copy(values_hbm.at[s], values.at[s], cache_sem.at[1, s]).wait()
        q = spread(unfold(qbuf[s]))
        fade = decay[s]
        fade = jnp.concatenate(
            [jnp.broadcast_to(fade[h : h + 1], (props, pos_dev)) for h in range(heads)], axis=0
        )
        scores = dot_nt(q, keys[s]) * scale + fade
        live = position < lengths[s]
        scores = jnp.where(live, scores, LOW)
        top = jnp.max(scores, axis=1, keepdims=True)
        w = jnp.where(live, jnp.exp(scores - top), 0.0)
        total = jnp.sum(w, axis=1, keepdims=True)
        mix[s] = fold(gather_diag(dot(w.astype(BF16), values[s]))).astype(BF16)
        stat[s] = to_lanes(top, 0) + to_lanes(total, heads)
        for which, (src, dst) in enumerate(((mix, mix_in), (stat, stat_in))):
            _, copy = c_copy(s, which, src, dst)
            pl.when(d != me)(copy.start)
        return carry

    ex_r = lax.broadcasted_iota(jnp.int32, (LANES, width), 0)
    ex_c = lax.broadcasted_iota(jnp.int32, (LANES, width), 1)
    widen = (ex_r == lax.div(ex_c, head_dim)).astype(F32)

    def merge(r):
        s = slot_seq(r)
        for k in range(1, n):
            for which, (src, dst) in enumerate(((mix, mix_in), (stat, stat_in))):
                pltpu.make_async_remote_copy(
                    src_ref=src.at[0],
                    dst_ref=dst.at[k - 1, r],
                    send_sem=c_send.at[which, 0],
                    recv_sem=c_recv.at[which, k - 1, r],
                    device_id={"kv": lax.rem(me + k, n)},
                ).wait_recv()
        stats = jnp.concatenate([stat[s]] + [stat_in[k, r] for k in range(n - 1)], axis=0)
        totals = pltpu.roll(stats, LANES - heads, 1).reshape(n, props, LANES)
        tops = stats.reshape(n, props, LANES) + path_s[r][None]
        tops = jnp.where((lane_p < heads)[None], tops, LOW)
        ttop = jnp.where(lane_p < heads, tstat[r, 0], LOW)
        best = jnp.maximum(jnp.max(tops, axis=0), ttop)
        factors = jnp.exp(tops - best[None])
        tfactor = jnp.exp(ttop - best)
        denom = jnp.sum(factors * totals, axis=0) + tfactor * tstat[r, 1]
        packed = jnp.concatenate([factors.reshape(n * props, LANES), tfactor, denom], axis=0)
        wide = dot(packed, widen, HIGH)
        numer = wide[n * props : (n + 1) * props] * tmix[r] + wide[:props] * unfold(mix[s])
        for k in range(1, n):
            numer = numer + wide[k * props : (k + 1) * props] * unfold(mix_in[k - 1, r])
        att[s] = fold(numer / wide[(n + 1) * props :]).astype(BF16)
        for k in range(1, n):
            b_copy(r, k, att, d_send, d_recv).start()

    for r in range(slots):
        for_slot(r, functools.partial(project, r))
        if r > 0:
            for_slot(r - 1, functools.partial(merge, r - 1))
        for_slot(r, functools.partial(tree, r))
        lax.fori_loop(r * n, min((r + 1) * n, seqs), shard, 0)
    for_slot(slots - 1, functools.partial(merge, slots - 1))

    out_load.wait()
    block = rows // n_tp

    def e_copy(t):
        k = lax.rem(tp - t + n_tp, n_tp)
        return pltpu.make_async_remote_copy(
            src_ref=terms.at[t],
            dst_ref=terms_in.at[jnp.maximum(k - 1, 0)],
            send_sem=e_send.at[t],
            recv_sem=e_recv.at[jnp.maximum(k - 1, 0)],
            device_id={"tp": t},
        )

    arrived = 0
    for t in range(n_tp):
        first, last = t * block // props, ((t + 1) * block - 1) // props + 1
        for s in range(arrived, last):
            d = owner_of(s)

            @pl.when(d != me)
            def _(s=s, d=d):
                pltpu.make_async_remote_copy(
                    src_ref=att.at[s],
                    dst_ref=att.at[s],
                    send_sem=d_send.at[0, 0],
                    recv_sem=d_recv.at[s],
                    device_id={"kv": d},
                ).wait_recv()

        arrived = max(arrived, last)
        attended = jnp.concatenate([unfold(att[s]) for s in range(first, last)], axis=0)
        term = dot(attended.astype(BF16), out_w[...])
        begin = t * block - first * props
        terms[t] = term[begin : begin + block].astype(BF16)
        pl.when(tp != t)(e_copy(t).start)
    total = terms[tp].astype(F32)
    for k in range(1, n_tp):
        pltpu.make_async_remote_copy(
            src_ref=terms.at[0],
            dst_ref=terms_in.at[k - 1],
            send_sem=e_send.at[0],
            recv_sem=e_recv.at[k - 1],
            device_id={"tp": lax.rem(tp + k, n_tp)},
        ).wait_recv()
        total = total + terms_in[k - 1].astype(F32)
    out[...] = total.astype(BF16)

    for s in range(seqs):
        d = owner_of(s)
        for which in range(2):
            pl.when(crosses(s))(p_copy(s, which).wait_send)
            pl.when(passes(s))(a_copy(s, which).wait_send)
        for which, (src, dst) in enumerate(((mix, mix_in), (stat, stat_in))):
            _, copy = c_copy(s, which, src, dst)
            pl.when(d != me)(copy.wait_send)
    for r in range(slots):

        def drain(r=r):
            for k in range(1, n):
                b_copy(r, k, qbuf, b_send, b_recv).wait_send()
                b_copy(r, k, att, d_send, d_recv).wait_send()

        for_slot(r, drain)
    for t in range(n_tp):
        pl.when(tp != t)(e_copy(t).wait_send)


def split3(x):
    high = x.astype(BF16)
    rest = x - high.astype(F32)
    mid = rest.astype(BF16)
    low = (rest - mid.astype(F32)).astype(BF16)
    return high, mid, low


def tile_rows(rows, total):
    return jnp.concatenate([rows, jnp.zeros((total - rows.shape[0], rows.shape[1]), rows.dtype)], axis=0)


def by_heads(
    n,
    n_tp,
    wave,
    tokens_hbm,
    gain_hbm,
    query_hbm,
    key_hbm,
    value_hbm,
    gate_hbm,
    bias_hbm,
    out_hbm,
    keys_hbm,
    values_hbm,
    decay_hbm,
    lengths_hbm,
    parents_hbm,
    out,
    tokens,
    gain,
    query_w,
    key_w,
    value_w,
    gate_w,
    bias,
    decay,
    lengths,
    parents,
    out_w,
    keys,
    values,
    feats,
    q_out,
    q_in,
    q_own,
    q_far,
    q_last,
    q_last_in,
    q_cross,
    kv_out,
    kv_in,
    kv_own,
    kv_pass,
    kv_far,
    qbuf,
    mix,
    mix_in,
    stat,
    stat_in,
    att,
    terms,
    terms_in,
    par_pad,
    link_s,
    anc_s,
    path_s,
    inv_s,
    tmix,
    tstat,
    widen,
    load_sem,
    cache_sem,
    qx_send,
    qx_recv,
    kx_send,
    kx_recv,
    qz_send,
    qz_recv,
    kz_send,
    kz_recv,
    b_send,
    b_recv,
    c_send,
    c_recv,
    d_send,
    d_recv,
    e_send,
    e_recv,
    qr_send,
    qr_recv,
    ar_send,
    ar_recv,
    l_send,
    l_recv,
):
    me = lax.axis_index("kv")
    tp = lax.axis_index("tp")
    side = lax.rem(me, 2)
    far = lax.div(me, 2)
    n_far = n // 2
    rows, depth = tokens.shape
    seqs, props = parents.shape
    heads = decay.shape[1]
    pos_dev = keys.shape[1]
    width = query_w.shape[1]
    head_dim = width // heads
    scale = head_dim ** (-0.5)
    exact_scale = math.frexp(scale)[0] == 0.5
    own_heads = heads // n_far
    cols = width // n_far
    half_seqs = seqs // 2
    half = rows // 2
    waves = half_seqs // wave
    wrows = wave * props
    sources = n - 1

    pairs = (
        (tokens_hbm, tokens),
        (gain_hbm, gain),
        (gate_hbm.at[:, pl.ds(pl.multiple_of(me * depth, depth), depth)], gate_w),
        (query_hbm, query_w),
        (key_hbm, key_w),
        (value_hbm, value_w),
        (bias_hbm, bias),
        (parents_hbm, parents),
        (lengths_hbm, lengths),
        (decay_hbm, decay),
        (out_hbm, out_w),
    )
    loads = [pltpu.make_async_copy(src, dst, load_sem.at[i]) for i, (src, dst) in enumerate(pairs)]
    load_of = dict(
        zip(("tokens", "gain", "gate", "q", "k", "v", "bias", "parents", "lengths", "decay", "out"), loads)
    )
    for load in loads[:6]:
        load.start()
    barrier = pltpu.get_barrier_semaphore()
    for k in range(1, n):
        pl.semaphore_signal(barrier, inc=1, device_id={"kv": lax.rem(me + k, n)})
    for k in range(1, n_tp):
        pl.semaphore_signal(barrier, inc=1, device_id={"tp": lax.rem(tp + k, n_tp)})

    def iota(shape, dim):
        return lax.broadcasted_iota(jnp.int32, shape, dim)

    def far_id(d):
        return lax.rem(far + d, n_far)

    def near_id(z, x):
        return {"kv": z * 2 + x}

    own_half = pl.multiple_of(side * half, half)
    peer_half = pl.multiple_of((1 - side) * half, half)

    load_of["tokens"].wait()
    load_of["gain"].wait()
    for load in loads[6:]:
        load.start()
    for s in range(seqs):
        pltpu.make_async_copy(keys_hbm.at[s], keys.at[s], cache_sem.at[0, s]).start()
        pltpu.make_async_copy(values_hbm.at[s], values.at[s], cache_sem.at[1, s]).start()
    xf = tokens[...].astype(F32)
    feats[:, :depth] = (xf * gain[...]).astype(BF16)
    square = xf * xf
    high = square.astype(BF16)
    feats[:, depth : 2 * depth] = high
    feats[:, 2 * depth :] = (square - high.astype(F32)).astype(BF16)

    load_of["gate"].wait()
    t_rows = n_far * 8
    p_row = iota((t_rows, gate_w.shape[0]), 0)
    p_col = iota((t_rows, gate_w.shape[0]), 1)
    p_in = lax.rem(p_row, 8)
    wanted = (p_in < own_heads) & (p_col == tp * heads + lax.div(p_row, 8) * own_heads + p_in)
    gates = dot(wanted.astype(BF16), gate_w[...]).astype(BF16)
    ones = (lax.rem(iota((t_rows, depth), 0), 8) == own_heads).astype(BF16)
    tails = jnp.concatenate([gates, ones, ones], axis=1)

    def project_q(base, dst, which):
        full = dot(feats[pl.ds(base, half), :depth], query_w[...])
        for i in range(waves):
            piece = full[i * wrows : (i + 1) * wrows]
            tail = dot_nt(tails, feats[pl.ds(base + i * wrows, wrows), :])
            tail = jnp.concatenate([tail, jnp.zeros((t_rows, LANES - wrows), F32)], axis=1)
            for f in range(n_far):
                for at, rows_of in (
                    (slice(0, wrows), piece[:, f * cols : (f + 1) * cols]),
                    (slice(wrows, wrows + 8), tail[f * 8 : (f + 1) * 8]),
                ):
                    if i < waves - 1:
                        dst[i, f, at] = rows_of
                    else:
                        q_last[f, which, at] = rows_of

    def project_kv(base, dst):
        for which, w in enumerate((key_w, value_w)):
            full = dot(feats[pl.ds(base, half), :depth], w[...])
            for i in range(waves):
                piece = full[i * wrows : (i + 1) * wrows].astype(dst.dtype)
                for f in range(n_far):
                    dst[i, f, which * wrows : (which + 1) * wrows] = piece[:, f * cols : (f + 1) * cols]

    def x_copy(i, src, dst, send, recv):
        return pltpu.make_async_remote_copy(
            src_ref=src.at[i],
            dst_ref=dst.at[i],
            send_sem=send.at[i],
            recv_sem=recv.at[i],
            device_id=near_id(far, 1 - side),
        )

    def z_copy(i, d, src, dst, send, recv):
        return pltpu.make_async_remote_copy(
            src_ref=src.at[i, far_id(d)],
            dst_ref=dst.at[d - 1, i],
            send_sem=send.at[d - 1, i],
            recv_sem=recv.at[d - 1, i],
            device_id=near_id(far_id(d), side),
        )

    def last_copy(d):
        return pltpu.make_async_remote_copy(
            src_ref=q_last.at[far_id(d)],
            dst_ref=q_last_in.at[d - 1],
            send_sem=l_send.at[d - 1],
            recv_sem=l_recv.at[d - 1],
            device_id=near_id(far_id(d), side),
        )

    def last_cross():
        return pltpu.make_async_remote_copy(
            src_ref=q_last.at[far, 1],
            dst_ref=q_cross,
            send_sem=l_send.at[n_far - 1],
            recv_sem=l_recv.at[n_far - 1],
            device_id=near_id(far, 1 - side),
        )

    load_of["q"].wait()
    project_q(peer_half, q_out, 1)
    pl.semaphore_wait(barrier, n + n_tp - 2)
    for i in range(waves - 1):
        x_copy(i, q_out, q_in, qx_send, qx_recv).start()
    project_q(own_half, q_own, 0)
    for d in range(1, n_far):
        last_copy(d).start()
    load_of["k"].wait()
    load_of["v"].wait()
    project_kv(peer_half, kv_out)
    for i in range(waves):
        x_copy(i, kv_out, kv_in, kx_send, kx_recv).start()
    project_kv(own_half, kv_own)

    load_of["bias"].wait()
    load_of["parents"].wait()
    load_of["lengths"].wait()
    load_of["decay"].wait()
    par_pad[...] = jnp.zeros(par_pad.shape, jnp.int32)
    par_pad[0:seqs, 0:props] = parents[...]
    r_i = iota((LANES, LANES), 0)
    c_i = iota((LANES, LANES), 1)
    lane1 = iota((1, LANES), 1)
    eye = r_i == c_i
    for i in range(waves):
        row = jnp.full((1, LANES), -1, jnp.int32)
        for j in range(wave):
            of = par_pad[pl.ds(side * half_seqs + i * wave + j, 1), :]
            if j:
                of = pltpu.roll(jnp.broadcast_to(of, (8, LANES)), j * props, 1)[0:1]
            inside = (lane1 >= j * props) & (lane1 < (j + 1) * props)
            row = jnp.where(inside, of + j * props, row)
        link = ((row == r_i) | eye).astype(F32).astype(BF16)
        for _ in range(props.bit_length()):
            link = jnp.minimum(dot(link, link), 1.0).astype(BF16)
        link_s[i] = link
        anc_s[i] = dot_nt(eye.astype(F32).astype(BF16), link)
    w_row = lax.rem(iota(widen.shape, 0), LANES)
    w_col = iota(widen.shape, 1)
    w_src = lax.div(w_col, cols) * 8 + lax.div(lax.rem(w_col, cols), head_dim)
    widen[...] = (w_row == w_src).astype(F32).astype(BF16)
    b_shape = (8, bias.shape[1])
    b_row, b_col = iota(b_shape, 0), iota(b_shape, 1)
    mine = (b_row < own_heads) & (b_col == tp * heads + far * own_heads + b_row)
    bias_col = jnp.sum(jnp.where(mine, jnp.broadcast_to(bias[...], b_shape), 0.0), axis=1, keepdims=True)

    for i in range(waves - 1):
        x_copy(i, q_out, q_in, qx_send, qx_recv).wait_recv()
        q_own[i] = q_own[i] + q_in[i]
        for d in range(1, n_far):
            z_copy(i, d, q_own, q_far, qz_send, qz_recv).start()
    for d in range(1, n_far):
        last_copy(d).wait_recv()
    q_last[far] = q_last[far] + functools.reduce(jnp.add, [q_last_in[d] for d in range(n_far - 1)])
    last_cross().start()

    targets = [(d, 0) for d in range(1, n_far)] + [(d, 1) for d in range(n_far)]

    def target_id(d, cross):
        return near_id(far_id(d), side if not cross else 1 - side)

    def spread_copy(i, t, buf, send, recv):
        d, cross = targets[t]
        block = side * waves + i
        return pltpu.make_async_remote_copy(
            src_ref=buf.at[block, far],
            dst_ref=buf.at[block, far],
            send_sem=send.at[t, i],
            recv_sem=recv.at[block, far],
            device_id=target_id(d, cross),
        )

    def relay_copy(i, buf, send, recv):
        block = side * waves + i
        return pltpu.make_async_remote_copy(
            src_ref=buf.at[block],
            dst_ref=buf.at[block],
            send_sem=send.at[i],
            recv_sem=recv.at[i],
            device_id=near_id(far, 1 - side),
        )

    def spread(i, direct, buf, send, recv):
        for t in range(sources if direct else n_far - 1):
            spread_copy(i, t, buf, send, recv).start()

    def sent(i, direct, buf, send, recv, r_send, r_recv):
        for t in range(sources if direct else n_far - 1):
            spread_copy(i, t, buf, send, recv).wait_send()
        if not direct:
            relay_copy(i, buf, r_send, r_recv).wait_send()

    def spread_wait(i, t, buf, send, recv):
        d, cross = targets[t]
        block = (1 - side if cross else side) * waves + i
        pltpu.make_async_remote_copy(
            src_ref=buf.at[block, far_id(d)],
            dst_ref=buf.at[block, far_id(d)],
            send_sem=send.at[t, i],
            recv_sem=recv.at[block, far_id(d)],
            device_id=target_id(d, cross),
        ).wait_recv()

    def pass_on(i, direct, buf, send, recv, r_send, r_recv):
        for t in range(n_far - 1):
            spread_wait(i, t, buf, send, recv)
        if not direct:
            relay_copy(i, buf, r_send, r_recv).start()

    def crossed(i, direct, buf, send, recv, r_send, r_recv):
        if not direct:
            relay_copy(i, buf, r_send, r_recv).wait_recv()
            return
        for t in range(n_far - 1, sources):
            spread_wait(i, t, buf, send, recv)

    q_route = (qbuf, b_send, b_recv, qr_send, qr_recv)
    a_route = (att, d_send, d_recv, ar_send, ar_recv)
    q_direct = [False] * waves
    a_direct = [i > 0 for i in range(waves)]

    strides = [1 << b for b in range(n_far.bit_length() - 1)]

    def halve_copy(i, st, m):
        slot = sum(n_far // (2 * x) for x in strides if x < st) + m
        partner = far + st - 2 * st * lax.rem(lax.div(far, st), 2)
        return pltpu.make_async_remote_copy(
            src_ref=kv_pass.at[i, lax.rem(partner, 2 * st) + 2 * st * m],
            dst_ref=kv_far.at[slot, i],
            send_sem=kz_send.at[slot, i],
            recv_sem=kz_recv.at[slot, i],
            device_id=near_id(partner, side),
        )

    def halve_start(i, st):
        partner = far + st - 2 * st * lax.rem(lax.div(far, st), 2)
        for m in range(n_far // (2 * st)):
            f = lax.rem(partner, 2 * st) + 2 * st * m
            kv_pass[i, f] = kv_own[i, f].astype(BF16)
            halve_copy(i, st, m).start()

    def halve_wait(i, st):
        for m in range(n_far // (2 * st)):
            halve_copy(i, st, m).wait_recv()
            f = lax.rem(far, 2 * st) + 2 * st * m
            slot = sum(n_far // (2 * x) for x in strides if x < st) + m
            kv_own[i, f] = kv_own[i, f] + kv_far[slot, i].astype(F32)

    def pass_kv(i, step):
        if step:
            halve_wait(i, strides[step - 1])
        else:
            x_copy(i, kv_out, kv_in, kx_send, kx_recv).wait_recv()
            kv_own[i] = kv_own[i] + kv_in[i].astype(F32)
        if step < len(strides):
            halve_start(i, strides[step])

    lane8 = iota((8, LANES), 1)
    row8 = iota((8, LANES), 0)

    def owner_q(i):
        if i < waves - 1:
            total = q_own[i, far]
            for d in range(1, n_far):
                z_copy(i, d, q_own, q_far, qz_send, qz_recv).wait_recv()
                total = total + q_far[d - 1, i]
        else:
            last_cross().wait_recv()
            total = q_last[far, 0] + q_cross[...]
        tail = total[wrows:]
        inverse = lax.rsqrt(tail / (depth * n) + 1e-06)
        column = tile_rows(inverse, LANES).T[:wrows, own_heads : own_heads + 1]
        inv_s[i] = jnp.broadcast_to(column, (wrows, cols))
        qbuf[side * waves + i, far] = (inv_s[i] * total[:wrows]).astype(BF16)
        spread(i, q_direct[i], qbuf, b_send, b_recv)
        inverse_row = jnp.broadcast_to(inverse[own_heads : own_heads + 1], (8, LANES))
        x = inverse_row * tail + bias_col
        log_gate = jnp.minimum(x, 0.0) - jnp.log1p(jnp.exp(-jnp.abs(x)))
        log_gate = jnp.where((row8 < own_heads) & (lane8 < wrows), log_gate, 0.0)
        parts = dot(jnp.concatenate(split3(log_gate), axis=0), link_s[i])
        path_s[i] = parts[:8] + parts[8:16] + parts[16:24]

    for i in range(waves):
        owner_q(i)
        if i < waves - 1:
            pass_kv(i, 0)

    group = min(heads, 256 // head_dim)
    gwidth = group * head_dim
    g_head = iota((group, props, gwidth), 0)
    g_col = lax.div(iota((group, props, gwidth), 2), head_dim)
    g_diag = (g_head == g_col).reshape(group * props, gwidth)
    lane_w = iota((wrows, LANES), 1)
    position = iota((heads, pos_dev), 1) + me * pos_dev

    def mix_copy(i, t, which, src, dst):
        d, cross = targets[t]
        block = (1 - side if cross else side) * waves + i
        return pltpu.make_async_remote_copy(
            src_ref=src.at[block, far_id(d)],
            dst_ref=dst.at[t, i],
            send_sem=c_send.at[which, t, i],
            recv_sem=c_recv.at[which, t, i],
            device_id=target_id(d, cross),
        )

    def attend(i, cross):
        place = 1 - side if cross else side
        block = place * waves + i
        if cross:
            crossed(i, q_direct[i], *q_route)
        first = place * half_seqs + i * wave
        for j in range(wave):
            s = first + j
            pltpu.make_async_copy(keys_hbm.at[s], keys.at[s], cache_sem.at[0, s]).wait()
            pltpu.make_async_copy(values_hbm.at[s], values.at[s], cache_sem.at[1, s]).wait()
        q_wave = jnp.concatenate([qbuf[block, f] for f in range(n_far)], axis=1).astype(F32)
        if exact_scale:
            q_wave = q_wave * scale
        chains = [(j, g) for j in range(wave) for g in range(heads // group)]
        scores_of, w_of, tops, totals, parts = {}, {}, {}, {}, {}
        for j in range(wave):
            s = first + j
            fade = jnp.where(position < lengths[s], decay[s], LOW)
            for g in range(heads // group):
                q = q_wave[j * props : (j + 1) * props, g * gwidth : (g + 1) * gwidth]
                q = jnp.broadcast_to(q[None], (group, props, gwidth)).reshape(group * props, gwidth)
                q = jnp.where(g_diag, q, 0.0).astype(BF16)
                scores = dot_nt(q, keys[s, :, g * gwidth : (g + 1) * gwidth])
                if not exact_scale:
                    scores = scores * scale
                fades = [
                    jnp.broadcast_to(fade[h : h + 1], (props, pos_dev))
                    for h in range(g * group, (g + 1) * group)
                ]
                scores_of[j, g] = scores + jnp.concatenate(fades, axis=0)
        for j, g in chains:
            top = jnp.max(scores_of[j, g], axis=1, keepdims=True)
            w = jnp.exp(scores_of[j, g] - top)
            total = jnp.sum(w, axis=1, keepdims=True)
            w_of[j, g] = w.astype(BF16)
            for h in range(group):
                tops[j, g * group + h] = top[h * props : (h + 1) * props]
                totals[j, g * group + h] = total[h * props : (h + 1) * props]
        for j, g in chains:
            m = dot(w_of[j, g], values[first + j, :, g * gwidth : (g + 1) * gwidth])
            m = jnp.where(g_diag, m, 0.0).reshape(group, props, gwidth)
            parts[j, g] = jnp.sum(m, axis=0)
        mixes = [
            jnp.concatenate([parts[j, g] for g in range(heads // group)], axis=1) for j in range(wave)
        ]
        mixed = jnp.concatenate(mixes, axis=0).astype(BF16)
        for f in range(n_far):
            mix[block, f] = mixed[:, f * cols : (f + 1) * cols]
        acc = jnp.zeros((wrows, LANES), F32)
        for h in range(heads):
            f, k = divmod(h, own_heads)
            for at, cols_of in ((k, tops), (own_heads + k, totals)):
                col = jnp.concatenate([cols_of[j, h] for j in range(wave)], axis=0)
                acc = jnp.where(lane_w == f * 8 + at, col, acc)
        flat = tile_rows(acc, LANES).T
        for f in range(n_far):
            stat[block, f] = flat[f * 8 : f * 8 + stat.shape[2]]
        for t in range(sources):
            if targets[t][1] == cross:
                mix_copy(i, t, 0, mix, mix_in).start()
                mix_copy(i, t, 1, stat, stat_in).start()

    own_head_of = lax.div(iota((wrows, cols), 1), head_dim)

    def tree(i):
        block = side * waves + i
        pass_kv(i, len(strides))
        total = kv_own[i, far]
        new_k = tile_rows(inv_s[i] * total[:wrows], LANES).astype(BF16)
        new_v = tile_rows(inv_s[i] * total[wrows:], LANES).astype(BF16)
        q = qbuf[block, far].astype(F32)
        q = jnp.concatenate([jnp.where(own_head_of == h, q, 0.0) for h in range(own_heads)], axis=0)
        scores = dot_nt(q.astype(BF16), new_k) * scale
        path = path_s[i]
        path_cols = tile_rows(path, LANES).T[:wrows]
        shifts = [path_cols[:, h : h + 1] - path[h : h + 1] for h in range(own_heads)]
        scores = scores + jnp.concatenate(shifts, axis=0)
        live = jnp.concatenate([anc_s[i, :wrows]] * own_heads, axis=0) > 0.5
        scores = jnp.where(live, scores, LOW)
        top = jnp.max(scores, axis=1, keepdims=True)
        w = jnp.where(live, jnp.exp(scores - top), 0.0)
        total = jnp.sum(w, axis=1, keepdims=True)
        m = dot(w.astype(BF16), new_v)
        merged = jnp.zeros((wrows, cols), F32)
        acc = jnp.zeros((wrows, LANES), F32)
        for h in range(own_heads):
            part = slice(h * wrows, (h + 1) * wrows)
            merged = jnp.where(own_head_of == h, m[part], merged)
            acc = jnp.where(lane_w == h, top[part], acc)
            acc = jnp.where(lane_w == own_heads + h, total[part], acc)
        tmix[i] = merged
        tstat[i] = tile_rows(acc, LANES).T[:8]

    def merge(i):
        block = side * waves + i
        for t in range(sources):
            mix_copy(i, t, 0, mix, mix_in).wait_recv()
            mix_copy(i, t, 1, stat, stat_in).wait_recv()
        stats = [stat[block, far]] + [stat_in[t, i] for t in range(sources)]
        stats = [tile_rows(st, 8) for st in stats]
        path = path_s[i]
        tops = [st + path for st in stats] + [tstat[i]]
        totals = [pltpu.roll(st, 8 - own_heads, 0) for st in stats + [tstat[i]]]
        best = functools.reduce(jnp.maximum, tops)
        factors = [jnp.exp(top - best) for top in tops]
        denom = functools.reduce(jnp.add, [f * t for f, t in zip(factors, totals)])
        factors = [jnp.where(row8 < own_heads, f / denom, 0.0) for f in factors]
        turned = tile_rows(jnp.concatenate(factors, axis=0), LANES).T[:wrows]
        high = turned.astype(BF16)
        low = (turned - high.astype(F32)).astype(BF16)
        wide = dot(jnp.concatenate([high, low], axis=1), widen[...])
        mixes = [mix[block, far]] + [mix_in[t, i] for t in range(sources)] + [tmix[i]]
        numer = jnp.zeros((wrows, cols), F32)
        for k, m in enumerate(mixes):
            numer = numer + wide[:, k * cols : (k + 1) * cols] * m.astype(F32)
        att[block, far] = numer.astype(BF16)
        spread(i, a_direct[i], att, d_send, d_recv)

    per_tp = seqs // n_tp

    def e_copy(s, t):
        k = jnp.maximum(lax.rem(tp - t + n_tp, n_tp) - 1, 0)
        return pltpu.make_async_remote_copy(
            src_ref=terms.at[s],
            dst_ref=terms_in.at[k, lax.rem(s, per_tp)],
            send_sem=e_send.at[s],
            recv_sem=e_recv.at[k, lax.rem(s, per_tp)],
            device_id={"tp": t},
        )

    def output(i, cross):
        place = 1 - side if cross else side
        block = place * waves + i
        if cross:
            crossed(i, a_direct[i], *a_route)
        attended = jnp.concatenate([att[block, f] for f in range(n_far)], axis=1)
        term = dot(attended, out_w[...])
        for j in range(wave):
            s = place * half_seqs + i * wave + j
            terms[s] = fold(term[j * props : (j + 1) * props]).astype(BF16)
            t = lax.div(s, per_tp)
            pl.when(tp != t)(e_copy(s, t).start)

    advanced = [0] * waves

    def advance(count):
        for i in range(waves):
            if count and advanced[i] + 1 < len(strides):
                advanced[i] += 1
                pass_kv(i, advanced[i])
                count -= 1

    pass_on(0, q_direct[0], *q_route)
    attend(0, 0)
    pass_kv(waves - 1, 0)
    advance(1)
    for i in range(1, waves):
        pass_on(i, q_direct[i], *q_route)
        if i == 1:
            attend(1, 0)
            advance(1)
    attend(0, 1)
    advance(1)
    for i in range(1, waves):
        if i + 1 < waves:
            attend(i + 1, 0)
        attend(i, 1)
    advance(waves * len(strides))
    load_of["out"].wait()
    for i in range(waves):
        tree(i)
        if i >= 2:
            pass_on(i - 2, a_direct[i - 2], *a_route)
        merge(i)
    if waves >= 2:
        pass_on(waves - 2, a_direct[waves - 2], *a_route)
    for i in range(waves):
        if i == waves - 1:
            pass_on(i, a_direct[i], *a_route)
        output(i, 0)
        output(i, 1)

    done = []
    for j in range(per_tp):
        total = unfold(terms[tp * per_tp + j])
        for k in range(1, n_tp):
            pltpu.make_async_remote_copy(
                src_ref=terms.at[0],
                dst_ref=terms_in.at[k - 1, j],
                send_sem=e_send.at[0],
                recv_sem=e_recv.at[k - 1, j],
                device_id={"tp": lax.rem(tp + k, n_tp)},
            ).wait_recv()
            total = total + unfold(terms_in[k - 1, j])
        done.append(total)
    out[...] = jnp.concatenate(done, axis=0).astype(BF16)

    for i in range(waves):
        if i < waves - 1:
            x_copy(i, q_out, q_in, qx_send, qx_recv).wait_send()
            for d in range(1, n_far):
                z_copy(i, d, q_own, q_far, qz_send, qz_recv).wait_send()
        x_copy(i, kv_out, kv_in, kx_send, kx_recv).wait_send()
        for st in strides:
            for m in range(n_far // (2 * st)):
                halve_copy(i, st, m).wait_send()
        sent(i, q_direct[i], *q_route)
        sent(i, a_direct[i], *a_route)
        for t in range(sources):
            mix_copy(i, t, 0, mix, mix_in).wait_send()
            mix_copy(i, t, 1, stat, stat_in).wait_send()
    for d in range(1, n_far):
        last_copy(d).wait_send()
    last_cross().wait_send()
    for s in range(seqs):
        t = s // per_tp
        pl.when(tp != t)(e_copy(s, t).wait_send)


def wave_size(n, n_tp, seqs, props, heads, width):
    n_far = n // 2
    if n < 4 or n & (n - 1) or seqs % 2 or seqs % n_tp or heads % n_far or width % (n_far * LANES):
        return 0
    head_dim = width // heads
    own = heads // n_far
    if own > 4 or 8 * (n + 1) > LANES or (heads % min(heads, max(256 // head_dim, 1))):
        return 0
    for wave in range(1, seqs // 2 + 1):
        fits = wave * props % 16 == 0 and wave * props <= LANES
        if seqs // 2 % wave == 0 and fits and props % 8 == 0:
            return wave
    return 0


def solution(mesh):
    n, n_tp = mesh.shape["kv"], mesh.shape["tp"]

    def body(
        tokens,
        norm_gain,
        query_weight,
        key_weight,
        value_weight,
        gate_weight,
        gate_bias,
        out_weight,
        cache_keys,
        cache_values,
        cache_decay,
        lengths,
        parents,
    ):
        rows, depth = tokens.shape
        seqs, props = parents.shape
        heads = cache_decay.shape[1]
        pos_dev = cache_keys.shape[1]
        width = query_weight.shape[1]
        cols = out_weight.shape[1]
        slots = -(-seqs // n)
        block = rows // n_tp
        all_w = 2 * width + LANES
        folded = (2 * props, width // 2)
        vmem = pl.BlockSpec(memory_space=pltpu.VMEM)
        hbm = pl.BlockSpec(memory_space=pltpu.HBM)
        dma = pltpu.SemaphoreType.DMA
        wave = wave_size(n, n_tp, seqs, props, heads, width)
        if wave:
            n_far = n // 2
            waves = seqs // 2 // wave
            q_waves = max(waves - 1, 1)
            wrows = wave * props
            wcols = width // n_far
            per_tp = seqs // n_tp
            s_rows = max(4, 2 * (heads // n_far))
            block_q = (n_far, wrows + 8, wcols)
            block_kv = (n_far, 2 * wrows, wcols)
            body_of = functools.partial(by_heads, n, n_tp, wave)
            scratch = [
                pltpu.VMEM(tokens.shape, BF16),
                pltpu.VMEM((1, depth), F32),
                pltpu.VMEM(query_weight.shape, BF16),
                pltpu.VMEM(key_weight.shape, BF16),
                pltpu.VMEM(value_weight.shape, BF16),
                pltpu.VMEM((gate_weight.shape[1], depth), BF16),
                pltpu.VMEM((1, gate_bias.shape[0]), F32),
                pltpu.VMEM(cache_decay.shape, F32),
                pltpu.SMEM(lengths.shape, jnp.int32),
                pltpu.VMEM(parents.shape, jnp.int32),
                pltpu.VMEM(out_weight.shape, BF16),
                pltpu.VMEM(cache_keys.shape, BF16),
                pltpu.VMEM(cache_values.shape, BF16),
                pltpu.VMEM((rows, 3 * depth), BF16),
                pltpu.VMEM((q_waves,) + block_q, F32),
                pltpu.VMEM((q_waves,) + block_q, F32),
                pltpu.VMEM((q_waves,) + block_q, F32),
                pltpu.VMEM((n_far - 1, q_waves) + block_q[1:], F32),
                pltpu.VMEM((n_far, 2) + block_q[1:], F32),
                pltpu.VMEM((n_far - 1, 2) + block_q[1:], F32),
                pltpu.VMEM(block_q[1:], F32),
                pltpu.VMEM((waves,) + block_kv, BF16),
                pltpu.VMEM((waves,) + block_kv, BF16),
                pltpu.VMEM((waves,) + block_kv, F32),
                pltpu.VMEM((waves,) + block_kv, BF16),
                pltpu.VMEM((n_far - 1, waves) + block_kv[1:], BF16),
                pltpu.VMEM((2 * waves, n_far, wrows, wcols), BF16),
                pltpu.VMEM((2 * waves, n_far, wrows, wcols), BF16),
                pltpu.VMEM((n - 1, waves, wrows, wcols), BF16),
                pltpu.VMEM((2 * waves, n_far, s_rows, LANES), F32),
                pltpu.VMEM((n - 1, waves, s_rows, LANES), F32),
                pltpu.VMEM((2 * waves, n_far, wrows, wcols), BF16),
                pltpu.VMEM((seqs,) + folded, BF16),
                pltpu.VMEM((n_tp - 1, per_tp) + folded, BF16),
                pltpu.VMEM((-(-seqs // 8) * 8, LANES), jnp.int32),
                pltpu.VMEM((waves, LANES, LANES), BF16),
                pltpu.VMEM((waves, LANES, LANES), F32),
                pltpu.VMEM((waves, 8, LANES), F32),
                pltpu.VMEM((waves, wrows, wcols), F32),
                pltpu.VMEM((waves, wrows, wcols), F32),
                pltpu.VMEM((waves, 8, LANES), F32),
                pltpu.VMEM((2 * LANES, (n + 1) * wcols), BF16),
                dma((11,)),
                dma((2, seqs)),
                dma((waves,)),
                dma((waves,)),
                dma((waves,)),
                dma((waves,)),
                dma((n_far - 1, waves)),
                dma((n_far - 1, waves)),
                dma((n_far - 1, waves)),
                dma((n_far - 1, waves)),
                dma((n - 1, waves)),
                dma((2 * waves, n_far)),
                dma((2, n - 1, waves)),
                dma((2, n - 1, waves)),
                dma((n - 1, waves)),
                dma((2 * waves, n_far)),
                dma((seqs,)),
                dma((n_tp - 1, per_tp)),
                dma((waves,)),
                dma((waves,)),
                dma((waves,)),
                dma((waves,)),
                dma((n_far,)),
                dma((n_far,)),
            ]
        else:
            body_of = functools.partial(by_sequence, n, n_tp)
            scratch = [
                pltpu.VMEM(tokens.shape, BF16),
                pltpu.VMEM((1, depth), F32),
                pltpu.VMEM(query_weight.shape, BF16),
                pltpu.VMEM(key_weight.shape, BF16),
                pltpu.VMEM(value_weight.shape, BF16),
                pltpu.VMEM((1, gate_bias.shape[0]), F32),
                pltpu.VMEM(cache_decay.shape, F32),
                pltpu.SMEM(lengths.shape, jnp.int32),
                pltpu.VMEM(parents.shape, jnp.int32),
                dma((9,)),
                pltpu.VMEM((seqs, props, all_w), F32),
                pltpu.VMEM((seqs,) + folded, BF16),
                pltpu.VMEM((seqs, props, all_w), F32),
                pltpu.VMEM((seqs,) + folded, BF16),
                pltpu.VMEM((n // 2 - 1, slots, props, all_w), F32),
                pltpu.VMEM((n // 2 - 1, slots) + folded, BF16),
                pltpu.VMEM((gate_weight.shape[1], depth), BF16),
                pltpu.VMEM(out_weight.shape, BF16),
                pltpu.VMEM(cache_keys.shape, BF16),
                pltpu.VMEM(cache_values.shape, BF16),
                pltpu.VMEM((seqs,) + folded, BF16),
                pltpu.VMEM((seqs,) + folded, BF16),
                pltpu.VMEM((seqs, props, LANES), F32),
                pltpu.VMEM((n - 1, slots) + folded, BF16),
                pltpu.VMEM((n - 1, slots, props, LANES), F32),
                pltpu.VMEM((seqs,) + folded, BF16),
                pltpu.VMEM((slots, props, LANES), F32),
                pltpu.VMEM((slots, props, LANES), F32),
                pltpu.VMEM((slots, props, width), F32),
                pltpu.VMEM((slots, 2, props, LANES), F32),
                pltpu.VMEM((slots, 2, LANES, width), F32),
                pltpu.VMEM((n_tp, block, cols), BF16),
                pltpu.VMEM((n_tp - 1, block, cols), BF16),
                pltpu.VMEM((-(-seqs // 8) * 8, LANES), jnp.int32),
                dma((2,)),
                dma((2, seqs)),
                dma((2, seqs)),
                dma((2, seqs)),
                dma((2, seqs)),
                dma((2, n // 2 - 1, slots)),
                dma((slots, n - 1)),
                dma((seqs,)),
                dma((2, seqs)),
                dma((2, n - 1, slots)),
                dma((slots, n - 1)),
                dma((seqs,)),
                dma((n_tp,)),
                dma((n_tp - 1,)),
            ]
        return pl.pallas_call(
            body_of,
            out_shape=pltpu.VMEM((block, cols), BF16),
            in_specs=[hbm] * 13,
            out_specs=vmem,
            scratch_shapes=scratch,
            compiler_params=pltpu.CompilerParams(
                collective_id=0, has_side_effects=True, vmem_limit_bytes=67_043_328 - 131072
            ),
        )(
            tokens,
            norm_gain.reshape(1, depth),
            query_weight,
            key_weight,
            value_weight,
            gate_weight.T,
            gate_bias.reshape(1, gate_bias.shape[0]),
            out_weight,
            cache_keys,
            cache_values,
            cache_decay,
            lengths,
            parents,
        )

    in_specs = (
        P(None, "kv"),
        P("kv"),
        P("kv", "tp"),
        P("kv", "tp"),
        P("kv", "tp"),
        P(),
        P(),
        P("tp", "kv"),
        P(None, "kv", "tp"),
        P(None, "kv", "tp"),
        P(None, "tp", "kv"),
        P(),
        P(),
    )
    out_specs = P("tp", "kv")
    return jax.shard_map(body, mesh=mesh, in_specs=in_specs, out_specs=out_specs, check_vma=False)
```

```python
import functools
import math

import jax
import jax.numpy as jnp
from jax import lax
from jax.experimental import pallas as pl
from jax.experimental.pallas import tpu as pltpu
from jax.sharding import PartitionSpec as P

F32 = jnp.float32
BF16 = jnp.bfloat16
LANES = 128
LOW = -1e30
NT = (((1,), (1,)), ((), ()))
HIGH = lax.Precision.HIGHEST


def dot(a, b, precision=None):
    return jnp.dot(a, b, preferred_element_type=F32, precision=precision)


def dot_nt(a, b, precision=None):
    return lax.dot_general(a, b, NT, preferred_element_type=F32, precision=precision)


def fold(x):
    half = x.shape[1] // 2
    return jnp.concatenate([x[:, :half], x[:, half:]], axis=0)


def unfold(x):
    rows = x.shape[0] // 2
    x = x.astype(F32)
    return jnp.concatenate([x[:rows], x[rows:]], axis=1)


def by_sequence(
    n,
    n_tp,
    tokens_hbm,
    gain_hbm,
    query_hbm,
    key_hbm,
    value_hbm,
    gate_hbm,
    bias_hbm,
    out_hbm,
    keys_hbm,
    values_hbm,
    decay_hbm,
    lengths_hbm,
    parents_hbm,
    out,
    tokens,
    gain,
    query_w,
    key_w,
    value_w,
    bias,
    decay,
    lengths,
    parents,
    small_sem,
    part,
    part_v,
    pair_in,
    pair_in_v,
    part_in,
    part_in_v,
    gate_w,
    out_w,
    keys,
    values,
    qbuf,
    mix,
    stat,
    mix_in,
    stat_in,
    att,
    anc,
    path_s,
    tmix,
    tstat,
    kvnew,
    terms,
    terms_in,
    par_pad,
    load_sem,
    cache_sem,
    p_send,
    p_recv,
    a_send,
    a_recv,
    b_send,
    b_recv,
    c_send,
    c_recv,
    d_send,
    d_recv,
    e_send,
    e_recv,
):
    me = lax.axis_index("kv")
    tp = lax.axis_index("tp")
    rows, depth = tokens.shape
    seqs, props = parents.shape
    heads = decay.shape[1]
    pos_dev = keys.shape[1]
    width = query_w.shape[1]
    head_dim = width // heads
    scale = head_dim ** (-0.5)
    slots = part_in.shape[1]
    parity = lax.rem(tp, 2)
    left_over = seqs % n
    hp = heads * props

    barrier = pltpu.get_barrier_semaphore()
    for k in range(1, n):
        pl.semaphore_signal(barrier, inc=1, device_id={"kv": lax.rem(me + k, n)})
    for k in range(1, n_tp):
        pl.semaphore_signal(barrier, inc=1, device_id={"tp": lax.rem(tp + k, n_tp)})

    pairs = (
        (tokens_hbm, tokens),
        (gain_hbm, gain),
        (query_hbm, query_w),
        (key_hbm, key_w),
        (value_hbm, value_w),
        (bias_hbm, bias),
        (parents_hbm, parents),
        (decay_hbm, decay),
        (lengths_hbm, lengths),
    )
    small_loads = [
        pltpu.make_async_copy(src, dst, small_sem.at[i]) for i, (src, dst) in enumerate(pairs)
    ]
    for load in small_loads:
        load.start()
    gate_load = pltpu.make_async_copy(
        gate_hbm.at[:, pl.ds(pl.multiple_of(me * depth, depth), depth)], gate_w, load_sem.at[0]
    )
    gate_load.start()
    cache_loads = []
    for s in range(seqs):
        k_load = pltpu.make_async_copy(keys_hbm.at[s], keys.at[s], cache_sem.at[0, s])
        v_load = pltpu.make_async_copy(values_hbm.at[s], values.at[s], cache_sem.at[1, s])
        k_load.start()
        v_load.start()
        cache_loads.append((k_load, v_load))
    out_load = pltpu.make_async_copy(out_hbm, out_w, load_sem.at[1])
    out_load.start()

    def owner_of(s):
        if isinstance(s, int):
            place = s % n
            shift = parity * left_over if s // n == seqs // n else 0
        else:
            place = lax.rem(s, n)
            shift = jnp.where(lax.div(s, n) == seqs // n, parity * left_over, 0)
        return lax.rem(place + shift, n)

    def slot_seq(r):
        shift = parity * left_over if r == seqs // n else 0
        return r * n + lax.rem(me + 2 * n - shift, n)

    def for_slot(r, f):
        if (r + 1) * n <= seqs:
            f()
        else:
            pl.when(slot_seq(r) < seqs)(f)

    for load in small_loads:
        load.wait()
    xf = tokens[...].astype(F32)
    squares = jnp.sum(xf * xf, axis=1, keepdims=True)
    normed = (xf * gain[...]).astype(BF16)
    sel_rows = lax.broadcasted_iota(jnp.int32, (bias.shape[1], LANES), 0)
    sel_cols = lax.broadcasted_iota(jnp.int32, (bias.shape[1], LANES), 1)
    select = ((sel_rows == sel_cols + tp * heads) & (sel_cols < heads)).astype(F32)
    for i, w in enumerate((query_w, key_w)):
        part[:, :, i * width : (i + 1) * width] = dot(normed, w[...]).reshape(seqs, props, width)
    value_part = dot(normed, value_w[...])
    for s in range(seqs):
        part_v[s] = fold(value_part[s * props : (s + 1) * props]).astype(BF16)
    gate_load.wait()
    gates_w = lax.dot_general(
        select.astype(BF16), gate_w[...], (((0,), (0,)), ((), ())), preferred_element_type=F32
    )
    gate_part = dot_nt(normed, gates_w.astype(BF16))
    lane = lax.broadcasted_iota(jnp.int32, (rows, LANES), 1)
    gate_part = jnp.where(lane == LANES // 2, squares, gate_part)
    part[:, :, 2 * width :] = gate_part.reshape(seqs, props, LANES)
    pl.semaphore_wait(barrier, n + n_tp - 2)

    side = lax.rem(me, 2)
    partner = me + 1 - 2 * side
    n_far = n // 2
    shares = ((part, pair_in, part_in), (part_v, pair_in_v, part_in_v))

    def p_copy(s, which):
        src, dst, _ = shares[which]
        return pltpu.make_async_remote_copy(
            src_ref=src.at[s],
            dst_ref=dst.at[s],
            send_sem=p_send.at[which, s],
            recv_sem=p_recv.at[which, s],
            device_id={"kv": partner},
        )

    def a_copy(s, which):
        src, _, dst = shares[which]
        d = owner_of(s)
        k = jnp.maximum(lax.rem(lax.div(me, 2) - lax.div(d, 2) + n_far, n_far) - 1, 0)
        return pltpu.make_async_remote_copy(
            src_ref=src.at[s],
            dst_ref=dst.at[k, s // n],
            send_sem=a_send.at[which, s],
            recv_sem=a_recv.at[which, k, s // n],
            device_id={"kv": d},
        )

    def crosses(s):
        return lax.rem(owner_of(s), 2) != side

    def passes(s):
        d = owner_of(s)
        return (lax.rem(d, 2) == side) & (d != me)

    for s in range(seqs):
        for which in range(2):
            pl.when(crosses(s))(p_copy(s, which).start)

    par_pad[...] = jnp.zeros(par_pad.shape, jnp.int32)
    par_pad[0:seqs, 0:props] = parents[...]
    r_i = lax.broadcasted_iota(jnp.int32, (LANES, LANES), 0)
    c_i = lax.broadcasted_iota(jnp.int32, (LANES, LANES), 1)
    eye = (r_i == c_i).astype(F32)
    bias_row = dot(jnp.broadcast_to(bias[...], (8, bias.shape[1])), select, HIGH)[0:1]

    def ancestry(r):
        s = slot_seq(r)
        row = par_pad[pl.ds(s, 1), :]
        link = jnp.maximum((row == r_i).astype(F32), eye).astype(BF16)
        for _ in range(props.bit_length()):
            link = jnp.minimum(dot(link, link), 1.0).astype(BF16)
        anc[r] = dot_nt(eye.astype(BF16), link)[:props]

    for r in range(slots):
        for_slot(r, functools.partial(ancestry, r))

    def pass_on(s):
        for which in range(2):
            p_copy(s, which).wait_recv()
        part[s] = part[s] + pair_in[s]
        part_v[s] = (part_v[s].astype(F32) + pair_in_v[s].astype(F32)).astype(BF16)
        for which in range(2):
            a_copy(s, which).start()

    for s in range(seqs):
        pl.when(passes(s))(functools.partial(pass_on, s))

    lane_p = lax.broadcasted_iota(jnp.int32, (props, LANES), 1)
    bd_row = lax.broadcasted_iota(jnp.int32, (heads, props, width), 0)
    bd_col = lax.broadcasted_iota(jnp.int32, (heads, props, width), 2)
    diag = (lax.div(bd_col, head_dim) == bd_row).reshape(hp, width)

    def spread(q):
        wide = jnp.broadcast_to(q[None], (heads, props, width)).reshape(hp, width)
        return jnp.where(diag, wide, 0.0).astype(BF16)

    def gather_diag(m):
        return jnp.sum(jnp.where(diag, m, 0.0).reshape(heads, props, width), axis=0)

    def to_lanes(col, first):
        acc = jnp.zeros((props, LANES), F32)
        for h in range(heads):
            acc = jnp.where(lane_p == h + first, col[h * props : (h + 1) * props], acc)
        return acc

    def b_copy(r, k, buf, send, recv):
        s = slot_seq(r)
        return pltpu.make_async_remote_copy(
            src_ref=buf.at[s],
            dst_ref=buf.at[s],
            send_sem=send.at[r, k - 1],
            recv_sem=recv.at[s],
            device_id={"kv": lax.rem(me + k, n)},
        )

    pad_rows = LANES - props

    def project(r):
        s = slot_seq(r)
        for which, (src, near, far) in enumerate(shares):
            pltpu.make_async_remote_copy(
                src_ref=src.at[0],
                dst_ref=near.at[s],
                send_sem=p_send.at[which, 0],
                recv_sem=p_recv.at[which, s],
                device_id={"kv": partner},
            ).wait_recv()
            for k in range(1, n_far):
                pltpu.make_async_remote_copy(
                    src_ref=src.at[0],
                    dst_ref=far.at[k - 1, r],
                    send_sem=a_send.at[which, 0],
                    recv_sem=a_recv.at[which, k - 1, r],
                    device_id={"kv": lax.rem(me + 2 * k, n)},
                ).wait_recv()
        total = part[s] + pair_in[s]
        total_v = unfold(part_v[s]) + unfold(pair_in_v[s])
        for k in range(1, n_far):
            total = total + part_in[k - 1, r]
            total_v = total_v + unfold(part_in_v[k - 1, r])
        tail = total[:, 2 * width :]
        square = jnp.sum(jnp.where(lane_p == LANES // 2, tail, 0.0), axis=1, keepdims=True)
        inverse = lax.rsqrt(square / (depth * n) + 1e-06)
        q = inverse * total[:, :width]
        qbuf[s] = fold(q).astype(BF16)
        for k in range(1, n):
            b_copy(r, k, qbuf, b_send, b_recv).start()
        kvnew[r, 0, 0:props] = inverse * total[:, width : 2 * width]
        kvnew[r, 1, 0:props] = inverse * total_v
        kvnew[r, :, props:] = jnp.zeros((2, pad_rows, width), F32)
        x = inverse * tail + bias_row
        log_gate = jnp.minimum(x, 0.0) - jnp.log1p(jnp.exp(-jnp.abs(x)))
        padded = jnp.concatenate([log_gate, jnp.zeros((pad_rows, LANES), F32)], axis=0)
        path_s[r] = dot(anc[r], padded, HIGH)

    def tree(r):
        s = slot_seq(r)
        path = path_s[r]
        q = spread(unfold(qbuf[s]))
        head_of = lax.broadcasted_iota(jnp.int32, (heads, props, LANES), 0)
        lane_of = lax.broadcasted_iota(jnp.int32, (heads, props, LANES), 2)
        pick = (head_of == lane_of).reshape(hp, LANES)
        tiled = jnp.broadcast_to(path[None], (heads, props, LANES)).reshape(hp, LANES)
        own = jnp.sum(jnp.where(pick, tiled, 0.0), axis=1, keepdims=True)
        padded = jnp.concatenate([path, jnp.zeros((pad_rows, LANES), F32)], axis=0)
        other = dot_nt(pick.astype(F32), padded, HIGH)
        scores = dot_nt(q, kvnew[r, 0].astype(BF16)) * scale + own - other
        live = jnp.broadcast_to(anc[r][None], (heads, props, LANES)).reshape(hp, LANES) > 0.5
        scores = jnp.where(live, scores, LOW)
        top = jnp.max(scores, axis=1, keepdims=True)
        w = jnp.where(live, jnp.exp(scores - top), 0.0)
        total = jnp.sum(w, axis=1, keepdims=True)
        tmix[r] = gather_diag(dot(w.astype(BF16), kvnew[r, 1].astype(BF16)))
        tstat[r, 0] = to_lanes(top, 0)
        tstat[r, 1] = to_lanes(total, 0)

    position = lax.broadcasted_iota(jnp.int32, (hp, pos_dev), 1) + me * pos_dev

    def c_copy(s, which, src, dst):
        d = owner_of(s)
        k = jnp.maximum(lax.rem(me - d + n, n) - 1, 0)
        slot = s // n if isinstance(s, int) else lax.div(s, n)
        return d, pltpu.make_async_remote_copy(
            src_ref=src.at[s],
            dst_ref=dst.at[k, slot],
            send_sem=c_send.at[which, s],
            recv_sem=c_recv.at[which, k, slot],
            device_id={"kv": d},
        )

    def shard(s, carry):
        d = owner_of(s)

        @pl.when(d != me)
        def _():
            pltpu.make_async_remote_copy(
                src_ref=qbuf.at[s],
                dst_ref=qbuf.at[s],
                send_sem=b_send.at[0, 0],
                recv_sem=b_recv.at[s],
                device_id={"kv": d},
            ).wait_recv()

        pltpu.make_async_copy(keys_hbm.at[s], keys.at[s], cache_sem.at[0, s]).wait()
        pltpu.make_async_copy(values_hbm.at[s], values.at[s], cache_sem.at[1, s]).wait()
        q = spread(unfold(qbuf[s]))
        fade = decay[s]
        fade = jnp.concatenate(
            [jnp.broadcast_to(fade[h : h + 1], (props, pos_dev)) for h in range(heads)], axis=0
        )
        scores = dot_nt(q, keys[s]) * scale + fade
        live = position < lengths[s]
        scores = jnp.where(live, scores, LOW)
        top = jnp.max(scores, axis=1, keepdims=True)
        w = jnp.where(live, jnp.exp(scores - top), 0.0)
        total = jnp.sum(w, axis=1, keepdims=True)
        mix[s] = fold(gather_diag(dot(w.astype(BF16), values[s]))).astype(BF16)
        stat[s] = to_lanes(top, 0) + to_lanes(total, heads)
        for which, (src, dst) in enumerate(((mix, mix_in), (stat, stat_in))):
            _, copy = c_copy(s, which, src, dst)
            pl.when(d != me)(copy.start)
        return carry

    ex_r = lax.broadcasted_iota(jnp.int32, (LANES, width), 0)
    ex_c = lax.broadcasted_iota(jnp.int32, (LANES, width), 1)
    widen = (ex_r == lax.div(ex_c, head_dim)).astype(F32)

    def merge(r):
        s = slot_seq(r)
        for k in range(1, n):
            for which, (src, dst) in enumerate(((mix, mix_in), (stat, stat_in))):
                pltpu.make_async_remote_copy(
                    src_ref=src.at[0],
                    dst_ref=dst.at[k - 1, r],
                    send_sem=c_send.at[which, 0],
                    recv_sem=c_recv.at[which, k - 1, r],
                    device_id={"kv": lax.rem(me + k, n)},
                ).wait_recv()
        stats = jnp.concatenate([stat[s]] + [stat_in[k, r] for k in range(n - 1)], axis=0)
        totals = pltpu.roll(stats, LANES - heads, 1).reshape(n, props, LANES)
        tops = stats.reshape(n, props, LANES) + path_s[r][None]
        tops = jnp.where((lane_p < heads)[None], tops, LOW)
        ttop = jnp.where(lane_p < heads, tstat[r, 0], LOW)
        best = jnp.maximum(jnp.max(tops, axis=0), ttop)
        factors = jnp.exp(tops - best[None])
        tfactor = jnp.exp(ttop - best)
        denom = jnp.sum(factors * totals, axis=0) + tfactor * tstat[r, 1]
        packed = jnp.concatenate([factors.reshape(n * props, LANES), tfactor, denom], axis=0)
        wide = dot(packed, widen, HIGH)
        numer = wide[n * props : (n + 1) * props] * tmix[r] + wide[:props] * unfold(mix[s])
        for k in range(1, n):
            numer = numer + wide[k * props : (k + 1) * props] * unfold(mix_in[k - 1, r])
        att[s] = fold(numer / wide[(n + 1) * props :]).astype(BF16)
        for k in range(1, n):
            b_copy(r, k, att, d_send, d_recv).start()

    for r in range(slots):
        for_slot(r, functools.partial(project, r))
        if r > 0:
            for_slot(r - 1, functools.partial(merge, r - 1))
        for_slot(r, functools.partial(tree, r))
        lax.fori_loop(r * n, min((r + 1) * n, seqs), shard, 0)
    for_slot(slots - 1, functools.partial(merge, slots - 1))

    out_load.wait()
    block = rows // n_tp

    def e_copy(t):
        k = lax.rem(tp - t + n_tp, n_tp)
        return pltpu.make_async_remote_copy(
            src_ref=terms.at[t],
            dst_ref=terms_in.at[jnp.maximum(k - 1, 0)],
            send_sem=e_send.at[t],
            recv_sem=e_recv.at[jnp.maximum(k - 1, 0)],
            device_id={"tp": t},
        )

    arrived = 0
    for t in range(n_tp):
        first, last = t * block // props, ((t + 1) * block - 1) // props + 1
        for s in range(arrived, last):
            d = owner_of(s)

            @pl.when(d != me)
            def _(s=s, d=d):
                pltpu.make_async_remote_copy(
                    src_ref=att.at[s],
                    dst_ref=att.at[s],
                    send_sem=d_send.at[0, 0],
                    recv_sem=d_recv.at[s],
                    device_id={"kv": d},
                ).wait_recv()

        arrived = max(arrived, last)
        attended = jnp.concatenate([unfold(att[s]) for s in range(first, last)], axis=0)
        term = dot(attended.astype(BF16), out_w[...])
        begin = t * block - first * props
        terms[t] = term[begin : begin + block].astype(BF16)
        pl.when(tp != t)(e_copy(t).start)
    total = terms[tp].astype(F32)
    for k in range(1, n_tp):
        pltpu.make_async_remote_copy(
            src_ref=terms.at[0],
            dst_ref=terms_in.at[k - 1],
            send_sem=e_send.at[0],
            recv_sem=e_recv.at[k - 1],
            device_id={"tp": lax.rem(tp + k, n_tp)},
        ).wait_recv()
        total = total + terms_in[k - 1].astype(F32)
    out[...] = total.astype(BF16)

    for s in range(seqs):
        d = owner_of(s)
        for which in range(2):
            pl.when(crosses(s))(p_copy(s, which).wait_send)
            pl.when(passes(s))(a_copy(s, which).wait_send)
        for which, (src, dst) in enumerate(((mix, mix_in), (stat, stat_in))):
            _, copy = c_copy(s, which, src, dst)
            pl.when(d != me)(copy.wait_send)
    for r in range(slots):

        def drain(r=r):
            for k in range(1, n):
                b_copy(r, k, qbuf, b_send, b_recv).wait_send()
                b_copy(r, k, att, d_send, d_recv).wait_send()

        for_slot(r, drain)
    for t in range(n_tp):
        pl.when(tp != t)(e_copy(t).wait_send)


def split3(x):
    high = x.astype(BF16)
    rest = x - high.astype(F32)
    mid = rest.astype(BF16)
    low = (rest - mid.astype(F32)).astype(BF16)
    return high, mid, low


def tile_rows(rows, total):
    return jnp.concatenate([rows, jnp.zeros((total - rows.shape[0], rows.shape[1]), rows.dtype)], axis=0)


def by_heads(
    n,
    n_tp,
    wave,
    tokens_hbm,
    gain_hbm,
    query_hbm,
    key_hbm,
    value_hbm,
    gate_hbm,
    bias_hbm,
    out_hbm,
    keys_hbm,
    values_hbm,
    decay_hbm,
    lengths_hbm,
    parents_hbm,
    out,
    tokens,
    gain,
    query_w,
    key_w,
    value_w,
    gate_w,
    bias,
    decay,
    lengths,
    parents,
    out_w,
    keys,
    values,
    feats,
    q_out,
    q_in,
    q_own,
    q_far,
    q_last,
    q_last_in,
    q_cross,
    kv_out,
    kv_in,
    kv_own,
    kv_pass,
    kv_far,
    qbuf,
    mix,
    mix_in,
    stat,
    stat_in,
    att,
    terms,
    terms_in,
    par_pad,
    link_s,
    anc_s,
    path_s,
    inv_s,
    tmix,
    tstat,
    held,
    swap,
    swap_in,
    swap_stat,
    swap_stat_in,
    widen,
    load_sem,
    cache_sem,
    qx_send,
    qx_recv,
    kx_send,
    kx_recv,
    qz_send,
    qz_recv,
    kz_send,
    kz_recv,
    b_send,
    b_recv,
    c_send,
    c_recv,
    d_send,
    d_recv,
    e_send,
    e_recv,
    qr_send,
    qr_recv,
    s_send,
    s_recv,
    l_send,
    l_recv,
):
    me = lax.axis_index("kv")
    tp = lax.axis_index("tp")
    side = lax.rem(me, 2)
    far = lax.div(me, 2)
    n_far = n // 2
    rows, depth = tokens.shape
    seqs, props = parents.shape
    heads = decay.shape[1]
    pos_dev = keys.shape[1]
    width = query_w.shape[1]
    head_dim = width // heads
    scale = head_dim ** (-0.5)
    exact_scale = math.frexp(scale)[0] == 0.5
    own_heads = heads // n_far
    cols = width // n_far
    half_seqs = seqs // 2
    half = rows // 2
    waves = half_seqs // wave
    wrows = wave * props
    sources = n - 1

    pairs = (
        (tokens_hbm, tokens),
        (gain_hbm, gain),
        (gate_hbm.at[:, pl.ds(pl.multiple_of(me * depth, depth), depth)], gate_w),
        (query_hbm, query_w),
        (key_hbm, key_w),
        (value_hbm, value_w),
        (bias_hbm, bias),
        (parents_hbm, parents),
        (lengths_hbm, lengths),
        (decay_hbm, decay),
        (out_hbm, out_w),
    )
    loads = [pltpu.make_async_copy(src, dst, load_sem.at[i]) for i, (src, dst) in enumerate(pairs)]
    load_of = dict(
        zip(("tokens", "gain", "gate", "q", "k", "v", "bias", "parents", "lengths", "decay", "out"), loads)
    )
    for load in loads[:6]:
        load.start()
    barrier = pltpu.get_barrier_semaphore()
    for k in range(1, n):
        pl.semaphore_signal(barrier, inc=1, device_id={"kv": lax.rem(me + k, n)})
    for k in range(1, n_tp):
        pl.semaphore_signal(barrier, inc=1, device_id={"tp": lax.rem(tp + k, n_tp)})

    def iota(shape, dim):
        return lax.broadcasted_iota(jnp.int32, shape, dim)

    def far_id(d):
        return lax.rem(far + d, n_far)

    def near_id(z, x):
        return {"kv": z * 2 + x}

    own_half = pl.multiple_of(side * half, half)
    peer_half = pl.multiple_of((1 - side) * half, half)

    load_of["tokens"].wait()
    load_of["gain"].wait()
    for load in loads[6:]:
        load.start()
    for s in range(seqs):
        pltpu.make_async_copy(keys_hbm.at[s], keys.at[s], cache_sem.at[0, s]).start()
        pltpu.make_async_copy(values_hbm.at[s], values.at[s], cache_sem.at[1, s]).start()
    xf = tokens[...].astype(F32)
    feats[:, :depth] = (xf * gain[...]).astype(BF16)
    square = xf * xf
    high = square.astype(BF16)
    feats[:, depth : 2 * depth] = high
    feats[:, 2 * depth :] = (square - high.astype(F32)).astype(BF16)

    load_of["gate"].wait()
    t_rows = n_far * 8
    p_row = iota((t_rows, gate_w.shape[0]), 0)
    p_col = iota((t_rows, gate_w.shape[0]), 1)
    p_in = lax.rem(p_row, 8)
    wanted = (p_in < own_heads) & (p_col == tp * heads + lax.div(p_row, 8) * own_heads + p_in)
    gates = dot(wanted.astype(BF16), gate_w[...]).astype(BF16)
    ones = (lax.rem(iota((t_rows, depth), 0), 8) == own_heads).astype(BF16)
    tails = jnp.concatenate([gates, ones, ones], axis=1)

    def project_q(base, dst, which):
        full = dot(feats[pl.ds(base, half), :depth], query_w[...])
        for i in range(waves):
            piece = full[i * wrows : (i + 1) * wrows]
            tail = dot_nt(tails, feats[pl.ds(base + i * wrows, wrows), :])
            tail = jnp.concatenate([tail, jnp.zeros((t_rows, LANES - wrows), F32)], axis=1)
            for f in range(n_far):
                for at, rows_of in (
                    (slice(0, wrows), piece[:, f * cols : (f + 1) * cols]),
                    (slice(wrows, wrows + 8), tail[f * 8 : (f + 1) * 8]),
                ):
                    if i < waves - 1:
                        dst[i, f, at] = rows_of
                    else:
                        q_last[f, which, at] = rows_of

    def project_kv(base, dst):
        for which, w in enumerate((key_w, value_w)):
            full = dot(feats[pl.ds(base, half), :depth], w[...])
            for i in range(waves):
                piece = full[i * wrows : (i + 1) * wrows].astype(dst.dtype)
                for f in range(n_far):
                    dst[i, f, which * wrows : (which + 1) * wrows] = piece[:, f * cols : (f + 1) * cols]

    def x_copy(i, src, dst, send, recv):
        return pltpu.make_async_remote_copy(
            src_ref=src.at[i],
            dst_ref=dst.at[i],
            send_sem=send.at[i],
            recv_sem=recv.at[i],
            device_id=near_id(far, 1 - side),
        )

    def z_copy(i, d, src, dst, send, recv):
        return pltpu.make_async_remote_copy(
            src_ref=src.at[i, far_id(d)],
            dst_ref=dst.at[d - 1, i],
            send_sem=send.at[d - 1, i],
            recv_sem=recv.at[d - 1, i],
            device_id=near_id(far_id(d), side),
        )

    def last_copy(d):
        return pltpu.make_async_remote_copy(
            src_ref=q_last.at[far_id(d)],
            dst_ref=q_last_in.at[d - 1],
            send_sem=l_send.at[d - 1],
            recv_sem=l_recv.at[d - 1],
            device_id=near_id(far_id(d), side),
        )

    def last_cross():
        return pltpu.make_async_remote_copy(
            src_ref=q_last.at[far, 1],
            dst_ref=q_cross,
            send_sem=l_send.at[n_far - 1],
            recv_sem=l_recv.at[n_far - 1],
            device_id=near_id(far, 1 - side),
        )

    load_of["q"].wait()
    project_q(peer_half, q_out, 1)
    pl.semaphore_wait(barrier, n + n_tp - 2)
    for i in range(waves - 1):
        x_copy(i, q_out, q_in, qx_send, qx_recv).start()
    project_q(own_half, q_own, 0)
    for d in range(1, n_far):
        last_copy(d).start()
    load_of["k"].wait()
    load_of["v"].wait()
    project_kv(peer_half, kv_out)
    for i in range(waves):
        x_copy(i, kv_out, kv_in, kx_send, kx_recv).start()
    project_kv(own_half, kv_own)

    load_of["bias"].wait()
    load_of["parents"].wait()
    load_of["lengths"].wait()
    load_of["decay"].wait()
    par_pad[...] = jnp.zeros(par_pad.shape, jnp.int32)
    par_pad[0:seqs, 0:props] = parents[...]
    r_i = iota((LANES, LANES), 0)
    c_i = iota((LANES, LANES), 1)
    lane1 = iota((1, LANES), 1)
    eye = r_i == c_i
    for i in range(waves):
        row = jnp.full((1, LANES), -1, jnp.int32)
        for j in range(wave):
            of = par_pad[pl.ds(side * half_seqs + i * wave + j, 1), :]
            if j:
                of = pltpu.roll(jnp.broadcast_to(of, (8, LANES)), j * props, 1)[0:1]
            inside = (lane1 >= j * props) & (lane1 < (j + 1) * props)
            row = jnp.where(inside, of + j * props, row)
        link = ((row == r_i) | eye).astype(F32).astype(BF16)
        for _ in range(props.bit_length()):
            link = jnp.minimum(dot(link, link), 1.0).astype(BF16)
        link_s[i] = link
        anc_s[i] = dot_nt(eye.astype(F32).astype(BF16), link)
    w_row = lax.rem(iota(widen.shape, 0), LANES)
    w_col = iota(widen.shape, 1)
    w_src = lax.div(w_col, cols) * 8 + lax.div(lax.rem(w_col, cols), head_dim)
    widen[...] = (w_row == w_src).astype(F32).astype(BF16)
    b_shape = (8, bias.shape[1])
    b_row, b_col = iota(b_shape, 0), iota(b_shape, 1)
    mine = (b_row < own_heads) & (b_col == tp * heads + far * own_heads + b_row)
    bias_col = jnp.sum(jnp.where(mine, jnp.broadcast_to(bias[...], b_shape), 0.0), axis=1, keepdims=True)

    for i in range(waves - 1):
        x_copy(i, q_out, q_in, qx_send, qx_recv).wait_recv()
        q_own[i] = q_own[i] + q_in[i]
        for d in range(1, n_far):
            z_copy(i, d, q_own, q_far, qz_send, qz_recv).start()
    for d in range(1, n_far):
        last_copy(d).wait_recv()
    q_last[far] = q_last[far] + functools.reduce(jnp.add, [q_last_in[d] for d in range(n_far - 1)])
    last_cross().start()

    targets = [(d, 0) for d in range(1, n_far)] + [(d, 1) for d in range(n_far)]

    def target_id(d, cross):
        return near_id(far_id(d), side if not cross else 1 - side)

    def spread_copy(i, t, buf, send, recv):
        d, cross = targets[t]
        block = side * waves + i
        return pltpu.make_async_remote_copy(
            src_ref=buf.at[block, far],
            dst_ref=buf.at[block, far],
            send_sem=send.at[t, i],
            recv_sem=recv.at[block, far],
            device_id=target_id(d, cross),
        )

    def relay_copy(i, buf, send, recv):
        block = side * waves + i
        return pltpu.make_async_remote_copy(
            src_ref=buf.at[block],
            dst_ref=buf.at[block],
            send_sem=send.at[i],
            recv_sem=recv.at[i],
            device_id=near_id(far, 1 - side),
        )

    def spread(i, direct, buf, send, recv):
        for t in range(sources if direct else n_far - 1):
            spread_copy(i, t, buf, send, recv).start()

    def sent(i, direct, buf, send, recv, r_send, r_recv):
        for t in range(sources if direct else n_far - 1):
            spread_copy(i, t, buf, send, recv).wait_send()
        if not direct:
            relay_copy(i, buf, r_send, r_recv).wait_send()

    def spread_wait(i, t, buf, send, recv):
        d, cross = targets[t]
        block = (1 - side if cross else side) * waves + i
        pltpu.make_async_remote_copy(
            src_ref=buf.at[block, far_id(d)],
            dst_ref=buf.at[block, far_id(d)],
            send_sem=send.at[t, i],
            recv_sem=recv.at[block, far_id(d)],
            device_id=target_id(d, cross),
        ).wait_recv()

    def pass_on(i, direct, buf, send, recv, r_send, r_recv):
        for t in range(n_far - 1):
            spread_wait(i, t, buf, send, recv)
        if not direct:
            relay_copy(i, buf, r_send, r_recv).start()

    def crossed(i, direct, buf, send, recv, r_send, r_recv):
        if not direct:
            relay_copy(i, buf, r_send, r_recv).wait_recv()
            return
        for t in range(n_far - 1, sources):
            spread_wait(i, t, buf, send, recv)

    q_route = (qbuf, b_send, b_recv, qr_send, qr_recv)
    zone = n_far // 2
    place_in = lax.rem(far, zone)
    zone_of = lax.div(far, zone)
    near = [(d, 0) for d in range(1, zone)] + [(d, 1) for d in range(zone)]

    def place_at(d):
        return lax.rem(place_in + d, zone)

    def zone_id(d, cross):
        return near_id(zone_of * zone + place_at(d), 1 - side if cross else side)

    q_direct = [False] * waves

    strides = [1 << b for b in range(n_far.bit_length() - 1)]

    def halve_copy(i, st, m):
        slot = sum(n_far // (2 * x) for x in strides if x < st) + m
        partner = far + st - 2 * st * lax.rem(lax.div(far, st), 2)
        return pltpu.make_async_remote_copy(
            src_ref=kv_pass.at[i, lax.rem(partner, 2 * st) + 2 * st * m],
            dst_ref=kv_far.at[slot, i],
            send_sem=kz_send.at[slot, i],
            recv_sem=kz_recv.at[slot, i],
            device_id=near_id(partner, side),
        )

    def halve_start(i, st):
        partner = far + st - 2 * st * lax.rem(lax.div(far, st), 2)
        for m in range(n_far // (2 * st)):
            f = lax.rem(partner, 2 * st) + 2 * st * m
            kv_pass[i, f] = kv_own[i, f].astype(BF16)
            halve_copy(i, st, m).start()

    def halve_wait(i, st):
        for m in range(n_far // (2 * st)):
            halve_copy(i, st, m).wait_recv()
            f = lax.rem(far, 2 * st) + 2 * st * m
            slot = sum(n_far // (2 * x) for x in strides if x < st) + m
            kv_own[i, f] = kv_own[i, f] + kv_far[slot, i].astype(F32)

    def pass_kv(i, step):
        if step:
            halve_wait(i, strides[step - 1])
        else:
            x_copy(i, kv_out, kv_in, kx_send, kx_recv).wait_recv()
            kv_own[i] = kv_own[i] + kv_in[i].astype(F32)
        if step < len(strides):
            halve_start(i, strides[step])

    lane8 = iota((8, LANES), 1)
    row8 = iota((8, LANES), 0)

    def owner_q(i):
        if i < waves - 1:
            total = q_own[i, far]
            for d in range(1, n_far):
                z_copy(i, d, q_own, q_far, qz_send, qz_recv).wait_recv()
                total = total + q_far[d - 1, i]
        else:
            last_cross().wait_recv()
            total = q_last[far, 0] + q_cross[...]
        tail = total[wrows:]
        inverse = lax.rsqrt(tail / (depth * n) + 1e-06)
        column = tile_rows(inverse, LANES).T[:wrows, own_heads : own_heads + 1]
        inv_s[i] = jnp.broadcast_to(column, (wrows, cols))
        qbuf[side * waves + i, far] = (inv_s[i] * total[:wrows]).astype(BF16)
        spread(i, q_direct[i], qbuf, b_send, b_recv)
        inverse_row = jnp.broadcast_to(inverse[own_heads : own_heads + 1], (8, LANES))
        x = inverse_row * tail + bias_col
        log_gate = jnp.minimum(x, 0.0) - jnp.log1p(jnp.exp(-jnp.abs(x)))
        log_gate = jnp.where((row8 < own_heads) & (lane8 < wrows), log_gate, 0.0)
        parts = dot(jnp.concatenate(split3(log_gate), axis=0), link_s[i])
        path_s[i] = parts[:8] + parts[8:16] + parts[16:24]

    for i in range(waves):
        owner_q(i)
        if i < waves - 1:
            pass_kv(i, 0)

    group = min(heads, 256 // head_dim)
    gwidth = group * head_dim
    g_head = iota((group, props, gwidth), 0)
    g_col = lax.div(iota((group, props, gwidth), 2), head_dim)
    g_diag = (g_head == g_col).reshape(group * props, gwidth)
    lane_w = iota((wrows, LANES), 1)
    position = iota((heads, pos_dev), 1) + me * pos_dev

    def mix_copy(i, t, which, src, dst):
        d, cross = near[t]
        block = (1 - side if cross else side) * waves + i
        return pltpu.make_async_remote_copy(
            src_ref=src.at[block, place_at(d)],
            dst_ref=dst.at[t, i],
            send_sem=c_send.at[which, t, i],
            recv_sem=c_recv.at[which, t, i],
            device_id=zone_id(d, cross),
        )

    def attend(i, cross):
        place = 1 - side if cross else side
        block = place * waves + i
        if cross:
            crossed(i, q_direct[i], *q_route)
        first = place * half_seqs + i * wave
        for j in range(wave):
            s = first + j
            pltpu.make_async_copy(keys_hbm.at[s], keys.at[s], cache_sem.at[0, s]).wait()
            pltpu.make_async_copy(values_hbm.at[s], values.at[s], cache_sem.at[1, s]).wait()
        q_wave = jnp.concatenate([qbuf[block, f] for f in range(n_far)], axis=1).astype(F32)
        if exact_scale:
            q_wave = q_wave * scale
        chains = [(j, g) for j in range(wave) for g in range(heads // group)]
        scores_of, w_of, tops, totals, parts = {}, {}, {}, {}, {}
        for j in range(wave):
            s = first + j
            fade = jnp.where(position < lengths[s], decay[s], LOW)
            for g in range(heads // group):
                q = q_wave[j * props : (j + 1) * props, g * gwidth : (g + 1) * gwidth]
                q = jnp.broadcast_to(q[None], (group, props, gwidth)).reshape(group * props, gwidth)
                q = jnp.where(g_diag, q, 0.0).astype(BF16)
                scores = dot_nt(q, keys[s, :, g * gwidth : (g + 1) * gwidth])
                if not exact_scale:
                    scores = scores * scale
                fades = [
                    jnp.broadcast_to(fade[h : h + 1], (props, pos_dev))
                    for h in range(g * group, (g + 1) * group)
                ]
                scores_of[j, g] = scores + jnp.concatenate(fades, axis=0)
        for j, g in chains:
            top = jnp.max(scores_of[j, g], axis=1, keepdims=True)
            w = jnp.exp(scores_of[j, g] - top)
            total = jnp.sum(w, axis=1, keepdims=True)
            w_of[j, g] = w.astype(BF16)
            for h in range(group):
                tops[j, g * group + h] = top[h * props : (h + 1) * props]
                totals[j, g * group + h] = total[h * props : (h + 1) * props]
        for j, g in chains:
            m = dot(w_of[j, g], values[first + j, :, g * gwidth : (g + 1) * gwidth])
            m = jnp.where(g_diag, m, 0.0).reshape(group, props, gwidth)
            parts[j, g] = jnp.sum(m, axis=0)
        mixes = [
            jnp.concatenate([parts[j, g] for g in range(heads // group)], axis=1) for j in range(wave)
        ]
        mixed = jnp.concatenate(mixes, axis=0).astype(BF16)
        for f in range(n_far):
            mix[block, f % zone, f // zone] = mixed[:, f * cols : (f + 1) * cols]
        acc = jnp.zeros((wrows, LANES), F32)
        for h in range(heads):
            f, k = divmod(h, own_heads)
            for at, cols_of in ((k, tops), (own_heads + k, totals)):
                col = jnp.concatenate([cols_of[j, h] for j in range(wave)], axis=0)
                acc = jnp.where(lane_w == f * 8 + at, col, acc)
        flat = tile_rows(acc, LANES).T
        for f in range(n_far):
            stat[block, f % zone, f // zone] = flat[f * 8 : f * 8 + stat.shape[3]]
        for t in range(len(near)):
            if near[t][1] == cross:
                mix_copy(i, t, 0, mix, mix_in).start()
                mix_copy(i, t, 1, stat, stat_in).start()

    own_head_of = lax.div(iota((wrows, cols), 1), head_dim)

    def tree(i):
        block = side * waves + i
        pass_kv(i, len(strides))
        total = kv_own[i, far]
        new_k = tile_rows(inv_s[i] * total[:wrows], LANES).astype(BF16)
        new_v = tile_rows(inv_s[i] * total[wrows:], LANES).astype(BF16)
        q = qbuf[block, far].astype(F32)
        q = jnp.concatenate([jnp.where(own_head_of == h, q, 0.0) for h in range(own_heads)], axis=0)
        scores = dot_nt(q.astype(BF16), new_k) * scale
        path = path_s[i]
        shifts = [jnp.broadcast_to(-path[h : h + 1], (wrows, LANES)) for h in range(own_heads)]
        scores = scores + jnp.concatenate(shifts, axis=0)
        live = jnp.concatenate([anc_s[i, :wrows]] * own_heads, axis=0) > 0.5
        scores = jnp.where(live, scores, LOW)
        top = jnp.max(scores, axis=1, keepdims=True)
        w = jnp.where(live, jnp.exp(scores - top), 0.0)
        total = jnp.sum(w, axis=1, keepdims=True)
        m = dot(w.astype(BF16), new_v)
        merged = jnp.zeros((wrows, cols), F32)
        acc = jnp.zeros((wrows, LANES), F32)
        for h in range(own_heads):
            part = slice(h * wrows, (h + 1) * wrows)
            merged = jnp.where(own_head_of == h, m[part], merged)
            acc = jnp.where(lane_w == h, top[part], acc)
            acc = jnp.where(lane_w == own_heads + h, total[part], acc)
        tmix[i] = merged
        tstat[i] = tile_rows(acc, LANES).T[:8]

    def swap_copy(i, which, src, dst):
        return pltpu.make_async_remote_copy(
            src_ref=src.at[i],
            dst_ref=dst.at[i],
            send_sem=s_send.at[which, i],
            recv_sem=s_recv.at[which, i],
            device_id=near_id((1 - zone_of) * zone + place_in, side),
        )

    def turn(tiles):
        flat = jnp.concatenate([jnp.where(row8 < own_heads, x, 0.0) for x in tiles], axis=0)
        turned = tile_rows(flat, LANES).T[:wrows]
        high = turned.astype(BF16)
        low = (turned - high.astype(F32)).astype(BF16)
        both = jnp.concatenate([high, low], axis=1)
        return dot(both, widen[:, : len(tiles) * cols])

    def lift(st):
        return pltpu.roll(st, 8 - own_heads, 0)

    def weigh(wide, first, parts):
        total = jnp.zeros((wrows, cols), F32)
        for k, m in enumerate(parts):
            at = (first + k) * cols
            total = total + wide[:, at : at + cols] * m.astype(F32)
        return total

    def merge(i):
        block = side * waves + i
        for t in range(len(near)):
            mix_copy(i, t, 0, mix, mix_in).wait_recv()
            mix_copy(i, t, 1, stat, stat_in).wait_recv()
        tiles = []
        for k in range(2):
            stats = [stat[block, place_in, k]] + [stat_in[t, i, k] for t in range(len(near))]
            stats = [tile_rows(st, 8) for st in stats]
            absent = jnp.where(row8 < own_heads, LOW, 0.0)
            stats.append(jnp.where(zone_of == k, tstat[i], absent))
            best = functools.reduce(jnp.maximum, stats)
            factors = [jnp.exp(st - best) for st in stats]
            total = functools.reduce(jnp.add, [f * lift(st) for f, st in zip(factors, stats)])
            packed = jnp.where(row8 < own_heads, best, pltpu.roll(total, own_heads, 0))
            swap_stat[i, k] = packed[: swap_stat.shape[2]]
            tiles += factors
        wide = turn(tiles)
        for k in range(2):
            parts = [mix[block, place_in, k]] + [mix_in[t, i, k] for t in range(len(near))] + [tmix[i]]
            held[i, k] = weigh(wide, k * len(parts), parts)
            swap[i, k] = held[i, k].astype(BF16)
        swap_copy(i, 0, swap, swap_in).start()
        swap_copy(i, 1, swap_stat, swap_stat_in).start()

    def att_copy(i, t, block, place):
        d, cross = near[t]
        return pltpu.make_async_remote_copy(
            src_ref=att.at[block, place],
            dst_ref=att.at[block, place],
            send_sem=d_send.at[t, i],
            recv_sem=d_recv.at[block, place],
            device_id=zone_id(d, cross),
        )

    def finish(i):
        block = side * waves + i
        swap_copy(i, 0, swap, swap_in).wait_recv()
        swap_copy(i, 1, swap_stat, swap_stat_in).wait_recv()
        tiles = []
        for k in range(2):
            stats = [tile_rows(st[i, k], 8) for st in (swap_stat, swap_stat_in)]
            best = jnp.maximum(stats[0], stats[1])
            factors = [jnp.exp(st - best) for st in stats]
            denom = functools.reduce(jnp.add, [f * lift(st) for f, st in zip(factors, stats)])
            tiles += [f / denom for f in factors]
        wide = turn(tiles)
        for k in range(2):
            att[block, place_in, k] = weigh(wide, 2 * k, (held[i, k], swap_in[i, k])).astype(BF16)
        for t in range(len(near)):
            att_copy(i, t, block, place_in).start()

    per_tp = seqs // n_tp

    def e_copy(s, t):
        k = jnp.maximum(lax.rem(tp - t + n_tp, n_tp) - 1, 0)
        return pltpu.make_async_remote_copy(
            src_ref=terms.at[s],
            dst_ref=terms_in.at[k, lax.rem(s, per_tp)],
            send_sem=e_send.at[s],
            recv_sem=e_recv.at[k, lax.rem(s, per_tp)],
            device_id={"tp": t},
        )

    def output(i, cross):
        place = 1 - side if cross else side
        block = place * waves + i
        for t, (d, over) in enumerate(near):
            if over == cross:
                att_copy(i, t, block, place_at(d)).wait_recv()
        attended = jnp.concatenate([att[block, f % zone, f // zone] for f in range(n_far)], axis=1)
        term = dot(attended, out_w[...])
        for j in range(wave):
            s = place * half_seqs + i * wave + j
            terms[s] = fold(term[j * props : (j + 1) * props]).astype(BF16)
            t = lax.div(s, per_tp)
            pl.when(tp != t)(e_copy(s, t).start)

    advanced = [0] * waves

    def advance(count):
        for i in range(waves):
            if count and advanced[i] + 1 < len(strides):
                advanced[i] += 1
                pass_kv(i, advanced[i])
                count -= 1

    pass_on(0, q_direct[0], *q_route)
    attend(0, 0)
    pass_kv(waves - 1, 0)
    advance(1)
    for i in range(1, waves):
        pass_on(i, q_direct[i], *q_route)
        if i == 1:
            attend(1, 0)
            advance(1)
    attend(0, 1)
    advance(1)
    for i in range(1, waves):
        attend(i, 1)
    for i in range(2, waves):
        attend(i, 0)
    advance(waves * len(strides))
    load_of["out"].wait()
    for i in range(waves):
        tree(i)
        merge(i)
    for i in range(waves):
        finish(i)
    for i in range(waves):
        output(i, 0)
        output(i, 1)

    done = []
    for j in range(per_tp):
        total = unfold(terms[tp * per_tp + j])
        for k in range(1, n_tp):
            pltpu.make_async_remote_copy(
                src_ref=terms.at[0],
                dst_ref=terms_in.at[k - 1, j],
                send_sem=e_send.at[0],
                recv_sem=e_recv.at[k - 1, j],
                device_id={"tp": lax.rem(tp + k, n_tp)},
            ).wait_recv()
            total = total + unfold(terms_in[k - 1, j])
        done.append(total)
    out[...] = jnp.concatenate(done, axis=0).astype(BF16)

    for i in range(waves):
        if i < waves - 1:
            x_copy(i, q_out, q_in, qx_send, qx_recv).wait_send()
            for d in range(1, n_far):
                z_copy(i, d, q_own, q_far, qz_send, qz_recv).wait_send()
        x_copy(i, kv_out, kv_in, kx_send, kx_recv).wait_send()
        for st in strides:
            for m in range(n_far // (2 * st)):
                halve_copy(i, st, m).wait_send()
        sent(i, q_direct[i], *q_route)
        swap_copy(i, 0, swap, swap_in).wait_send()
        swap_copy(i, 1, swap_stat, swap_stat_in).wait_send()
        for t in range(len(near)):
            att_copy(i, t, side * waves + i, place_in).wait_send()
            mix_copy(i, t, 0, mix, mix_in).wait_send()
            mix_copy(i, t, 1, stat, stat_in).wait_send()
    for d in range(1, n_far):
        last_copy(d).wait_send()
    last_cross().wait_send()
    for s in range(seqs):
        t = s // per_tp
        pl.when(tp != t)(e_copy(s, t).wait_send)


def wave_size(n, n_tp, seqs, props, heads, width):
    n_far = n // 2
    if n < 4 or n & (n - 1) or seqs % 2 or seqs % n_tp or heads % n_far or width % (n_far * LANES):
        return 0
    head_dim = width // heads
    own = heads // n_far
    if own > 4 or 16 * (n_far + 1) > LANES or (heads % min(heads, max(256 // head_dim, 1))):
        return 0
    for wave in range(1, seqs // 2 + 1):
        fits = wave * props % 16 == 0 and wave * props <= LANES
        if seqs // 2 % wave == 0 and fits and props % 8 == 0:
            return wave
    return 0


def solution(mesh):
    n, n_tp = mesh.shape["kv"], mesh.shape["tp"]

    def body(
        tokens,
        norm_gain,
        query_weight,
        key_weight,
        value_weight,
        gate_weight,
        gate_bias,
        out_weight,
        cache_keys,
        cache_values,
        cache_decay,
        lengths,
        parents,
    ):
        rows, depth = tokens.shape
        seqs, props = parents.shape
        heads = cache_decay.shape[1]
        pos_dev = cache_keys.shape[1]
        width = query_weight.shape[1]
        cols = out_weight.shape[1]
        slots = -(-seqs // n)
        block = rows // n_tp
        all_w = 2 * width + LANES
        folded = (2 * props, width // 2)
        vmem = pl.BlockSpec(memory_space=pltpu.VMEM)
        hbm = pl.BlockSpec(memory_space=pltpu.HBM)
        dma = pltpu.SemaphoreType.DMA
        wave = wave_size(n, n_tp, seqs, props, heads, width)
        if wave:
            n_far = n // 2
            waves = seqs // 2 // wave
            q_waves = max(waves - 1, 1)
            zone = n_far // 2
            wrows = wave * props
            wcols = width // n_far
            per_tp = seqs // n_tp
            s_rows = max(4, 2 * (heads // n_far))
            block_q = (n_far, wrows + 8, wcols)
            block_kv = (n_far, 2 * wrows, wcols)
            body_of = functools.partial(by_heads, n, n_tp, wave)
            scratch = [
                pltpu.VMEM(tokens.shape, BF16),
                pltpu.VMEM((1, depth), F32),
                pltpu.VMEM(query_weight.shape, BF16),
                pltpu.VMEM(key_weight.shape, BF16),
                pltpu.VMEM(value_weight.shape, BF16),
                pltpu.VMEM((gate_weight.shape[1], depth), BF16),
                pltpu.VMEM((1, gate_bias.shape[0]), F32),
                pltpu.VMEM(cache_decay.shape, F32),
                pltpu.SMEM(lengths.shape, jnp.int32),
                pltpu.VMEM(parents.shape, jnp.int32),
                pltpu.VMEM(out_weight.shape, BF16),
                pltpu.VMEM(cache_keys.shape, BF16),
                pltpu.VMEM(cache_values.shape, BF16),
                pltpu.VMEM((rows, 3 * depth), BF16),
                pltpu.VMEM((q_waves,) + block_q, F32),
                pltpu.VMEM((q_waves,) + block_q, F32),
                pltpu.VMEM((q_waves,) + block_q, F32),
                pltpu.VMEM((n_far - 1, q_waves) + block_q[1:], F32),
                pltpu.VMEM((n_far, 2) + block_q[1:], F32),
                pltpu.VMEM((n_far - 1, 2) + block_q[1:], F32),
                pltpu.VMEM(block_q[1:], F32),
                pltpu.VMEM((waves,) + block_kv, BF16),
                pltpu.VMEM((waves,) + block_kv, BF16),
                pltpu.VMEM((waves,) + block_kv, F32),
                pltpu.VMEM((waves,) + block_kv, BF16),
                pltpu.VMEM((n_far - 1, waves) + block_kv[1:], BF16),
                pltpu.VMEM((2 * waves, n_far, wrows, wcols), BF16),
                pltpu.VMEM((2 * waves, zone, 2, wrows, wcols), BF16),
                pltpu.VMEM((n_far - 1, waves, 2, wrows, wcols), BF16),
                pltpu.VMEM((2 * waves, zone, 2, s_rows, LANES), F32),
                pltpu.VMEM((n_far - 1, waves, 2, s_rows, LANES), F32),
                pltpu.VMEM((2 * waves, zone, 2, wrows, wcols), BF16),
                pltpu.VMEM((seqs,) + folded, BF16),
                pltpu.VMEM((n_tp - 1, per_tp) + folded, BF16),
                pltpu.VMEM((-(-seqs // 8) * 8, LANES), jnp.int32),
                pltpu.VMEM((waves, LANES, LANES), BF16),
                pltpu.VMEM((waves, LANES, LANES), F32),
                pltpu.VMEM((waves, 8, LANES), F32),
                pltpu.VMEM((waves, wrows, wcols), F32),
                pltpu.VMEM((waves, wrows, wcols), F32),
                pltpu.VMEM((waves, 8, LANES), F32),
                pltpu.VMEM((waves, 2, wrows, wcols), F32),
                pltpu.VMEM((waves, 2, wrows, wcols), BF16),
                pltpu.VMEM((waves, 2, wrows, wcols), BF16),
                pltpu.VMEM((waves, 2, s_rows, LANES), F32),
                pltpu.VMEM((waves, 2, s_rows, LANES), F32),
                pltpu.VMEM((2 * LANES, 2 * (n_far + 1) * wcols), BF16),
                dma((11,)),
                dma((2, seqs)),
                dma((waves,)),
                dma((waves,)),
                dma((waves,)),
                dma((waves,)),
                dma((n_far - 1, waves)),
                dma((n_far - 1, waves)),
                dma((n_far - 1, waves)),
                dma((n_far - 1, waves)),
                dma((n - 1, waves)),
                dma((2 * waves, n_far)),
                dma((2, n_far - 1, waves)),
                dma((2, n_far - 1, waves)),
                dma((n_far - 1, waves)),
                dma((2 * waves, zone)),
                dma((seqs,)),
                dma((n_tp - 1, per_tp)),
                dma((waves,)),
                dma((waves,)),
                dma((2, waves)),
                dma((2, waves)),
                dma((n_far,)),
                dma((n_far,)),
            ]
        else:
            body_of = functools.partial(by_sequence, n, n_tp)
            scratch = [
                pltpu.VMEM(tokens.shape, BF16),
                pltpu.VMEM((1, depth), F32),
                pltpu.VMEM(query_weight.shape, BF16),
                pltpu.VMEM(key_weight.shape, BF16),
                pltpu.VMEM(value_weight.shape, BF16),
                pltpu.VMEM((1, gate_bias.shape[0]), F32),
                pltpu.VMEM(cache_decay.shape, F32),
                pltpu.SMEM(lengths.shape, jnp.int32),
                pltpu.VMEM(parents.shape, jnp.int32),
                dma((9,)),
                pltpu.VMEM((seqs, props, all_w), F32),
                pltpu.VMEM((seqs,) + folded, BF16),
                pltpu.VMEM((seqs, props, all_w), F32),
                pltpu.VMEM((seqs,) + folded, BF16),
                pltpu.VMEM((n // 2 - 1, slots, props, all_w), F32),
                pltpu.VMEM((n // 2 - 1, slots) + folded, BF16),
                pltpu.VMEM((gate_weight.shape[1], depth), BF16),
                pltpu.VMEM(out_weight.shape, BF16),
                pltpu.VMEM(cache_keys.shape, BF16),
                pltpu.VMEM(cache_values.shape, BF16),
                pltpu.VMEM((seqs,) + folded, BF16),
                pltpu.VMEM((seqs,) + folded, BF16),
                pltpu.VMEM((seqs, props, LANES), F32),
                pltpu.VMEM((n - 1, slots) + folded, BF16),
                pltpu.VMEM((n - 1, slots, props, LANES), F32),
                pltpu.VMEM((seqs,) + folded, BF16),
                pltpu.VMEM((slots, props, LANES), F32),
                pltpu.VMEM((slots, props, LANES), F32),
                pltpu.VMEM((slots, props, width), F32),
                pltpu.VMEM((slots, 2, props, LANES), F32),
                pltpu.VMEM((slots, 2, LANES, width), F32),
                pltpu.VMEM((n_tp, block, cols), BF16),
                pltpu.VMEM((n_tp - 1, block, cols), BF16),
                pltpu.VMEM((-(-seqs // 8) * 8, LANES), jnp.int32),
                dma((2,)),
                dma((2, seqs)),
                dma((2, seqs)),
                dma((2, seqs)),
                dma((2, seqs)),
                dma((2, n // 2 - 1, slots)),
                dma((slots, n - 1)),
                dma((seqs,)),
                dma((2, seqs)),
                dma((2, n - 1, slots)),
                dma((slots, n - 1)),
                dma((seqs,)),
                dma((n_tp,)),
                dma((n_tp - 1,)),
            ]
        return pl.pallas_call(
            body_of,
            out_shape=pltpu.VMEM((block, cols), BF16),
            in_specs=[hbm] * 13,
            out_specs=vmem,
            scratch_shapes=scratch,
            compiler_params=pltpu.CompilerParams(
                collective_id=0, has_side_effects=True, vmem_limit_bytes=67_043_328 - 131072
            ),
        )(
            tokens,
            norm_gain.reshape(1, depth),
            query_weight,
            key_weight,
            value_weight,
            gate_weight.T,
            gate_bias.reshape(1, gate_bias.shape[0]),
            out_weight,
            cache_keys,
            cache_values,
            cache_decay,
            lengths,
            parents,
        )

    in_specs = (
        P(None, "kv"),
        P("kv"),
        P("kv", "tp"),
        P("kv", "tp"),
        P("kv", "tp"),
        P(),
        P(),
        P("tp", "kv"),
        P(None, "kv", "tp"),
        P(None, "kv", "tp"),
        P(None, "tp", "kv"),
        P(),
        P(),
    )
    out_specs = P("tp", "kv")
    return jax.shard_map(body, mesh=mesh, in_specs=in_specs, out_specs=out_specs, check_vma=False)
```

```python
import functools
import math

import jax
import jax.numpy as jnp
from jax import lax
from jax.experimental import pallas as pl
from jax.experimental.pallas import tpu as pltpu
from jax.sharding import PartitionSpec as P

F32 = jnp.float32
BF16 = jnp.bfloat16
LANES = 128
LOW = -1e30
NT = (((1,), (1,)), ((), ()))
HIGH = lax.Precision.HIGHEST


def dot(a, b, precision=None):
    return jnp.dot(a, b, preferred_element_type=F32, precision=precision)


def dot_nt(a, b, precision=None):
    return lax.dot_general(a, b, NT, preferred_element_type=F32, precision=precision)


def fold(x):
    half = x.shape[1] // 2
    return jnp.concatenate([x[:, :half], x[:, half:]], axis=0)


def unfold(x):
    rows = x.shape[0] // 2
    x = x.astype(F32)
    return jnp.concatenate([x[:rows], x[rows:]], axis=1)


def by_sequence(
    n,
    n_tp,
    tokens_hbm,
    gain_hbm,
    query_hbm,
    key_hbm,
    value_hbm,
    gate_hbm,
    bias_hbm,
    out_hbm,
    keys_hbm,
    values_hbm,
    decay_hbm,
    lengths_hbm,
    parents_hbm,
    out,
    tokens,
    gain,
    query_w,
    key_w,
    value_w,
    bias,
    decay,
    lengths,
    parents,
    small_sem,
    part,
    part_v,
    pair_in,
    pair_in_v,
    part_in,
    part_in_v,
    gate_w,
    out_w,
    keys,
    values,
    qbuf,
    mix,
    stat,
    mix_in,
    stat_in,
    att,
    anc,
    path_s,
    tmix,
    tstat,
    kvnew,
    terms,
    terms_in,
    par_pad,
    load_sem,
    cache_sem,
    p_send,
    p_recv,
    a_send,
    a_recv,
    b_send,
    b_recv,
    c_send,
    c_recv,
    d_send,
    d_recv,
    e_send,
    e_recv,
):
    me = lax.axis_index("kv")
    tp = lax.axis_index("tp")
    rows, depth = tokens.shape
    seqs, props = parents.shape
    heads = decay.shape[1]
    pos_dev = keys.shape[1]
    width = query_w.shape[1]
    head_dim = width // heads
    scale = head_dim ** (-0.5)
    slots = part_in.shape[1]
    parity = lax.rem(tp, 2)
    left_over = seqs % n
    hp = heads * props

    barrier = pltpu.get_barrier_semaphore()
    for k in range(1, n):
        pl.semaphore_signal(barrier, inc=1, device_id={"kv": lax.rem(me + k, n)})
    for k in range(1, n_tp):
        pl.semaphore_signal(barrier, inc=1, device_id={"tp": lax.rem(tp + k, n_tp)})

    pairs = (
        (tokens_hbm, tokens),
        (gain_hbm, gain),
        (query_hbm, query_w),
        (key_hbm, key_w),
        (value_hbm, value_w),
        (bias_hbm, bias),
        (parents_hbm, parents),
        (decay_hbm, decay),
        (lengths_hbm, lengths),
    )
    small_loads = [
        pltpu.make_async_copy(src, dst, small_sem.at[i]) for i, (src, dst) in enumerate(pairs)
    ]
    for load in small_loads:
        load.start()
    gate_load = pltpu.make_async_copy(
        gate_hbm.at[:, pl.ds(pl.multiple_of(me * depth, depth), depth)], gate_w, load_sem.at[0]
    )
    gate_load.start()
    cache_loads = []
    for s in range(seqs):
        k_load = pltpu.make_async_copy(keys_hbm.at[s], keys.at[s], cache_sem.at[0, s])
        v_load = pltpu.make_async_copy(values_hbm.at[s], values.at[s], cache_sem.at[1, s])
        k_load.start()
        v_load.start()
        cache_loads.append((k_load, v_load))
    out_load = pltpu.make_async_copy(out_hbm, out_w, load_sem.at[1])
    out_load.start()

    def owner_of(s):
        if isinstance(s, int):
            place = s % n
            shift = parity * left_over if s // n == seqs // n else 0
        else:
            place = lax.rem(s, n)
            shift = jnp.where(lax.div(s, n) == seqs // n, parity * left_over, 0)
        return lax.rem(place + shift, n)

    def slot_seq(r):
        shift = parity * left_over if r == seqs // n else 0
        return r * n + lax.rem(me + 2 * n - shift, n)

    def for_slot(r, f):
        if (r + 1) * n <= seqs:
            f()
        else:
            pl.when(slot_seq(r) < seqs)(f)

    for load in small_loads:
        load.wait()
    xf = tokens[...].astype(F32)
    squares = jnp.sum(xf * xf, axis=1, keepdims=True)
    normed = (xf * gain[...]).astype(BF16)
    sel_rows = lax.broadcasted_iota(jnp.int32, (bias.shape[1], LANES), 0)
    sel_cols = lax.broadcasted_iota(jnp.int32, (bias.shape[1], LANES), 1)
    select = ((sel_rows == sel_cols + tp * heads) & (sel_cols < heads)).astype(F32)
    for i, w in enumerate((query_w, key_w)):
        part[:, :, i * width : (i + 1) * width] = dot(normed, w[...]).reshape(seqs, props, width)
    value_part = dot(normed, value_w[...])
    for s in range(seqs):
        part_v[s] = fold(value_part[s * props : (s + 1) * props]).astype(BF16)
    gate_load.wait()
    gates_w = lax.dot_general(
        select.astype(BF16), gate_w[...], (((0,), (0,)), ((), ())), preferred_element_type=F32
    )
    gate_part = dot_nt(normed, gates_w.astype(BF16))
    lane = lax.broadcasted_iota(jnp.int32, (rows, LANES), 1)
    gate_part = jnp.where(lane == LANES // 2, squares, gate_part)
    part[:, :, 2 * width :] = gate_part.reshape(seqs, props, LANES)
    pl.semaphore_wait(barrier, n + n_tp - 2)

    side = lax.rem(me, 2)
    partner = me + 1 - 2 * side
    n_far = n // 2
    shares = ((part, pair_in, part_in), (part_v, pair_in_v, part_in_v))

    def p_copy(s, which):
        src, dst, _ = shares[which]
        return pltpu.make_async_remote_copy(
            src_ref=src.at[s],
            dst_ref=dst.at[s],
            send_sem=p_send.at[which, s],
            recv_sem=p_recv.at[which, s],
            device_id={"kv": partner},
        )

    def a_copy(s, which):
        src, _, dst = shares[which]
        d = owner_of(s)
        k = jnp.maximum(lax.rem(lax.div(me, 2) - lax.div(d, 2) + n_far, n_far) - 1, 0)
        return pltpu.make_async_remote_copy(
            src_ref=src.at[s],
            dst_ref=dst.at[k, s // n],
            send_sem=a_send.at[which, s],
            recv_sem=a_recv.at[which, k, s // n],
            device_id={"kv": d},
        )

    def crosses(s):
        return lax.rem(owner_of(s), 2) != side

    def passes(s):
        d = owner_of(s)
        return (lax.rem(d, 2) == side) & (d != me)

    for s in range(seqs):
        for which in range(2):
            pl.when(crosses(s))(p_copy(s, which).start)

    par_pad[...] = jnp.zeros(par_pad.shape, jnp.int32)
    par_pad[0:seqs, 0:props] = parents[...]
    r_i = lax.broadcasted_iota(jnp.int32, (LANES, LANES), 0)
    c_i = lax.broadcasted_iota(jnp.int32, (LANES, LANES), 1)
    eye = (r_i == c_i).astype(F32)
    bias_row = dot(jnp.broadcast_to(bias[...], (8, bias.shape[1])), select, HIGH)[0:1]

    def ancestry(r):
        s = slot_seq(r)
        row = par_pad[pl.ds(s, 1), :]
        link = jnp.maximum((row == r_i).astype(F32), eye).astype(BF16)
        for _ in range(props.bit_length()):
            link = jnp.minimum(dot(link, link), 1.0).astype(BF16)
        anc[r] = dot_nt(eye.astype(BF16), link)[:props]

    for r in range(slots):
        for_slot(r, functools.partial(ancestry, r))

    def pass_on(s):
        for which in range(2):
            p_copy(s, which).wait_recv()
        part[s] = part[s] + pair_in[s]
        part_v[s] = (part_v[s].astype(F32) + pair_in_v[s].astype(F32)).astype(BF16)
        for which in range(2):
            a_copy(s, which).start()

    for s in range(seqs):
        pl.when(passes(s))(functools.partial(pass_on, s))

    lane_p = lax.broadcasted_iota(jnp.int32, (props, LANES), 1)
    bd_row = lax.broadcasted_iota(jnp.int32, (heads, props, width), 0)
    bd_col = lax.broadcasted_iota(jnp.int32, (heads, props, width), 2)
    diag = (lax.div(bd_col, head_dim) == bd_row).reshape(hp, width)

    def spread(q):
        wide = jnp.broadcast_to(q[None], (heads, props, width)).reshape(hp, width)
        return jnp.where(diag, wide, 0.0).astype(BF16)

    def gather_diag(m):
        return jnp.sum(jnp.where(diag, m, 0.0).reshape(heads, props, width), axis=0)

    def to_lanes(col, first):
        acc = jnp.zeros((props, LANES), F32)
        for h in range(heads):
            acc = jnp.where(lane_p == h + first, col[h * props : (h + 1) * props], acc)
        return acc

    def b_copy(r, k, buf, send, recv):
        s = slot_seq(r)
        return pltpu.make_async_remote_copy(
            src_ref=buf.at[s],
            dst_ref=buf.at[s],
            send_sem=send.at[r, k - 1],
            recv_sem=recv.at[s],
            device_id={"kv": lax.rem(me + k, n)},
        )

    pad_rows = LANES - props

    def project(r):
        s = slot_seq(r)
        for which, (src, near, far) in enumerate(shares):
            pltpu.make_async_remote_copy(
                src_ref=src.at[0],
                dst_ref=near.at[s],
                send_sem=p_send.at[which, 0],
                recv_sem=p_recv.at[which, s],
                device_id={"kv": partner},
            ).wait_recv()
            for k in range(1, n_far):
                pltpu.make_async_remote_copy(
                    src_ref=src.at[0],
                    dst_ref=far.at[k - 1, r],
                    send_sem=a_send.at[which, 0],
                    recv_sem=a_recv.at[which, k - 1, r],
                    device_id={"kv": lax.rem(me + 2 * k, n)},
                ).wait_recv()
        total = part[s] + pair_in[s]
        total_v = unfold(part_v[s]) + unfold(pair_in_v[s])
        for k in range(1, n_far):
            total = total + part_in[k - 1, r]
            total_v = total_v + unfold(part_in_v[k - 1, r])
        tail = total[:, 2 * width :]
        square = jnp.sum(jnp.where(lane_p == LANES // 2, tail, 0.0), axis=1, keepdims=True)
        inverse = lax.rsqrt(square / (depth * n) + 1e-06)
        q = inverse * total[:, :width]
        qbuf[s] = fold(q).astype(BF16)
        for k in range(1, n):
            b_copy(r, k, qbuf, b_send, b_recv).start()
        kvnew[r, 0, 0:props] = inverse * total[:, width : 2 * width]
        kvnew[r, 1, 0:props] = inverse * total_v
        kvnew[r, :, props:] = jnp.zeros((2, pad_rows, width), F32)
        x = inverse * tail + bias_row
        log_gate = jnp.minimum(x, 0.0) - jnp.log1p(jnp.exp(-jnp.abs(x)))
        padded = jnp.concatenate([log_gate, jnp.zeros((pad_rows, LANES), F32)], axis=0)
        path_s[r] = dot(anc[r], padded, HIGH)

    def tree(r):
        s = slot_seq(r)
        path = path_s[r]
        q = spread(unfold(qbuf[s]))
        head_of = lax.broadcasted_iota(jnp.int32, (heads, props, LANES), 0)
        lane_of = lax.broadcasted_iota(jnp.int32, (heads, props, LANES), 2)
        pick = (head_of == lane_of).reshape(hp, LANES)
        tiled = jnp.broadcast_to(path[None], (heads, props, LANES)).reshape(hp, LANES)
        own = jnp.sum(jnp.where(pick, tiled, 0.0), axis=1, keepdims=True)
        padded = jnp.concatenate([path, jnp.zeros((pad_rows, LANES), F32)], axis=0)
        other = dot_nt(pick.astype(F32), padded, HIGH)
        scores = dot_nt(q, kvnew[r, 0].astype(BF16)) * scale + own - other
        live = jnp.broadcast_to(anc[r][None], (heads, props, LANES)).reshape(hp, LANES) > 0.5
        scores = jnp.where(live, scores, LOW)
        top = jnp.max(scores, axis=1, keepdims=True)
        w = jnp.where(live, jnp.exp(scores - top), 0.0)
        total = jnp.sum(w, axis=1, keepdims=True)
        tmix[r] = gather_diag(dot(w.astype(BF16), kvnew[r, 1].astype(BF16)))
        tstat[r, 0] = to_lanes(top, 0)
        tstat[r, 1] = to_lanes(total, 0)

    position = lax.broadcasted_iota(jnp.int32, (hp, pos_dev), 1) + me * pos_dev

    def c_copy(s, which, src, dst):
        d = owner_of(s)
        k = jnp.maximum(lax.rem(me - d + n, n) - 1, 0)
        slot = s // n if isinstance(s, int) else lax.div(s, n)
        return d, pltpu.make_async_remote_copy(
            src_ref=src.at[s],
            dst_ref=dst.at[k, slot],
            send_sem=c_send.at[which, s],
            recv_sem=c_recv.at[which, k, slot],
            device_id={"kv": d},
        )

    def shard(s, carry):
        d = owner_of(s)

        @pl.when(d != me)
        def _():
            pltpu.make_async_remote_copy(
                src_ref=qbuf.at[s],
                dst_ref=qbuf.at[s],
                send_sem=b_send.at[0, 0],
                recv_sem=b_recv.at[s],
                device_id={"kv": d},
            ).wait_recv()

        pltpu.make_async_copy(keys_hbm.at[s], keys.at[s], cache_sem.at[0, s]).wait()
        pltpu.make_async_copy(values_hbm.at[s], values.at[s], cache_sem.at[1, s]).wait()
        q = spread(unfold(qbuf[s]))
        fade = decay[s]
        fade = jnp.concatenate(
            [jnp.broadcast_to(fade[h : h + 1], (props, pos_dev)) for h in range(heads)], axis=0
        )
        scores = dot_nt(q, keys[s]) * scale + fade
        live = position < lengths[s]
        scores = jnp.where(live, scores, LOW)
        top = jnp.max(scores, axis=1, keepdims=True)
        w = jnp.where(live, jnp.exp(scores - top), 0.0)
        total = jnp.sum(w, axis=1, keepdims=True)
        mix[s] = fold(gather_diag(dot(w.astype(BF16), values[s]))).astype(BF16)
        stat[s] = to_lanes(top, 0) + to_lanes(total, heads)
        for which, (src, dst) in enumerate(((mix, mix_in), (stat, stat_in))):
            _, copy = c_copy(s, which, src, dst)
            pl.when(d != me)(copy.start)
        return carry

    ex_r = lax.broadcasted_iota(jnp.int32, (LANES, width), 0)
    ex_c = lax.broadcasted_iota(jnp.int32, (LANES, width), 1)
    widen = (ex_r == lax.div(ex_c, head_dim)).astype(F32)

    def merge(r):
        s = slot_seq(r)
        for k in range(1, n):
            for which, (src, dst) in enumerate(((mix, mix_in), (stat, stat_in))):
                pltpu.make_async_remote_copy(
                    src_ref=src.at[0],
                    dst_ref=dst.at[k - 1, r],
                    send_sem=c_send.at[which, 0],
                    recv_sem=c_recv.at[which, k - 1, r],
                    device_id={"kv": lax.rem(me + k, n)},
                ).wait_recv()
        stats = jnp.concatenate([stat[s]] + [stat_in[k, r] for k in range(n - 1)], axis=0)
        totals = pltpu.roll(stats, LANES - heads, 1).reshape(n, props, LANES)
        tops = stats.reshape(n, props, LANES) + path_s[r][None]
        tops = jnp.where((lane_p < heads)[None], tops, LOW)
        ttop = jnp.where(lane_p < heads, tstat[r, 0], LOW)
        best = jnp.maximum(jnp.max(tops, axis=0), ttop)
        factors = jnp.exp(tops - best[None])
        tfactor = jnp.exp(ttop - best)
        denom = jnp.sum(factors * totals, axis=0) + tfactor * tstat[r, 1]
        packed = jnp.concatenate([factors.reshape(n * props, LANES), tfactor, denom], axis=0)
        wide = dot(packed, widen, HIGH)
        numer = wide[n * props : (n + 1) * props] * tmix[r] + wide[:props] * unfold(mix[s])
        for k in range(1, n):
            numer = numer + wide[k * props : (k + 1) * props] * unfold(mix_in[k - 1, r])
        att[s] = fold(numer / wide[(n + 1) * props :]).astype(BF16)
        for k in range(1, n):
            b_copy(r, k, att, d_send, d_recv).start()

    for r in range(slots):
        for_slot(r, functools.partial(project, r))
        if r > 0:
            for_slot(r - 1, functools.partial(merge, r - 1))
        for_slot(r, functools.partial(tree, r))
        lax.fori_loop(r * n, min((r + 1) * n, seqs), shard, 0)
    for_slot(slots - 1, functools.partial(merge, slots - 1))

    out_load.wait()
    block = rows // n_tp

    def e_copy(t):
        k = lax.rem(tp - t + n_tp, n_tp)
        return pltpu.make_async_remote_copy(
            src_ref=terms.at[t],
            dst_ref=terms_in.at[jnp.maximum(k - 1, 0)],
            send_sem=e_send.at[t],
            recv_sem=e_recv.at[jnp.maximum(k - 1, 0)],
            device_id={"tp": t},
        )

    arrived = 0
    for t in range(n_tp):
        first, last = t * block // props, ((t + 1) * block - 1) // props + 1
        for s in range(arrived, last):
            d = owner_of(s)

            @pl.when(d != me)
            def _(s=s, d=d):
                pltpu.make_async_remote_copy(
                    src_ref=att.at[s],
                    dst_ref=att.at[s],
                    send_sem=d_send.at[0, 0],
                    recv_sem=d_recv.at[s],
                    device_id={"kv": d},
                ).wait_recv()

        arrived = max(arrived, last)
        attended = jnp.concatenate([unfold(att[s]) for s in range(first, last)], axis=0)
        term = dot(attended.astype(BF16), out_w[...])
        begin = t * block - first * props
        terms[t] = term[begin : begin + block].astype(BF16)
        pl.when(tp != t)(e_copy(t).start)
    total = terms[tp].astype(F32)
    for k in range(1, n_tp):
        pltpu.make_async_remote_copy(
            src_ref=terms.at[0],
            dst_ref=terms_in.at[k - 1],
            send_sem=e_send.at[0],
            recv_sem=e_recv.at[k - 1],
            device_id={"tp": lax.rem(tp + k, n_tp)},
        ).wait_recv()
        total = total + terms_in[k - 1].astype(F32)
    out[...] = total.astype(BF16)

    for s in range(seqs):
        d = owner_of(s)
        for which in range(2):
            pl.when(crosses(s))(p_copy(s, which).wait_send)
            pl.when(passes(s))(a_copy(s, which).wait_send)
        for which, (src, dst) in enumerate(((mix, mix_in), (stat, stat_in))):
            _, copy = c_copy(s, which, src, dst)
            pl.when(d != me)(copy.wait_send)
    for r in range(slots):

        def drain(r=r):
            for k in range(1, n):
                b_copy(r, k, qbuf, b_send, b_recv).wait_send()
                b_copy(r, k, att, d_send, d_recv).wait_send()

        for_slot(r, drain)
    for t in range(n_tp):
        pl.when(tp != t)(e_copy(t).wait_send)


def split3(x):
    high = x.astype(BF16)
    rest = x - high.astype(F32)
    mid = rest.astype(BF16)
    low = (rest - mid.astype(F32)).astype(BF16)
    return high, mid, low


def tile_rows(rows, total):
    return jnp.concatenate([rows, jnp.zeros((total - rows.shape[0], rows.shape[1]), rows.dtype)], axis=0)


def by_heads(
    n,
    n_tp,
    wave,
    tokens_hbm,
    gain_hbm,
    query_hbm,
    key_hbm,
    value_hbm,
    gate_hbm,
    bias_hbm,
    out_hbm,
    keys_hbm,
    values_hbm,
    decay_hbm,
    lengths_hbm,
    parents_hbm,
    out,
    tokens,
    gain,
    query_w,
    key_w,
    value_w,
    gate_w,
    bias,
    decay,
    lengths,
    parents,
    out_w,
    keys,
    values,
    feats,
    q_out,
    q_in,
    q_own,
    q_far,
    q_last,
    q_last_in,
    q_cross,
    kv_out,
    kv_in,
    kv_own,
    kv_pass,
    kv_far,
    qbuf,
    mix,
    mix_in,
    stat,
    stat_in,
    att,
    terms,
    terms_in,
    par_pad,
    link_s,
    anc_s,
    path_s,
    inv_s,
    tmix,
    tstat,
    held,
    swap,
    swap_in,
    swap_stat,
    swap_stat_in,
    widen,
    load_sem,
    cache_sem,
    qx_send,
    qx_recv,
    kx_send,
    kx_recv,
    qz_send,
    qz_recv,
    kz_send,
    kz_recv,
    b_send,
    b_recv,
    c_send,
    c_recv,
    d_send,
    d_recv,
    e_send,
    e_recv,
    qr_send,
    qr_recv,
    s_send,
    s_recv,
    l_send,
    l_recv,
):
    me = lax.axis_index("kv")
    tp = lax.axis_index("tp")
    side = lax.rem(me, 2)
    far = lax.div(me, 2)
    n_far = n // 2
    rows, depth = tokens.shape
    seqs, props = parents.shape
    heads = decay.shape[1]
    pos_dev = keys.shape[1]
    width = query_w.shape[1]
    head_dim = width // heads
    scale = head_dim ** (-0.5)
    exact_scale = math.frexp(scale)[0] == 0.5
    own_heads = heads // n_far
    cols = width // n_far
    half_seqs = seqs // 2
    half = rows // 2
    waves = half_seqs // wave
    wrows = wave * props
    sources = n - 1

    pairs = (
        (tokens_hbm, tokens),
        (gain_hbm, gain),
        (gate_hbm.at[:, pl.ds(pl.multiple_of(me * depth, depth), depth)], gate_w),
        (query_hbm, query_w),
        (key_hbm, key_w),
        (value_hbm, value_w),
        (bias_hbm, bias),
        (parents_hbm, parents),
        (lengths_hbm, lengths),
        (decay_hbm, decay),
        (out_hbm, out_w),
    )
    loads = [pltpu.make_async_copy(src, dst, load_sem.at[i]) for i, (src, dst) in enumerate(pairs)]
    load_of = dict(
        zip(("tokens", "gain", "gate", "q", "k", "v", "bias", "parents", "lengths", "decay", "out"), loads)
    )
    for load in loads[:6]:
        load.start()
    barrier = pltpu.get_barrier_semaphore()
    for k in range(1, n):
        pl.semaphore_signal(barrier, inc=1, device_id={"kv": lax.rem(me + k, n)})
    for k in range(1, n_tp):
        pl.semaphore_signal(barrier, inc=1, device_id={"tp": lax.rem(tp + k, n_tp)})

    def iota(shape, dim):
        return lax.broadcasted_iota(jnp.int32, shape, dim)

    def far_id(d):
        return lax.rem(far + d, n_far)

    def near_id(z, x):
        return {"kv": z * 2 + x}

    own_half = pl.multiple_of(side * half, half)
    peer_half = pl.multiple_of((1 - side) * half, half)

    load_of["tokens"].wait()
    load_of["gain"].wait()
    for load in loads[6:]:
        load.start()
    for s in range(seqs):
        pltpu.make_async_copy(keys_hbm.at[s], keys.at[s], cache_sem.at[0, s]).start()
        pltpu.make_async_copy(values_hbm.at[s], values.at[s], cache_sem.at[1, s]).start()
    xf = tokens[...].astype(F32)
    feats[:, :depth] = (xf * gain[...]).astype(BF16)
    square = xf * xf
    high = square.astype(BF16)
    feats[:, depth : 2 * depth] = high
    feats[:, 2 * depth :] = (square - high.astype(F32)).astype(BF16)

    load_of["gate"].wait()
    t_rows = n_far * 8
    p_row = iota((t_rows, gate_w.shape[0]), 0)
    p_col = iota((t_rows, gate_w.shape[0]), 1)
    p_in = lax.rem(p_row, 8)
    wanted = (p_in < own_heads) & (p_col == tp * heads + lax.div(p_row, 8) * own_heads + p_in)
    gates = dot(wanted.astype(BF16), gate_w[...]).astype(BF16)
    ones = (lax.rem(iota((t_rows, depth), 0), 8) == own_heads).astype(BF16)
    tails = jnp.concatenate([gates, ones, ones], axis=1)

    def project_q(base, dst, which):
        full = dot(feats[pl.ds(base, half), :depth], query_w[...])
        for i in range(waves):
            piece = full[i * wrows : (i + 1) * wrows]
            tail = dot_nt(tails, feats[pl.ds(base + i * wrows, wrows), :])
            tail = jnp.concatenate([tail, jnp.zeros((t_rows, LANES - wrows), F32)], axis=1)
            for f in range(n_far):
                for at, rows_of in (
                    (slice(0, wrows), piece[:, f * cols : (f + 1) * cols]),
                    (slice(wrows, wrows + 8), tail[f * 8 : (f + 1) * 8]),
                ):
                    if i < waves - 1:
                        dst[i, f, at] = rows_of
                    else:
                        q_last[f, which, at] = rows_of

    def project_kv(base, dst):
        for which, w in enumerate((key_w, value_w)):
            full = dot(feats[pl.ds(base, half), :depth], w[...])
            for i in range(waves):
                piece = full[i * wrows : (i + 1) * wrows].astype(dst.dtype)
                for f in range(n_far):
                    dst[i, f, which * wrows : (which + 1) * wrows] = piece[:, f * cols : (f + 1) * cols]

    def x_copy(i, src, dst, send, recv):
        return pltpu.make_async_remote_copy(
            src_ref=src.at[i],
            dst_ref=dst.at[i],
            send_sem=send.at[i],
            recv_sem=recv.at[i],
            device_id=near_id(far, 1 - side),
        )

    def z_copy(i, d, src, dst, send, recv):
        return pltpu.make_async_remote_copy(
            src_ref=src.at[i, far_id(d)],
            dst_ref=dst.at[d - 1, i],
            send_sem=send.at[d - 1, i],
            recv_sem=recv.at[d - 1, i],
            device_id=near_id(far_id(d), side),
        )

    def last_copy(d):
        return pltpu.make_async_remote_copy(
            src_ref=q_last.at[far_id(d)],
            dst_ref=q_last_in.at[d - 1],
            send_sem=l_send.at[d - 1],
            recv_sem=l_recv.at[d - 1],
            device_id=near_id(far_id(d), side),
        )

    def last_cross():
        return pltpu.make_async_remote_copy(
            src_ref=q_last.at[far, 1],
            dst_ref=q_cross,
            send_sem=l_send.at[n_far - 1],
            recv_sem=l_recv.at[n_far - 1],
            device_id=near_id(far, 1 - side),
        )

    load_of["q"].wait()
    project_q(peer_half, q_out, 1)
    pl.semaphore_wait(barrier, n + n_tp - 2)
    for i in range(waves - 1):
        x_copy(i, q_out, q_in, qx_send, qx_recv).start()
    project_q(own_half, q_own, 0)
    for d in range(1, n_far):
        last_copy(d).start()
    load_of["k"].wait()
    load_of["v"].wait()
    project_kv(peer_half, kv_out)
    for i in range(waves):
        x_copy(i, kv_out, kv_in, kx_send, kx_recv).start()
    project_kv(own_half, kv_own)

    load_of["bias"].wait()
    load_of["parents"].wait()
    load_of["lengths"].wait()
    load_of["decay"].wait()
    par_pad[...] = jnp.zeros(par_pad.shape, jnp.int32)
    par_pad[0:seqs, 0:props] = parents[...]
    r_i = iota((LANES, LANES), 0)
    c_i = iota((LANES, LANES), 1)
    lane1 = iota((1, LANES), 1)
    eye = r_i == c_i
    for i in range(waves):
        row = jnp.full((1, LANES), -1, jnp.int32)
        for j in range(wave):
            of = par_pad[pl.ds(side * half_seqs + i * wave + j, 1), :]
            if j:
                of = pltpu.roll(jnp.broadcast_to(of, (8, LANES)), j * props, 1)[0:1]
            inside = (lane1 >= j * props) & (lane1 < (j + 1) * props)
            row = jnp.where(inside, of + j * props, row)
        link = ((row == r_i) | eye).astype(F32).astype(BF16)
        for _ in range(props.bit_length()):
            link = jnp.minimum(dot(link, link), 1.0).astype(BF16)
        link_s[i] = link
        anc_s[i] = dot_nt(eye.astype(F32).astype(BF16), link)
    w_row = lax.rem(iota(widen.shape, 0), LANES)
    w_col = iota(widen.shape, 1)
    w_src = lax.div(w_col, cols) * 8 + lax.div(lax.rem(w_col, cols), head_dim)
    widen[...] = (w_row == w_src).astype(F32).astype(BF16)
    b_shape = (8, bias.shape[1])
    b_row, b_col = iota(b_shape, 0), iota(b_shape, 1)
    mine = (b_row < own_heads) & (b_col == tp * heads + far * own_heads + b_row)
    bias_col = jnp.sum(jnp.where(mine, jnp.broadcast_to(bias[...], b_shape), 0.0), axis=1, keepdims=True)

    for i in range(waves - 1):
        x_copy(i, q_out, q_in, qx_send, qx_recv).wait_recv()
        q_own[i] = q_own[i] + q_in[i]
        for d in range(1, n_far):
            z_copy(i, d, q_own, q_far, qz_send, qz_recv).start()
    for d in range(1, n_far):
        last_copy(d).wait_recv()
    q_last[far] = q_last[far] + functools.reduce(jnp.add, [q_last_in[d] for d in range(n_far - 1)])
    last_cross().start()

    targets = [(d, 0) for d in range(1, n_far)] + [(d, 1) for d in range(n_far)]

    def target_id(d, cross):
        return near_id(far_id(d), side if not cross else 1 - side)

    def spread_copy(i, t, buf, send, recv):
        d, cross = targets[t]
        block = side * waves + i
        return pltpu.make_async_remote_copy(
            src_ref=buf.at[block, far],
            dst_ref=buf.at[block, far],
            send_sem=send.at[t, i],
            recv_sem=recv.at[block, far],
            device_id=target_id(d, cross),
        )

    def relay_copy(i, buf, send, recv):
        block = side * waves + i
        return pltpu.make_async_remote_copy(
            src_ref=buf.at[block],
            dst_ref=buf.at[block],
            send_sem=send.at[i],
            recv_sem=recv.at[i],
            device_id=near_id(far, 1 - side),
        )

    def spread(i, direct, buf, send, recv):
        for t in range(sources if direct else n_far - 1):
            spread_copy(i, t, buf, send, recv).start()

    def sent(i, direct, buf, send, recv, r_send, r_recv):
        for t in range(sources if direct else n_far - 1):
            spread_copy(i, t, buf, send, recv).wait_send()
        if not direct:
            relay_copy(i, buf, r_send, r_recv).wait_send()

    def spread_wait(i, t, buf, send, recv):
        d, cross = targets[t]
        block = (1 - side if cross else side) * waves + i
        pltpu.make_async_remote_copy(
            src_ref=buf.at[block, far_id(d)],
            dst_ref=buf.at[block, far_id(d)],
            send_sem=send.at[t, i],
            recv_sem=recv.at[block, far_id(d)],
            device_id=target_id(d, cross),
        ).wait_recv()

    def pass_on(i, direct, buf, send, recv, r_send, r_recv):
        for t in range(n_far - 1):
            spread_wait(i, t, buf, send, recv)
        if not direct:
            relay_copy(i, buf, r_send, r_recv).start()

    def crossed(i, direct, buf, send, recv, r_send, r_recv):
        if not direct:
            relay_copy(i, buf, r_send, r_recv).wait_recv()
            return
        for t in range(n_far - 1, sources):
            spread_wait(i, t, buf, send, recv)

    q_route = (qbuf, b_send, b_recv, qr_send, qr_recv)
    zone = n_far // 2
    place_in = lax.rem(far, zone)
    zone_of = lax.div(far, zone)
    near = [(d, 0) for d in range(1, zone)] + [(d, 1) for d in range(zone)]

    def place_at(d):
        return lax.rem(place_in + d, zone)

    def zone_id(d, cross):
        return near_id(zone_of * zone + place_at(d), 1 - side if cross else side)

    q_direct = [False] * waves

    strides = [1 << b for b in range(n_far.bit_length() - 1)]

    def halve_copy(i, st, m):
        slot = sum(n_far // (2 * x) for x in strides if x < st) + m
        partner = far + st - 2 * st * lax.rem(lax.div(far, st), 2)
        return pltpu.make_async_remote_copy(
            src_ref=kv_pass.at[i, lax.rem(partner, 2 * st) + 2 * st * m],
            dst_ref=kv_far.at[slot, i],
            send_sem=kz_send.at[slot, i],
            recv_sem=kz_recv.at[slot, i],
            device_id=near_id(partner, side),
        )

    def halve_start(i, st):
        partner = far + st - 2 * st * lax.rem(lax.div(far, st), 2)
        for m in range(n_far // (2 * st)):
            f = lax.rem(partner, 2 * st) + 2 * st * m
            kv_pass[i, f] = kv_own[i, f].astype(BF16)
            halve_copy(i, st, m).start()

    def halve_wait(i, st):
        for m in range(n_far // (2 * st)):
            halve_copy(i, st, m).wait_recv()
            f = lax.rem(far, 2 * st) + 2 * st * m
            slot = sum(n_far // (2 * x) for x in strides if x < st) + m
            kv_own[i, f] = kv_own[i, f] + kv_far[slot, i].astype(F32)

    def pass_kv(i, step):
        if step:
            halve_wait(i, strides[step - 1])
        else:
            x_copy(i, kv_out, kv_in, kx_send, kx_recv).wait_recv()
            kv_own[i] = kv_own[i] + kv_in[i].astype(F32)
        if step < len(strides):
            halve_start(i, strides[step])

    lane8 = iota((8, LANES), 1)
    row8 = iota((8, LANES), 0)

    def owner_q(i):
        if i < waves - 1:
            total = q_own[i, far]
            for d in range(1, n_far):
                z_copy(i, d, q_own, q_far, qz_send, qz_recv).wait_recv()
                total = total + q_far[d - 1, i]
        else:
            last_cross().wait_recv()
            total = q_last[far, 0] + q_cross[...]
        tail = total[wrows:]
        inverse = lax.rsqrt(tail / (depth * n) + 1e-06)
        column = tile_rows(inverse, LANES).T[:wrows, own_heads : own_heads + 1]
        inv_s[i] = jnp.broadcast_to(column, (wrows, cols))
        qbuf[side * waves + i, far] = (inv_s[i] * total[:wrows]).astype(BF16)
        spread(i, q_direct[i], qbuf, b_send, b_recv)
        inverse_row = jnp.broadcast_to(inverse[own_heads : own_heads + 1], (8, LANES))
        x = inverse_row * tail + bias_col
        log_gate = jnp.minimum(x, 0.0) - jnp.log1p(jnp.exp(-jnp.abs(x)))
        log_gate = jnp.where((row8 < own_heads) & (lane8 < wrows), log_gate, 0.0)
        parts = dot(jnp.concatenate(split3(log_gate), axis=0), link_s[i])
        path_s[i] = parts[:8] + parts[8:16] + parts[16:24]

    for i in range(waves):
        owner_q(i)
        if i < waves - 1:
            pass_kv(i, 0)

    group = min(heads, 256 // head_dim)
    gwidth = group * head_dim
    g_head = iota((group, props, gwidth), 0)
    g_col = lax.div(iota((group, props, gwidth), 2), head_dim)
    g_diag = (g_head == g_col).reshape(group * props, gwidth)
    lane_w = iota((wrows, LANES), 1)
    position = iota((heads, pos_dev), 1) + me * pos_dev

    def mix_copy(i, t, which, src, dst):
        d, cross = near[t]
        block = (1 - side if cross else side) * waves + i
        return pltpu.make_async_remote_copy(
            src_ref=src.at[block, place_at(d)],
            dst_ref=dst.at[t, i],
            send_sem=c_send.at[which, t, i],
            recv_sem=c_recv.at[which, t, i],
            device_id=zone_id(d, cross),
        )

    def attend(i, cross):
        place = 1 - side if cross else side
        block = place * waves + i
        if cross:
            crossed(i, q_direct[i], *q_route)
        first = place * half_seqs + i * wave
        for j in range(wave):
            s = first + j
            pltpu.make_async_copy(keys_hbm.at[s], keys.at[s], cache_sem.at[0, s]).wait()
            pltpu.make_async_copy(values_hbm.at[s], values.at[s], cache_sem.at[1, s]).wait()
        q_wave = jnp.concatenate([qbuf[block, f] for f in range(n_far)], axis=1).astype(F32)
        if exact_scale:
            q_wave = q_wave * scale
        chains = [(j, g) for j in range(wave) for g in range(heads // group)]
        scores_of, w_of, tops, totals, parts = {}, {}, {}, {}, {}
        for j in range(wave):
            s = first + j
            fade = jnp.where(position < lengths[s], decay[s], LOW)
            for g in range(heads // group):
                q = q_wave[j * props : (j + 1) * props, g * gwidth : (g + 1) * gwidth]
                q = jnp.broadcast_to(q[None], (group, props, gwidth)).reshape(group * props, gwidth)
                q = jnp.where(g_diag, q, 0.0).astype(BF16)
                scores = dot_nt(q, keys[s, :, g * gwidth : (g + 1) * gwidth])
                if not exact_scale:
                    scores = scores * scale
                fades = [
                    jnp.broadcast_to(fade[h : h + 1], (props, pos_dev))
                    for h in range(g * group, (g + 1) * group)
                ]
                scores_of[j, g] = scores + jnp.concatenate(fades, axis=0)
        for j, g in chains:
            top = jnp.max(scores_of[j, g], axis=1, keepdims=True)
            w = jnp.exp(scores_of[j, g] - top)
            total = jnp.sum(w, axis=1, keepdims=True)
            w_of[j, g] = w.astype(BF16)
            for h in range(group):
                tops[j, g * group + h] = top[h * props : (h + 1) * props]
                totals[j, g * group + h] = total[h * props : (h + 1) * props]
        for j, g in chains:
            m = dot(w_of[j, g], values[first + j, :, g * gwidth : (g + 1) * gwidth])
            m = jnp.where(g_diag, m, 0.0).reshape(group, props, gwidth)
            parts[j, g] = jnp.sum(m, axis=0)
        mixes = [
            jnp.concatenate([parts[j, g] for g in range(heads // group)], axis=1) for j in range(wave)
        ]
        mixed = jnp.concatenate(mixes, axis=0).astype(BF16)
        for f in range(n_far):
            mix[block, f % zone, f // zone] = mixed[:, f * cols : (f + 1) * cols]
        acc = jnp.zeros((wrows, LANES), F32)
        for h in range(heads):
            f, k = divmod(h, own_heads)
            for at, cols_of in ((k, tops), (own_heads + k, totals)):
                col = jnp.concatenate([cols_of[j, h] for j in range(wave)], axis=0)
                acc = jnp.where(lane_w == f * 8 + at, col, acc)
        flat = tile_rows(acc, LANES).T
        for f in range(n_far):
            stat[block, f % zone, f // zone] = flat[f * 8 : f * 8 + stat.shape[3]]
        for t in range(len(near)):
            if near[t][1] == cross:
                mix_copy(i, t, 0, mix, mix_in).start()
                mix_copy(i, t, 1, stat, stat_in).start()

    own_head_of = lax.div(iota((wrows, cols), 1), head_dim)

    def tree(i):
        block = side * waves + i
        pass_kv(i, len(strides))
        total = kv_own[i, far]
        new_k = tile_rows(inv_s[i] * total[:wrows], LANES).astype(BF16)
        new_v = tile_rows(inv_s[i] * total[wrows:], LANES).astype(BF16)
        q = qbuf[block, far].astype(F32)
        q = jnp.concatenate([jnp.where(own_head_of == h, q, 0.0) for h in range(own_heads)], axis=0)
        scores = dot_nt(q.astype(BF16), new_k) * scale
        path = path_s[i]
        shifts = [jnp.broadcast_to(-path[h : h + 1], (wrows, LANES)) for h in range(own_heads)]
        scores = scores + jnp.concatenate(shifts, axis=0)
        live = jnp.concatenate([anc_s[i, :wrows]] * own_heads, axis=0) > 0.5
        scores = jnp.where(live, scores, LOW)
        top = jnp.max(scores, axis=1, keepdims=True)
        w = jnp.where(live, jnp.exp(scores - top), 0.0)
        total = jnp.sum(w, axis=1, keepdims=True)
        m = dot(w.astype(BF16), new_v)
        merged = jnp.zeros((wrows, cols), F32)
        acc = jnp.zeros((wrows, LANES), F32)
        for h in range(own_heads):
            part = slice(h * wrows, (h + 1) * wrows)
            merged = jnp.where(own_head_of == h, m[part], merged)
            acc = jnp.where(lane_w == h, top[part], acc)
            acc = jnp.where(lane_w == own_heads + h, total[part], acc)
        tmix[i] = merged
        tstat[i] = tile_rows(acc, LANES).T[:8]

    def swap_copy(i, which, src, dst):
        return pltpu.make_async_remote_copy(
            src_ref=src.at[i],
            dst_ref=dst.at[i],
            send_sem=s_send.at[which, i],
            recv_sem=s_recv.at[which, i],
            device_id=near_id((1 - zone_of) * zone + place_in, side),
        )

    def turn(tiles):
        flat = jnp.concatenate([jnp.where(row8 < own_heads, x, 0.0) for x in tiles], axis=0)
        turned = tile_rows(flat, LANES).T[:wrows]
        high = turned.astype(BF16)
        low = (turned - high.astype(F32)).astype(BF16)
        both = jnp.concatenate([high, low], axis=1)
        return dot(both, widen[:, : len(tiles) * cols])

    def lift(st):
        return pltpu.roll(st, 8 - own_heads, 0)

    def weigh(wide, first, parts):
        total = jnp.zeros((wrows, cols), F32)
        for k, m in enumerate(parts):
            at = (first + k) * cols
            total = total + wide[:, at : at + cols] * m.astype(F32)
        return total

    def merge(i):
        block = side * waves + i
        for t in range(len(near)):
            mix_copy(i, t, 0, mix, mix_in).wait_recv()
            mix_copy(i, t, 1, stat, stat_in).wait_recv()
        tiles = []
        for k in range(2):
            stats = [stat[block, place_in, k]] + [stat_in[t, i, k] for t in range(len(near))]
            stats = [tile_rows(st, 8) for st in stats]
            absent = jnp.where(row8 < own_heads, LOW, 0.0)
            stats.append(jnp.where(zone_of == k, tstat[i], absent))
            best = functools.reduce(jnp.maximum, stats)
            factors = [jnp.exp(st - best) for st in stats]
            total = functools.reduce(jnp.add, [f * lift(st) for f, st in zip(factors, stats)])
            packed = jnp.where(row8 < own_heads, best, pltpu.roll(total, own_heads, 0))
            swap_stat[i, k] = packed[: swap_stat.shape[2]]
            tiles += factors
        wide = turn(tiles)
        for k in range(2):
            parts = [mix[block, place_in, k]] + [mix_in[t, i, k] for t in range(len(near))] + [tmix[i]]
            held[i, k] = weigh(wide, k * len(parts), parts)
            swap[i, k] = held[i, k].astype(BF16)
        swap_copy(i, 0, swap, swap_in).start()
        swap_copy(i, 1, swap_stat, swap_stat_in).start()

    def att_copy(i, t, block, place):
        d, cross = near[t]
        return pltpu.make_async_remote_copy(
            src_ref=att.at[block, place],
            dst_ref=att.at[block, place],
            send_sem=d_send.at[t, i],
            recv_sem=d_recv.at[block, place],
            device_id=zone_id(d, cross),
        )

    def finish(i):
        block = side * waves + i
        swap_copy(i, 0, swap, swap_in).wait_recv()
        swap_copy(i, 1, swap_stat, swap_stat_in).wait_recv()
        tiles = []
        for k in range(2):
            stats = [tile_rows(st[i, k], 8) for st in (swap_stat, swap_stat_in)]
            best = jnp.maximum(stats[0], stats[1])
            factors = [jnp.exp(st - best) for st in stats]
            denom = functools.reduce(jnp.add, [f * lift(st) for f, st in zip(factors, stats)])
            tiles += [f / denom for f in factors]
        wide = turn(tiles)
        for k in range(2):
            att[block, place_in, k] = weigh(wide, 2 * k, (held[i, k], swap_in[i, k])).astype(BF16)
        for t in range(len(near)):
            att_copy(i, t, block, place_in).start()

    per_tp = seqs // n_tp

    def e_copy(s, t):
        k = jnp.maximum(lax.rem(tp - t + n_tp, n_tp) - 1, 0)
        return pltpu.make_async_remote_copy(
            src_ref=terms.at[s],
            dst_ref=terms_in.at[k, lax.rem(s, per_tp)],
            send_sem=e_send.at[s],
            recv_sem=e_recv.at[k, lax.rem(s, per_tp)],
            device_id={"tp": t},
        )

    def output(i, cross):
        place = 1 - side if cross else side
        block = place * waves + i
        for t, (d, over) in enumerate(near):
            if over == cross:
                att_copy(i, t, block, place_at(d)).wait_recv()
        attended = jnp.concatenate([att[block, f % zone, f // zone] for f in range(n_far)], axis=1)
        term = dot(attended, out_w[...])
        for j in range(wave):
            s = place * half_seqs + i * wave + j
            terms[s] = fold(term[j * props : (j + 1) * props]).astype(BF16)
            t = lax.div(s, per_tp)
            pl.when(tp != t)(e_copy(s, t).start)

    advanced = [0] * waves

    def advance(count):
        for i in range(waves):
            if count and advanced[i] + 1 < len(strides):
                advanced[i] += 1
                pass_kv(i, advanced[i])
                count -= 1

    pass_on(0, q_direct[0], *q_route)
    attend(0, 0)
    pass_kv(waves - 1, 0)
    advance(1)
    for i in range(1, waves):
        pass_on(i, q_direct[i], *q_route)
        if i == 1:
            attend(1, 0)
            advance(1)
    attend(0, 1)
    advance(1)
    for i in range(1, waves):
        if i == waves - 1:
            for k in range(2, waves):
                attend(k, 0)
        attend(i, 1)
    advance(waves * len(strides))
    load_of["out"].wait()
    for i in range(waves):
        tree(i)
        merge(i)
    for i in range(waves):
        finish(i)
    for i in range(waves):
        output(i, 0)
        output(i, 1)

    done = []
    for j in range(per_tp):
        total = unfold(terms[tp * per_tp + j])
        for k in range(1, n_tp):
            pltpu.make_async_remote_copy(
                src_ref=terms.at[0],
                dst_ref=terms_in.at[k - 1, j],
                send_sem=e_send.at[0],
                recv_sem=e_recv.at[k - 1, j],
                device_id={"tp": lax.rem(tp + k, n_tp)},
            ).wait_recv()
            total = total + unfold(terms_in[k - 1, j])
        done.append(total)
    out[...] = jnp.concatenate(done, axis=0).astype(BF16)

    for i in range(waves):
        if i < waves - 1:
            x_copy(i, q_out, q_in, qx_send, qx_recv).wait_send()
            for d in range(1, n_far):
                z_copy(i, d, q_own, q_far, qz_send, qz_recv).wait_send()
        x_copy(i, kv_out, kv_in, kx_send, kx_recv).wait_send()
        for st in strides:
            for m in range(n_far // (2 * st)):
                halve_copy(i, st, m).wait_send()
        sent(i, q_direct[i], *q_route)
        swap_copy(i, 0, swap, swap_in).wait_send()
        swap_copy(i, 1, swap_stat, swap_stat_in).wait_send()
        for t in range(len(near)):
            att_copy(i, t, side * waves + i, place_in).wait_send()
            mix_copy(i, t, 0, mix, mix_in).wait_send()
            mix_copy(i, t, 1, stat, stat_in).wait_send()
    for d in range(1, n_far):
        last_copy(d).wait_send()
    last_cross().wait_send()
    for s in range(seqs):
        t = s // per_tp
        pl.when(tp != t)(e_copy(s, t).wait_send)


def wave_size(n, n_tp, seqs, props, heads, width):
    n_far = n // 2
    if n < 4 or n & (n - 1) or seqs % 2 or seqs % n_tp or heads % n_far or width % (n_far * LANES):
        return 0
    head_dim = width // heads
    own = heads // n_far
    if own > 4 or 16 * (n_far + 1) > LANES or (heads % min(heads, max(256 // head_dim, 1))):
        return 0
    for wave in range(1, seqs // 2 + 1):
        fits = wave * props % 16 == 0 and wave * props <= LANES
        if seqs // 2 % wave == 0 and fits and props % 8 == 0:
            return wave
    return 0


def solution(mesh):
    n, n_tp = mesh.shape["kv"], mesh.shape["tp"]

    def body(
        tokens,
        norm_gain,
        query_weight,
        key_weight,
        value_weight,
        gate_weight,
        gate_bias,
        out_weight,
        cache_keys,
        cache_values,
        cache_decay,
        lengths,
        parents,
    ):
        rows, depth = tokens.shape
        seqs, props = parents.shape
        heads = cache_decay.shape[1]
        pos_dev = cache_keys.shape[1]
        width = query_weight.shape[1]
        cols = out_weight.shape[1]
        slots = -(-seqs // n)
        block = rows // n_tp
        all_w = 2 * width + LANES
        folded = (2 * props, width // 2)
        vmem = pl.BlockSpec(memory_space=pltpu.VMEM)
        hbm = pl.BlockSpec(memory_space=pltpu.HBM)
        dma = pltpu.SemaphoreType.DMA
        wave = wave_size(n, n_tp, seqs, props, heads, width)
        if wave:
            n_far = n // 2
            waves = seqs // 2 // wave
            q_waves = max(waves - 1, 1)
            zone = n_far // 2
            wrows = wave * props
            wcols = width // n_far
            per_tp = seqs // n_tp
            s_rows = max(4, 2 * (heads // n_far))
            block_q = (n_far, wrows + 8, wcols)
            block_kv = (n_far, 2 * wrows, wcols)
            body_of = functools.partial(by_heads, n, n_tp, wave)
            scratch = [
                pltpu.VMEM(tokens.shape, BF16),
                pltpu.VMEM((1, depth), F32),
                pltpu.VMEM(query_weight.shape, BF16),
                pltpu.VMEM(key_weight.shape, BF16),
                pltpu.VMEM(value_weight.shape, BF16),
                pltpu.VMEM((gate_weight.shape[1], depth), BF16),
                pltpu.VMEM((1, gate_bias.shape[0]), F32),
                pltpu.VMEM(cache_decay.shape, F32),
                pltpu.SMEM(lengths.shape, jnp.int32),
                pltpu.VMEM(parents.shape, jnp.int32),
                pltpu.VMEM(out_weight.shape, BF16),
                pltpu.VMEM(cache_keys.shape, BF16),
                pltpu.VMEM(cache_values.shape, BF16),
                pltpu.VMEM((rows, 3 * depth), BF16),
                pltpu.VMEM((q_waves,) + block_q, F32),
                pltpu.VMEM((q_waves,) + block_q, F32),
                pltpu.VMEM((q_waves,) + block_q, F32),
                pltpu.VMEM((n_far - 1, q_waves) + block_q[1:], F32),
                pltpu.VMEM((n_far, 2) + block_q[1:], F32),
                pltpu.VMEM((n_far - 1, 2) + block_q[1:], F32),
                pltpu.VMEM(block_q[1:], F32),
                pltpu.VMEM((waves,) + block_kv, BF16),
                pltpu.VMEM((waves,) + block_kv, BF16),
                pltpu.VMEM((waves,) + block_kv, F32),
                pltpu.VMEM((waves,) + block_kv, BF16),
                pltpu.VMEM((n_far - 1, waves) + block_kv[1:], BF16),
                pltpu.VMEM((2 * waves, n_far, wrows, wcols), BF16),
                pltpu.VMEM((2 * waves, zone, 2, wrows, wcols), BF16),
                pltpu.VMEM((n_far - 1, waves, 2, wrows, wcols), BF16),
                pltpu.VMEM((2 * waves, zone, 2, s_rows, LANES), F32),
                pltpu.VMEM((n_far - 1, waves, 2, s_rows, LANES), F32),
                pltpu.VMEM((2 * waves, zone, 2, wrows, wcols), BF16),
                pltpu.VMEM((seqs,) + folded, BF16),
                pltpu.VMEM((n_tp - 1, per_tp) + folded, BF16),
                pltpu.VMEM((-(-seqs // 8) * 8, LANES), jnp.int32),
                pltpu.VMEM((waves, LANES, LANES), BF16),
                pltpu.VMEM((waves, LANES, LANES), F32),
                pltpu.VMEM((waves, 8, LANES), F32),
                pltpu.VMEM((waves, wrows, wcols), F32),
                pltpu.VMEM((waves, wrows, wcols), F32),
                pltpu.VMEM((waves, 8, LANES), F32),
                pltpu.VMEM((waves, 2, wrows, wcols), F32),
                pltpu.VMEM((waves, 2, wrows, wcols), BF16),
                pltpu.VMEM((waves, 2, wrows, wcols), BF16),
                pltpu.VMEM((waves, 2, s_rows, LANES), F32),
                pltpu.VMEM((waves, 2, s_rows, LANES), F32),
                pltpu.VMEM((2 * LANES, 2 * (n_far + 1) * wcols), BF16),
                dma((11,)),
                dma((2, seqs)),
                dma((waves,)),
                dma((waves,)),
                dma((waves,)),
                dma((waves,)),
                dma((n_far - 1, waves)),
                dma((n_far - 1, waves)),
                dma((n_far - 1, waves)),
                dma((n_far - 1, waves)),
                dma((n - 1, waves)),
                dma((2 * waves, n_far)),
                dma((2, n_far - 1, waves)),
                dma((2, n_far - 1, waves)),
                dma((n_far - 1, waves)),
                dma((2 * waves, zone)),
                dma((seqs,)),
                dma((n_tp - 1, per_tp)),
                dma((waves,)),
                dma((waves,)),
                dma((2, waves)),
                dma((2, waves)),
                dma((n_far,)),
                dma((n_far,)),
            ]
        else:
            body_of = functools.partial(by_sequence, n, n_tp)
            scratch = [
                pltpu.VMEM(tokens.shape, BF16),
                pltpu.VMEM((1, depth), F32),
                pltpu.VMEM(query_weight.shape, BF16),
                pltpu.VMEM(key_weight.shape, BF16),
                pltpu.VMEM(value_weight.shape, BF16),
                pltpu.VMEM((1, gate_bias.shape[0]), F32),
                pltpu.VMEM(cache_decay.shape, F32),
                pltpu.SMEM(lengths.shape, jnp.int32),
                pltpu.VMEM(parents.shape, jnp.int32),
                dma((9,)),
                pltpu.VMEM((seqs, props, all_w), F32),
                pltpu.VMEM((seqs,) + folded, BF16),
                pltpu.VMEM((seqs, props, all_w), F32),
                pltpu.VMEM((seqs,) + folded, BF16),
                pltpu.VMEM((n // 2 - 1, slots, props, all_w), F32),
                pltpu.VMEM((n // 2 - 1, slots) + folded, BF16),
                pltpu.VMEM((gate_weight.shape[1], depth), BF16),
                pltpu.VMEM(out_weight.shape, BF16),
                pltpu.VMEM(cache_keys.shape, BF16),
                pltpu.VMEM(cache_values.shape, BF16),
                pltpu.VMEM((seqs,) + folded, BF16),
                pltpu.VMEM((seqs,) + folded, BF16),
                pltpu.VMEM((seqs, props, LANES), F32),
                pltpu.VMEM((n - 1, slots) + folded, BF16),
                pltpu.VMEM((n - 1, slots, props, LANES), F32),
                pltpu.VMEM((seqs,) + folded, BF16),
                pltpu.VMEM((slots, props, LANES), F32),
                pltpu.VMEM((slots, props, LANES), F32),
                pltpu.VMEM((slots, props, width), F32),
                pltpu.VMEM((slots, 2, props, LANES), F32),
                pltpu.VMEM((slots, 2, LANES, width), F32),
                pltpu.VMEM((n_tp, block, cols), BF16),
                pltpu.VMEM((n_tp - 1, block, cols), BF16),
                pltpu.VMEM((-(-seqs // 8) * 8, LANES), jnp.int32),
                dma((2,)),
                dma((2, seqs)),
                dma((2, seqs)),
                dma((2, seqs)),
                dma((2, seqs)),
                dma((2, n // 2 - 1, slots)),
                dma((slots, n - 1)),
                dma((seqs,)),
                dma((2, seqs)),
                dma((2, n - 1, slots)),
                dma((slots, n - 1)),
                dma((seqs,)),
                dma((n_tp,)),
                dma((n_tp - 1,)),
            ]
        return pl.pallas_call(
            body_of,
            out_shape=pltpu.VMEM((block, cols), BF16),
            in_specs=[hbm] * 13,
            out_specs=vmem,
            scratch_shapes=scratch,
            compiler_params=pltpu.CompilerParams(
                collective_id=0, has_side_effects=True, vmem_limit_bytes=67_043_328 - 131072
            ),
        )(
            tokens,
            norm_gain.reshape(1, depth),
            query_weight,
            key_weight,
            value_weight,
            gate_weight.T,
            gate_bias.reshape(1, gate_bias.shape[0]),
            out_weight,
            cache_keys,
            cache_values,
            cache_decay,
            lengths,
            parents,
        )

    in_specs = (
        P(None, "kv"),
        P("kv"),
        P("kv", "tp"),
        P("kv", "tp"),
        P("kv", "tp"),
        P(),
        P(),
        P("tp", "kv"),
        P(None, "kv", "tp"),
        P(None, "kv", "tp"),
        P(None, "tp", "kv"),
        P(),
        P(),
    )
    out_specs = P("tp", "kv")
    return jax.shard_map(body, mesh=mesh, in_specs=in_specs, out_specs=out_specs, check_vma=False)
```

```python
import functools
import math

import jax
import jax.numpy as jnp
from jax import lax
from jax.experimental import pallas as pl
from jax.experimental.pallas import tpu as pltpu
from jax.sharding import PartitionSpec as P

F32 = jnp.float32
BF16 = jnp.bfloat16
LANES = 128
LOW = -1e30
NT = (((1,), (1,)), ((), ()))
HIGH = lax.Precision.HIGHEST


def dot(a, b, precision=None):
    return jnp.dot(a, b, preferred_element_type=F32, precision=precision)


def dot_nt(a, b, precision=None):
    return lax.dot_general(a, b, NT, preferred_element_type=F32, precision=precision)


def fold(x):
    half = x.shape[1] // 2
    return jnp.concatenate([x[:, :half], x[:, half:]], axis=0)


def unfold(x):
    rows = x.shape[0] // 2
    x = x.astype(F32)
    return jnp.concatenate([x[:rows], x[rows:]], axis=1)


def by_sequence(
    n,
    n_tp,
    tokens_hbm,
    gain_hbm,
    query_hbm,
    key_hbm,
    value_hbm,
    gate_hbm,
    bias_hbm,
    out_hbm,
    keys_hbm,
    values_hbm,
    decay_hbm,
    lengths_hbm,
    parents_hbm,
    out,
    tokens,
    gain,
    query_w,
    key_w,
    value_w,
    bias,
    decay,
    lengths,
    parents,
    small_sem,
    part,
    part_v,
    pair_in,
    pair_in_v,
    part_in,
    part_in_v,
    gate_w,
    out_w,
    keys,
    values,
    qbuf,
    mix,
    stat,
    mix_in,
    stat_in,
    att,
    anc,
    path_s,
    tmix,
    tstat,
    kvnew,
    terms,
    terms_in,
    par_pad,
    load_sem,
    cache_sem,
    p_send,
    p_recv,
    a_send,
    a_recv,
    b_send,
    b_recv,
    c_send,
    c_recv,
    d_send,
    d_recv,
    e_send,
    e_recv,
):
    me = lax.axis_index("kv")
    tp = lax.axis_index("tp")
    rows, depth = tokens.shape
    seqs, props = parents.shape
    heads = decay.shape[1]
    pos_dev = keys.shape[1]
    width = query_w.shape[1]
    head_dim = width // heads
    scale = head_dim ** (-0.5)
    slots = part_in.shape[1]
    parity = lax.rem(tp, 2)
    left_over = seqs % n
    hp = heads * props

    barrier = pltpu.get_barrier_semaphore()
    for k in range(1, n):
        pl.semaphore_signal(barrier, inc=1, device_id={"kv": lax.rem(me + k, n)})
    for k in range(1, n_tp):
        pl.semaphore_signal(barrier, inc=1, device_id={"tp": lax.rem(tp + k, n_tp)})

    pairs = (
        (tokens_hbm, tokens),
        (gain_hbm, gain),
        (query_hbm, query_w),
        (key_hbm, key_w),
        (value_hbm, value_w),
        (bias_hbm, bias),
        (parents_hbm, parents),
        (decay_hbm, decay),
        (lengths_hbm, lengths),
    )
    small_loads = [
        pltpu.make_async_copy(src, dst, small_sem.at[i]) for i, (src, dst) in enumerate(pairs)
    ]
    for load in small_loads:
        load.start()
    gate_load = pltpu.make_async_copy(
        gate_hbm.at[:, pl.ds(pl.multiple_of(me * depth, depth), depth)], gate_w, load_sem.at[0]
    )
    gate_load.start()
    cache_loads = []
    for s in range(seqs):
        k_load = pltpu.make_async_copy(keys_hbm.at[s], keys.at[s], cache_sem.at[0, s])
        v_load = pltpu.make_async_copy(values_hbm.at[s], values.at[s], cache_sem.at[1, s])
        k_load.start()
        v_load.start()
        cache_loads.append((k_load, v_load))
    out_load = pltpu.make_async_copy(out_hbm, out_w, load_sem.at[1])
    out_load.start()

    def owner_of(s):
        if isinstance(s, int):
            place = s % n
            shift = parity * left_over if s // n == seqs // n else 0
        else:
            place = lax.rem(s, n)
            shift = jnp.where(lax.div(s, n) == seqs // n, parity * left_over, 0)
        return lax.rem(place + shift, n)

    def slot_seq(r):
        shift = parity * left_over if r == seqs // n else 0
        return r * n + lax.rem(me + 2 * n - shift, n)

    def for_slot(r, f):
        if (r + 1) * n <= seqs:
            f()
        else:
            pl.when(slot_seq(r) < seqs)(f)

    for load in small_loads:
        load.wait()
    xf = tokens[...].astype(F32)
    squares = jnp.sum(xf * xf, axis=1, keepdims=True)
    normed = (xf * gain[...]).astype(BF16)
    sel_rows = lax.broadcasted_iota(jnp.int32, (bias.shape[1], LANES), 0)
    sel_cols = lax.broadcasted_iota(jnp.int32, (bias.shape[1], LANES), 1)
    select = ((sel_rows == sel_cols + tp * heads) & (sel_cols < heads)).astype(F32)
    for i, w in enumerate((query_w, key_w)):
        part[:, :, i * width : (i + 1) * width] = dot(normed, w[...]).reshape(seqs, props, width)
    value_part = dot(normed, value_w[...])
    for s in range(seqs):
        part_v[s] = fold(value_part[s * props : (s + 1) * props]).astype(BF16)
    gate_load.wait()
    gates_w = lax.dot_general(
        select.astype(BF16), gate_w[...], (((0,), (0,)), ((), ())), preferred_element_type=F32
    )
    gate_part = dot_nt(normed, gates_w.astype(BF16))
    lane = lax.broadcasted_iota(jnp.int32, (rows, LANES), 1)
    gate_part = jnp.where(lane == LANES // 2, squares, gate_part)
    part[:, :, 2 * width :] = gate_part.reshape(seqs, props, LANES)
    pl.semaphore_wait(barrier, n + n_tp - 2)

    side = lax.rem(me, 2)
    partner = me + 1 - 2 * side
    n_far = n // 2
    shares = ((part, pair_in, part_in), (part_v, pair_in_v, part_in_v))

    def p_copy(s, which):
        src, dst, _ = shares[which]
        return pltpu.make_async_remote_copy(
            src_ref=src.at[s],
            dst_ref=dst.at[s],
            send_sem=p_send.at[which, s],
            recv_sem=p_recv.at[which, s],
            device_id={"kv": partner},
        )

    def a_copy(s, which):
        src, _, dst = shares[which]
        d = owner_of(s)
        k = jnp.maximum(lax.rem(lax.div(me, 2) - lax.div(d, 2) + n_far, n_far) - 1, 0)
        return pltpu.make_async_remote_copy(
            src_ref=src.at[s],
            dst_ref=dst.at[k, s // n],
            send_sem=a_send.at[which, s],
            recv_sem=a_recv.at[which, k, s // n],
            device_id={"kv": d},
        )

    def crosses(s):
        return lax.rem(owner_of(s), 2) != side

    def passes(s):
        d = owner_of(s)
        return (lax.rem(d, 2) == side) & (d != me)

    for s in range(seqs):
        for which in range(2):
            pl.when(crosses(s))(p_copy(s, which).start)

    par_pad[...] = jnp.zeros(par_pad.shape, jnp.int32)
    par_pad[0:seqs, 0:props] = parents[...]
    r_i = lax.broadcasted_iota(jnp.int32, (LANES, LANES), 0)
    c_i = lax.broadcasted_iota(jnp.int32, (LANES, LANES), 1)
    eye = (r_i == c_i).astype(F32)
    bias_row = dot(jnp.broadcast_to(bias[...], (8, bias.shape[1])), select, HIGH)[0:1]

    def ancestry(r):
        s = slot_seq(r)
        row = par_pad[pl.ds(s, 1), :]
        link = jnp.maximum((row == r_i).astype(F32), eye).astype(BF16)
        for _ in range(props.bit_length()):
            link = jnp.minimum(dot(link, link), 1.0).astype(BF16)
        anc[r] = dot_nt(eye.astype(BF16), link)[:props]

    for r in range(slots):
        for_slot(r, functools.partial(ancestry, r))

    def pass_on(s):
        for which in range(2):
            p_copy(s, which).wait_recv()
        part[s] = part[s] + pair_in[s]
        part_v[s] = (part_v[s].astype(F32) + pair_in_v[s].astype(F32)).astype(BF16)
        for which in range(2):
            a_copy(s, which).start()

    for s in range(seqs):
        pl.when(passes(s))(functools.partial(pass_on, s))

    lane_p = lax.broadcasted_iota(jnp.int32, (props, LANES), 1)
    bd_row = lax.broadcasted_iota(jnp.int32, (heads, props, width), 0)
    bd_col = lax.broadcasted_iota(jnp.int32, (heads, props, width), 2)
    diag = (lax.div(bd_col, head_dim) == bd_row).reshape(hp, width)

    def spread(q):
        wide = jnp.broadcast_to(q[None], (heads, props, width)).reshape(hp, width)
        return jnp.where(diag, wide, 0.0).astype(BF16)

    def gather_diag(m):
        return jnp.sum(jnp.where(diag, m, 0.0).reshape(heads, props, width), axis=0)

    def to_lanes(col, first):
        acc = jnp.zeros((props, LANES), F32)
        for h in range(heads):
            acc = jnp.where(lane_p == h + first, col[h * props : (h + 1) * props], acc)
        return acc

    def b_copy(r, k, buf, send, recv):
        s = slot_seq(r)
        return pltpu.make_async_remote_copy(
            src_ref=buf.at[s],
            dst_ref=buf.at[s],
            send_sem=send.at[r, k - 1],
            recv_sem=recv.at[s],
            device_id={"kv": lax.rem(me + k, n)},
        )

    pad_rows = LANES - props

    def project(r):
        s = slot_seq(r)
        for which, (src, near, far) in enumerate(shares):
            pltpu.make_async_remote_copy(
                src_ref=src.at[0],
                dst_ref=near.at[s],
                send_sem=p_send.at[which, 0],
                recv_sem=p_recv.at[which, s],
                device_id={"kv": partner},
            ).wait_recv()
            for k in range(1, n_far):
                pltpu.make_async_remote_copy(
                    src_ref=src.at[0],
                    dst_ref=far.at[k - 1, r],
                    send_sem=a_send.at[which, 0],
                    recv_sem=a_recv.at[which, k - 1, r],
                    device_id={"kv": lax.rem(me + 2 * k, n)},
                ).wait_recv()
        total = part[s] + pair_in[s]
        total_v = unfold(part_v[s]) + unfold(pair_in_v[s])
        for k in range(1, n_far):
            total = total + part_in[k - 1, r]
            total_v = total_v + unfold(part_in_v[k - 1, r])
        tail = total[:, 2 * width :]
        square = jnp.sum(jnp.where(lane_p == LANES // 2, tail, 0.0), axis=1, keepdims=True)
        inverse = lax.rsqrt(square / (depth * n) + 1e-06)
        q = inverse * total[:, :width]
        qbuf[s] = fold(q).astype(BF16)
        for k in range(1, n):
            b_copy(r, k, qbuf, b_send, b_recv).start()
        kvnew[r, 0, 0:props] = inverse * total[:, width : 2 * width]
        kvnew[r, 1, 0:props] = inverse * total_v
        kvnew[r, :, props:] = jnp.zeros((2, pad_rows, width), F32)
        x = inverse * tail + bias_row
        log_gate = jnp.minimum(x, 0.0) - jnp.log1p(jnp.exp(-jnp.abs(x)))
        padded = jnp.concatenate([log_gate, jnp.zeros((pad_rows, LANES), F32)], axis=0)
        path_s[r] = dot(anc[r], padded, HIGH)

    def tree(r):
        s = slot_seq(r)
        path = path_s[r]
        q = spread(unfold(qbuf[s]))
        head_of = lax.broadcasted_iota(jnp.int32, (heads, props, LANES), 0)
        lane_of = lax.broadcasted_iota(jnp.int32, (heads, props, LANES), 2)
        pick = (head_of == lane_of).reshape(hp, LANES)
        tiled = jnp.broadcast_to(path[None], (heads, props, LANES)).reshape(hp, LANES)
        own = jnp.sum(jnp.where(pick, tiled, 0.0), axis=1, keepdims=True)
        padded = jnp.concatenate([path, jnp.zeros((pad_rows, LANES), F32)], axis=0)
        other = dot_nt(pick.astype(F32), padded, HIGH)
        scores = dot_nt(q, kvnew[r, 0].astype(BF16)) * scale + own - other
        live = jnp.broadcast_to(anc[r][None], (heads, props, LANES)).reshape(hp, LANES) > 0.5
        scores = jnp.where(live, scores, LOW)
        top = jnp.max(scores, axis=1, keepdims=True)
        w = jnp.where(live, jnp.exp(scores - top), 0.0)
        total = jnp.sum(w, axis=1, keepdims=True)
        tmix[r] = gather_diag(dot(w.astype(BF16), kvnew[r, 1].astype(BF16)))
        tstat[r, 0] = to_lanes(top, 0)
        tstat[r, 1] = to_lanes(total, 0)

    position = lax.broadcasted_iota(jnp.int32, (hp, pos_dev), 1) + me * pos_dev

    def c_copy(s, which, src, dst):
        d = owner_of(s)
        k = jnp.maximum(lax.rem(me - d + n, n) - 1, 0)
        slot = s // n if isinstance(s, int) else lax.div(s, n)
        return d, pltpu.make_async_remote_copy(
            src_ref=src.at[s],
            dst_ref=dst.at[k, slot],
            send_sem=c_send.at[which, s],
            recv_sem=c_recv.at[which, k, slot],
            device_id={"kv": d},
        )

    def shard(s, carry):
        d = owner_of(s)

        @pl.when(d != me)
        def _():
            pltpu.make_async_remote_copy(
                src_ref=qbuf.at[s],
                dst_ref=qbuf.at[s],
                send_sem=b_send.at[0, 0],
                recv_sem=b_recv.at[s],
                device_id={"kv": d},
            ).wait_recv()

        pltpu.make_async_copy(keys_hbm.at[s], keys.at[s], cache_sem.at[0, s]).wait()
        pltpu.make_async_copy(values_hbm.at[s], values.at[s], cache_sem.at[1, s]).wait()
        q = spread(unfold(qbuf[s]))
        fade = decay[s]
        fade = jnp.concatenate(
            [jnp.broadcast_to(fade[h : h + 1], (props, pos_dev)) for h in range(heads)], axis=0
        )
        scores = dot_nt(q, keys[s]) * scale + fade
        live = position < lengths[s]
        scores = jnp.where(live, scores, LOW)
        top = jnp.max(scores, axis=1, keepdims=True)
        w = jnp.where(live, jnp.exp(scores - top), 0.0)
        total = jnp.sum(w, axis=1, keepdims=True)
        mix[s] = fold(gather_diag(dot(w.astype(BF16), values[s]))).astype(BF16)
        stat[s] = to_lanes(top, 0) + to_lanes(total, heads)
        for which, (src, dst) in enumerate(((mix, mix_in), (stat, stat_in))):
            _, copy = c_copy(s, which, src, dst)
            pl.when(d != me)(copy.start)
        return carry

    ex_r = lax.broadcasted_iota(jnp.int32, (LANES, width), 0)
    ex_c = lax.broadcasted_iota(jnp.int32, (LANES, width), 1)
    widen = (ex_r == lax.div(ex_c, head_dim)).astype(F32)

    def merge(r):
        s = slot_seq(r)
        for k in range(1, n):
            for which, (src, dst) in enumerate(((mix, mix_in), (stat, stat_in))):
                pltpu.make_async_remote_copy(
                    src_ref=src.at[0],
                    dst_ref=dst.at[k - 1, r],
                    send_sem=c_send.at[which, 0],
                    recv_sem=c_recv.at[which, k - 1, r],
                    device_id={"kv": lax.rem(me + k, n)},
                ).wait_recv()
        stats = jnp.concatenate([stat[s]] + [stat_in[k, r] for k in range(n - 1)], axis=0)
        totals = pltpu.roll(stats, LANES - heads, 1).reshape(n, props, LANES)
        tops = stats.reshape(n, props, LANES) + path_s[r][None]
        tops = jnp.where((lane_p < heads)[None], tops, LOW)
        ttop = jnp.where(lane_p < heads, tstat[r, 0], LOW)
        best = jnp.maximum(jnp.max(tops, axis=0), ttop)
        factors = jnp.exp(tops - best[None])
        tfactor = jnp.exp(ttop - best)
        denom = jnp.sum(factors * totals, axis=0) + tfactor * tstat[r, 1]
        packed = jnp.concatenate([factors.reshape(n * props, LANES), tfactor, denom], axis=0)
        wide = dot(packed, widen, HIGH)
        numer = wide[n * props : (n + 1) * props] * tmix[r] + wide[:props] * unfold(mix[s])
        for k in range(1, n):
            numer = numer + wide[k * props : (k + 1) * props] * unfold(mix_in[k - 1, r])
        att[s] = fold(numer / wide[(n + 1) * props :]).astype(BF16)
        for k in range(1, n):
            b_copy(r, k, att, d_send, d_recv).start()

    for r in range(slots):
        for_slot(r, functools.partial(project, r))
        if r > 0:
            for_slot(r - 1, functools.partial(merge, r - 1))
        for_slot(r, functools.partial(tree, r))
        lax.fori_loop(r * n, min((r + 1) * n, seqs), shard, 0)
    for_slot(slots - 1, functools.partial(merge, slots - 1))

    out_load.wait()
    block = rows // n_tp

    def e_copy(t):
        k = lax.rem(tp - t + n_tp, n_tp)
        return pltpu.make_async_remote_copy(
            src_ref=terms.at[t],
            dst_ref=terms_in.at[jnp.maximum(k - 1, 0)],
            send_sem=e_send.at[t],
            recv_sem=e_recv.at[jnp.maximum(k - 1, 0)],
            device_id={"tp": t},
        )

    arrived = 0
    for t in range(n_tp):
        first, last = t * block // props, ((t + 1) * block - 1) // props + 1
        for s in range(arrived, last):
            d = owner_of(s)

            @pl.when(d != me)
            def _(s=s, d=d):
                pltpu.make_async_remote_copy(
                    src_ref=att.at[s],
                    dst_ref=att.at[s],
                    send_sem=d_send.at[0, 0],
                    recv_sem=d_recv.at[s],
                    device_id={"kv": d},
                ).wait_recv()

        arrived = max(arrived, last)
        attended = jnp.concatenate([unfold(att[s]) for s in range(first, last)], axis=0)
        term = dot(attended.astype(BF16), out_w[...])
        begin = t * block - first * props
        terms[t] = term[begin : begin + block].astype(BF16)
        pl.when(tp != t)(e_copy(t).start)
    total = terms[tp].astype(F32)
    for k in range(1, n_tp):
        pltpu.make_async_remote_copy(
            src_ref=terms.at[0],
            dst_ref=terms_in.at[k - 1],
            send_sem=e_send.at[0],
            recv_sem=e_recv.at[k - 1],
            device_id={"tp": lax.rem(tp + k, n_tp)},
        ).wait_recv()
        total = total + terms_in[k - 1].astype(F32)
    out[...] = total.astype(BF16)

    for s in range(seqs):
        d = owner_of(s)
        for which in range(2):
            pl.when(crosses(s))(p_copy(s, which).wait_send)
            pl.when(passes(s))(a_copy(s, which).wait_send)
        for which, (src, dst) in enumerate(((mix, mix_in), (stat, stat_in))):
            _, copy = c_copy(s, which, src, dst)
            pl.when(d != me)(copy.wait_send)
    for r in range(slots):

        def drain(r=r):
            for k in range(1, n):
                b_copy(r, k, qbuf, b_send, b_recv).wait_send()
                b_copy(r, k, att, d_send, d_recv).wait_send()

        for_slot(r, drain)
    for t in range(n_tp):
        pl.when(tp != t)(e_copy(t).wait_send)


def split3(x):
    high = x.astype(BF16)
    rest = x - high.astype(F32)
    mid = rest.astype(BF16)
    low = (rest - mid.astype(F32)).astype(BF16)
    return high, mid, low


def tile_rows(rows, total):
    return jnp.concatenate([rows, jnp.zeros((total - rows.shape[0], rows.shape[1]), rows.dtype)], axis=0)


def by_heads(
    n,
    n_tp,
    wave,
    tokens_hbm,
    gain_hbm,
    query_hbm,
    key_hbm,
    value_hbm,
    gate_hbm,
    bias_hbm,
    out_hbm,
    keys_hbm,
    values_hbm,
    decay_hbm,
    lengths_hbm,
    parents_hbm,
    out,
    tokens,
    gain,
    query_w,
    key_w,
    value_w,
    gate_w,
    bias,
    decay,
    lengths,
    parents,
    out_w,
    keys,
    values,
    feats,
    q_out,
    q_in,
    q_own,
    q_far,
    q_last,
    q_last_in,
    q_cross,
    kv_out,
    kv_in,
    kv_own,
    kv_pass,
    kv_far,
    qbuf,
    mix,
    mix_in,
    stat,
    stat_in,
    att,
    terms,
    terms_in,
    par_pad,
    link_s,
    anc_s,
    path_s,
    inv_s,
    tmix,
    tstat,
    held,
    swap,
    swap_in,
    swap_stat,
    swap_stat_in,
    widen,
    load_sem,
    cache_sem,
    qx_send,
    qx_recv,
    kx_send,
    kx_recv,
    qz_send,
    qz_recv,
    kz_send,
    kz_recv,
    b_send,
    b_recv,
    c_send,
    c_recv,
    d_send,
    d_recv,
    e_send,
    e_recv,
    qr_send,
    qr_recv,
    s_send,
    s_recv,
    l_send,
    l_recv,
):
    me = lax.axis_index("kv")
    tp = lax.axis_index("tp")
    side = lax.rem(me, 2)
    far = lax.div(me, 2)
    n_far = n // 2
    rows, depth = tokens.shape
    seqs, props = parents.shape
    heads = decay.shape[1]
    pos_dev = keys.shape[1]
    width = query_w.shape[1]
    head_dim = width // heads
    scale = head_dim ** (-0.5)
    exact_scale = math.frexp(scale)[0] == 0.5
    own_heads = heads // n_far
    cols = width // n_far
    half_seqs = seqs // 2
    half = rows // 2
    waves = half_seqs // wave
    wrows = wave * props
    sources = n - 1

    pairs = (
        (tokens_hbm, tokens),
        (gain_hbm, gain),
        (gate_hbm.at[:, pl.ds(pl.multiple_of(me * depth, depth), depth)], gate_w),
        (query_hbm, query_w),
        (key_hbm, key_w),
        (value_hbm, value_w),
        (bias_hbm, bias),
        (parents_hbm, parents),
        (lengths_hbm, lengths),
        (decay_hbm, decay),
        (out_hbm, out_w),
    )
    loads = [pltpu.make_async_copy(src, dst, load_sem.at[i]) for i, (src, dst) in enumerate(pairs)]
    load_of = dict(
        zip(("tokens", "gain", "gate", "q", "k", "v", "bias", "parents", "lengths", "decay", "out"), loads)
    )
    for load in loads[:6]:
        load.start()
    barrier = pltpu.get_barrier_semaphore()
    for k in range(1, n):
        pl.semaphore_signal(barrier, inc=1, device_id={"kv": lax.rem(me + k, n)})
    for k in range(1, n_tp):
        pl.semaphore_signal(barrier, inc=1, device_id={"tp": lax.rem(tp + k, n_tp)})

    def iota(shape, dim):
        return lax.broadcasted_iota(jnp.int32, shape, dim)

    def far_id(d):
        return lax.rem(far + d, n_far)

    def near_id(z, x):
        return {"kv": z * 2 + x}

    own_half = pl.multiple_of(side * half, half)
    peer_half = pl.multiple_of((1 - side) * half, half)

    load_of["tokens"].wait()
    load_of["gain"].wait()
    for load in loads[6:]:
        load.start()
    for s in range(seqs):
        pltpu.make_async_copy(keys_hbm.at[s], keys.at[s], cache_sem.at[0, s]).start()
        pltpu.make_async_copy(values_hbm.at[s], values.at[s], cache_sem.at[1, s]).start()
    xf = tokens[...].astype(F32)
    feats[:, :depth] = (xf * gain[...]).astype(BF16)
    square = xf * xf
    high = square.astype(BF16)
    feats[:, depth : 2 * depth] = high
    feats[:, 2 * depth :] = (square - high.astype(F32)).astype(BF16)

    load_of["gate"].wait()
    t_rows = n_far * 8
    p_row = iota((t_rows, gate_w.shape[0]), 0)
    p_col = iota((t_rows, gate_w.shape[0]), 1)
    p_in = lax.rem(p_row, 8)
    wanted = (p_in < own_heads) & (p_col == tp * heads + lax.div(p_row, 8) * own_heads + p_in)
    gates = dot(wanted.astype(BF16), gate_w[...]).astype(BF16)
    ones = (lax.rem(iota((t_rows, depth), 0), 8) == own_heads).astype(BF16)
    tails = jnp.concatenate([gates, ones, ones], axis=1)

    def project_q(base, dst, which):
        full = dot(feats[pl.ds(base, half), :depth], query_w[...])
        for i in range(waves):
            piece = full[i * wrows : (i + 1) * wrows]
            tail = dot_nt(tails, feats[pl.ds(base + i * wrows, wrows), :])
            tail = jnp.concatenate([tail, jnp.zeros((t_rows, LANES - wrows), F32)], axis=1)
            for f in range(n_far):
                for at, rows_of in (
                    (slice(0, wrows), piece[:, f * cols : (f + 1) * cols]),
                    (slice(wrows, wrows + 8), tail[f * 8 : (f + 1) * 8]),
                ):
                    if i < waves - 1:
                        dst[i, f, at] = rows_of
                    else:
                        q_last[f, which, at] = rows_of

    def project_kv(base, dst):
        for which, w in enumerate((key_w, value_w)):
            full = dot(feats[pl.ds(base, half), :depth], w[...])
            for i in range(waves):
                piece = full[i * wrows : (i + 1) * wrows].astype(dst.dtype)
                for f in range(n_far):
                    dst[i, f, which * wrows : (which + 1) * wrows] = piece[:, f * cols : (f + 1) * cols]

    def x_copy(i, src, dst, send, recv):
        return pltpu.make_async_remote_copy(
            src_ref=src.at[i],
            dst_ref=dst.at[i],
            send_sem=send.at[i],
            recv_sem=recv.at[i],
            device_id=near_id(far, 1 - side),
        )

    def z_copy(i, d, src, dst, send, recv):
        return pltpu.make_async_remote_copy(
            src_ref=src.at[i, far_id(d)],
            dst_ref=dst.at[d - 1, i],
            send_sem=send.at[d - 1, i],
            recv_sem=recv.at[d - 1, i],
            device_id=near_id(far_id(d), side),
        )

    def last_copy(d):
        return pltpu.make_async_remote_copy(
            src_ref=q_last.at[far_id(d)],
            dst_ref=q_last_in.at[d - 1],
            send_sem=l_send.at[d - 1],
            recv_sem=l_recv.at[d - 1],
            device_id=near_id(far_id(d), side),
        )

    def last_cross():
        return pltpu.make_async_remote_copy(
            src_ref=q_last.at[far, 1],
            dst_ref=q_cross,
            send_sem=l_send.at[n_far - 1],
            recv_sem=l_recv.at[n_far - 1],
            device_id=near_id(far, 1 - side),
        )

    load_of["q"].wait()
    project_q(peer_half, q_out, 1)
    pl.semaphore_wait(barrier, n + n_tp - 2)
    for i in range(waves - 1):
        x_copy(i, q_out, q_in, qx_send, qx_recv).start()
    project_q(own_half, q_own, 0)
    for d in range(1, n_far):
        last_copy(d).start()
    load_of["k"].wait()
    load_of["v"].wait()
    project_kv(peer_half, kv_out)
    for i in range(waves):
        x_copy(i, kv_out, kv_in, kx_send, kx_recv).start()
    project_kv(own_half, kv_own)

    load_of["bias"].wait()
    load_of["parents"].wait()
    load_of["lengths"].wait()
    load_of["decay"].wait()
    par_pad[...] = jnp.zeros(par_pad.shape, jnp.int32)
    par_pad[0:seqs, 0:props] = parents[...]
    r_i = iota((LANES, LANES), 0)
    c_i = iota((LANES, LANES), 1)
    lane1 = iota((1, LANES), 1)
    eye = r_i == c_i
    for i in range(waves):
        row = jnp.full((1, LANES), -1, jnp.int32)
        for j in range(wave):
            of = par_pad[pl.ds(side * half_seqs + i * wave + j, 1), :]
            if j:
                of = pltpu.roll(jnp.broadcast_to(of, (8, LANES)), j * props, 1)[0:1]
            inside = (lane1 >= j * props) & (lane1 < (j + 1) * props)
            row = jnp.where(inside, of + j * props, row)
        link = ((row == r_i) | eye).astype(F32).astype(BF16)
        for _ in range(props.bit_length()):
            link = jnp.minimum(dot(link, link), 1.0).astype(BF16)
        link_s[i] = link
        anc_s[i] = dot_nt(eye.astype(F32).astype(BF16), link)
    w_row = lax.rem(iota(widen.shape, 0), LANES)
    w_col = iota(widen.shape, 1)
    w_src = lax.div(w_col, cols) * 8 + lax.div(lax.rem(w_col, cols), head_dim)
    widen[...] = (w_row == w_src).astype(F32).astype(BF16)
    b_shape = (8, bias.shape[1])
    b_row, b_col = iota(b_shape, 0), iota(b_shape, 1)
    mine = (b_row < own_heads) & (b_col == tp * heads + far * own_heads + b_row)
    bias_col = jnp.sum(jnp.where(mine, jnp.broadcast_to(bias[...], b_shape), 0.0), axis=1, keepdims=True)

    for i in range(waves - 1):
        x_copy(i, q_out, q_in, qx_send, qx_recv).wait_recv()
        q_own[i] = q_own[i] + q_in[i]
        for d in range(1, n_far):
            z_copy(i, d, q_own, q_far, qz_send, qz_recv).start()
    for d in range(1, n_far):
        last_copy(d).wait_recv()
    q_last[far] = q_last[far] + functools.reduce(jnp.add, [q_last_in[d] for d in range(n_far - 1)])
    last_cross().start()

    targets = [(d, 0) for d in range(1, n_far)] + [(d, 1) for d in range(n_far)]

    def target_id(d, cross):
        return near_id(far_id(d), side if not cross else 1 - side)

    def spread_copy(i, t, buf, send, recv):
        d, cross = targets[t]
        block = side * waves + i
        return pltpu.make_async_remote_copy(
            src_ref=buf.at[block, far],
            dst_ref=buf.at[block, far],
            send_sem=send.at[t, i],
            recv_sem=recv.at[block, far],
            device_id=target_id(d, cross),
        )

    def relay_copy(i, buf, send, recv):
        block = side * waves + i
        return pltpu.make_async_remote_copy(
            src_ref=buf.at[block],
            dst_ref=buf.at[block],
            send_sem=send.at[i],
            recv_sem=recv.at[i],
            device_id=near_id(far, 1 - side),
        )

    def spread(i, direct, buf, send, recv):
        for t in range(sources if direct else n_far - 1):
            spread_copy(i, t, buf, send, recv).start()

    def sent(i, direct, buf, send, recv, r_send, r_recv):
        for t in range(sources if direct else n_far - 1):
            spread_copy(i, t, buf, send, recv).wait_send()
        if not direct:
            relay_copy(i, buf, r_send, r_recv).wait_send()

    def spread_wait(i, t, buf, send, recv):
        d, cross = targets[t]
        block = (1 - side if cross else side) * waves + i
        pltpu.make_async_remote_copy(
            src_ref=buf.at[block, far_id(d)],
            dst_ref=buf.at[block, far_id(d)],
            send_sem=send.at[t, i],
            recv_sem=recv.at[block, far_id(d)],
            device_id=target_id(d, cross),
        ).wait_recv()

    def pass_on(i, direct, buf, send, recv, r_send, r_recv):
        for t in range(n_far - 1):
            spread_wait(i, t, buf, send, recv)
        if not direct:
            relay_copy(i, buf, r_send, r_recv).start()

    def crossed(i, direct, buf, send, recv, r_send, r_recv):
        if not direct:
            relay_copy(i, buf, r_send, r_recv).wait_recv()
            return
        for t in range(n_far - 1, sources):
            spread_wait(i, t, buf, send, recv)

    q_route = (qbuf, b_send, b_recv, qr_send, qr_recv)
    zone = n_far // 2
    place_in = lax.rem(far, zone)
    zone_of = lax.div(far, zone)
    near = [(d, 0) for d in range(1, zone)] + [(d, 1) for d in range(zone)]

    def place_at(d):
        return lax.rem(place_in + d, zone)

    def zone_id(d, cross):
        return near_id(zone_of * zone + place_at(d), 1 - side if cross else side)

    q_direct = [i == waves - 1 for i in range(waves)]

    strides = [1 << b for b in range(n_far.bit_length() - 1)]

    def halve_copy(i, st, m):
        slot = sum(n_far // (2 * x) for x in strides if x < st) + m
        partner = far + st - 2 * st * lax.rem(lax.div(far, st), 2)
        return pltpu.make_async_remote_copy(
            src_ref=kv_pass.at[i, lax.rem(partner, 2 * st) + 2 * st * m],
            dst_ref=kv_far.at[slot, i],
            send_sem=kz_send.at[slot, i],
            recv_sem=kz_recv.at[slot, i],
            device_id=near_id(partner, side),
        )

    def halve_start(i, st):
        partner = far + st - 2 * st * lax.rem(lax.div(far, st), 2)
        for m in range(n_far // (2 * st)):
            f = lax.rem(partner, 2 * st) + 2 * st * m
            kv_pass[i, f] = kv_own[i, f].astype(BF16)
            halve_copy(i, st, m).start()

    def halve_wait(i, st):
        for m in range(n_far // (2 * st)):
            halve_copy(i, st, m).wait_recv()
            f = lax.rem(far, 2 * st) + 2 * st * m
            slot = sum(n_far // (2 * x) for x in strides if x < st) + m
            kv_own[i, f] = kv_own[i, f] + kv_far[slot, i].astype(F32)

    def pass_kv(i, step):
        if step:
            halve_wait(i, strides[step - 1])
        else:
            x_copy(i, kv_out, kv_in, kx_send, kx_recv).wait_recv()
            kv_own[i] = kv_own[i] + kv_in[i].astype(F32)
        if step < len(strides):
            halve_start(i, strides[step])

    lane8 = iota((8, LANES), 1)
    row8 = iota((8, LANES), 0)

    def owner_q(i):
        if i < waves - 1:
            total = q_own[i, far]
            for d in range(1, n_far):
                z_copy(i, d, q_own, q_far, qz_send, qz_recv).wait_recv()
                total = total + q_far[d - 1, i]
        else:
            last_cross().wait_recv()
            total = q_last[far, 0] + q_cross[...]
        tail = total[wrows:]
        inverse = lax.rsqrt(tail / (depth * n) + 1e-06)
        column = tile_rows(inverse, LANES).T[:wrows, own_heads : own_heads + 1]
        inv_s[i] = jnp.broadcast_to(column, (wrows, cols))
        qbuf[side * waves + i, far] = (inv_s[i] * total[:wrows]).astype(BF16)
        spread(i, q_direct[i], qbuf, b_send, b_recv)
        inverse_row = jnp.broadcast_to(inverse[own_heads : own_heads + 1], (8, LANES))
        x = inverse_row * tail + bias_col
        log_gate = jnp.minimum(x, 0.0) - jnp.log1p(jnp.exp(-jnp.abs(x)))
        log_gate = jnp.where((row8 < own_heads) & (lane8 < wrows), log_gate, 0.0)
        parts = dot(jnp.concatenate(split3(log_gate), axis=0), link_s[i])
        path_s[i] = parts[:8] + parts[8:16] + parts[16:24]

    for i in range(waves):
        owner_q(i)
        if i < waves - 1:
            pass_kv(i, 0)

    group = min(heads, 256 // head_dim)
    gwidth = group * head_dim
    g_head = iota((group, props, gwidth), 0)
    g_col = lax.div(iota((group, props, gwidth), 2), head_dim)
    g_diag = (g_head == g_col).reshape(group * props, gwidth)
    lane_w = iota((wrows, LANES), 1)
    position = iota((heads, pos_dev), 1) + me * pos_dev

    def mix_copy(i, t, which, src, dst):
        d, cross = near[t]
        block = (1 - side if cross else side) * waves + i
        return pltpu.make_async_remote_copy(
            src_ref=src.at[block, place_at(d)],
            dst_ref=dst.at[t, i],
            send_sem=c_send.at[which, t, i],
            recv_sem=c_recv.at[which, t, i],
            device_id=zone_id(d, cross),
        )

    def attend(i, cross):
        place = 1 - side if cross else side
        block = place * waves + i
        if cross:
            crossed(i, q_direct[i], *q_route)
        first = place * half_seqs + i * wave
        for j in range(wave):
            s = first + j
            pltpu.make_async_copy(keys_hbm.at[s], keys.at[s], cache_sem.at[0, s]).wait()
            pltpu.make_async_copy(values_hbm.at[s], values.at[s], cache_sem.at[1, s]).wait()
        q_wave = jnp.concatenate([qbuf[block, f] for f in range(n_far)], axis=1).astype(F32)
        if exact_scale:
            q_wave = q_wave * scale
        chains = [(j, g) for j in range(wave) for g in range(heads // group)]
        scores_of, w_of, tops, totals, parts = {}, {}, {}, {}, {}
        for j in range(wave):
            s = first + j
            fade = jnp.where(position < lengths[s], decay[s], LOW)
            for g in range(heads // group):
                q = q_wave[j * props : (j + 1) * props, g * gwidth : (g + 1) * gwidth]
                q = jnp.broadcast_to(q[None], (group, props, gwidth)).reshape(group * props, gwidth)
                q = jnp.where(g_diag, q, 0.0).astype(BF16)
                scores = dot_nt(q, keys[s, :, g * gwidth : (g + 1) * gwidth])
                if not exact_scale:
                    scores = scores * scale
                fades = [
                    jnp.broadcast_to(fade[h : h + 1], (props, pos_dev))
                    for h in range(g * group, (g + 1) * group)
                ]
                scores_of[j, g] = scores + jnp.concatenate(fades, axis=0)
        for j, g in chains:
            top = jnp.max(scores_of[j, g], axis=1, keepdims=True)
            w = jnp.exp(scores_of[j, g] - top)
            total = jnp.sum(w, axis=1, keepdims=True)
            w_of[j, g] = w.astype(BF16)
            for h in range(group):
                tops[j, g * group + h] = top[h * props : (h + 1) * props]
                totals[j, g * group + h] = total[h * props : (h + 1) * props]
        for j, g in chains:
            m = dot(w_of[j, g], values[first + j, :, g * gwidth : (g + 1) * gwidth])
            m = jnp.where(g_diag, m, 0.0).reshape(group, props, gwidth)
            parts[j, g] = jnp.sum(m, axis=0)
        mixes = [
            jnp.concatenate([parts[j, g] for g in range(heads // group)], axis=1) for j in range(wave)
        ]
        mixed = jnp.concatenate(mixes, axis=0).astype(BF16)
        for f in range(n_far):
            mix[block, f % zone, f // zone] = mixed[:, f * cols : (f + 1) * cols]
        acc = jnp.zeros((wrows, LANES), F32)
        for h in range(heads):
            f, k = divmod(h, own_heads)
            for at, cols_of in ((k, tops), (own_heads + k, totals)):
                col = jnp.concatenate([cols_of[j, h] for j in range(wave)], axis=0)
                acc = jnp.where(lane_w == f * 8 + at, col, acc)
        flat = tile_rows(acc, LANES).T
        for f in range(n_far):
            stat[block, f % zone, f // zone] = flat[f * 8 : f * 8 + stat.shape[3]]
        for t in range(len(near)):
            if near[t][1] == cross:
                mix_copy(i, t, 0, mix, mix_in).start()
                mix_copy(i, t, 1, stat, stat_in).start()

    own_head_of = lax.div(iota((wrows, cols), 1), head_dim)

    def tree(i):
        block = side * waves + i
        pass_kv(i, len(strides))
        total = kv_own[i, far]
        new_k = tile_rows(inv_s[i] * total[:wrows], LANES).astype(BF16)
        new_v = tile_rows(inv_s[i] * total[wrows:], LANES).astype(BF16)
        q = qbuf[block, far].astype(F32)
        q = jnp.concatenate([jnp.where(own_head_of == h, q, 0.0) for h in range(own_heads)], axis=0)
        scores = dot_nt(q.astype(BF16), new_k) * scale
        path = path_s[i]
        shifts = [jnp.broadcast_to(-path[h : h + 1], (wrows, LANES)) for h in range(own_heads)]
        scores = scores + jnp.concatenate(shifts, axis=0)
        live = jnp.concatenate([anc_s[i, :wrows]] * own_heads, axis=0) > 0.5
        scores = jnp.where(live, scores, LOW)
        top = jnp.max(scores, axis=1, keepdims=True)
        w = jnp.where(live, jnp.exp(scores - top), 0.0)
        total = jnp.sum(w, axis=1, keepdims=True)
        m = dot(w.astype(BF16), new_v)
        merged = jnp.zeros((wrows, cols), F32)
        acc = jnp.zeros((wrows, LANES), F32)
        for h in range(own_heads):
            part = slice(h * wrows, (h + 1) * wrows)
            merged = jnp.where(own_head_of == h, m[part], merged)
            acc = jnp.where(lane_w == h, top[part], acc)
            acc = jnp.where(lane_w == own_heads + h, total[part], acc)
        tmix[i] = merged
        tstat[i] = tile_rows(acc, LANES).T[:8]

    def swap_copy(i, which, src, dst):
        return pltpu.make_async_remote_copy(
            src_ref=src.at[i],
            dst_ref=dst.at[i],
            send_sem=s_send.at[which, i],
            recv_sem=s_recv.at[which, i],
            device_id=near_id((1 - zone_of) * zone + place_in, side),
        )

    def turn(tiles):
        flat = jnp.concatenate([jnp.where(row8 < own_heads, x, 0.0) for x in tiles], axis=0)
        turned = tile_rows(flat, LANES).T[:wrows]
        high = turned.astype(BF16)
        low = (turned - high.astype(F32)).astype(BF16)
        both = jnp.concatenate([high, low], axis=1)
        return dot(both, widen[:, : len(tiles) * cols])

    def lift(st):
        return pltpu.roll(st, 8 - own_heads, 0)

    def weigh(wide, first, parts):
        total = jnp.zeros((wrows, cols), F32)
        for k, m in enumerate(parts):
            at = (first + k) * cols
            total = total + wide[:, at : at + cols] * m.astype(F32)
        return total

    def merge(i):
        block = side * waves + i
        for t in range(len(near)):
            mix_copy(i, t, 0, mix, mix_in).wait_recv()
            mix_copy(i, t, 1, stat, stat_in).wait_recv()
        tiles = []
        for k in range(2):
            stats = [stat[block, place_in, k]] + [stat_in[t, i, k] for t in range(len(near))]
            stats = [tile_rows(st, 8) for st in stats]
            absent = jnp.where(row8 < own_heads, LOW, 0.0)
            stats.append(jnp.where(zone_of == k, tstat[i], absent))
            best = functools.reduce(jnp.maximum, stats)
            factors = [jnp.exp(st - best) for st in stats]
            total = functools.reduce(jnp.add, [f * lift(st) for f, st in zip(factors, stats)])
            packed = jnp.where(row8 < own_heads, best, pltpu.roll(total, own_heads, 0))
            swap_stat[i, k] = packed[: swap_stat.shape[2]]
            tiles += factors
        wide = turn(tiles)
        for k in range(2):
            parts = [mix[block, place_in, k]] + [mix_in[t, i, k] for t in range(len(near))] + [tmix[i]]
            held[i, k] = weigh(wide, k * len(parts), parts)
            swap[i, k] = held[i, k].astype(BF16)
        swap_copy(i, 0, swap, swap_in).start()
        swap_copy(i, 1, swap_stat, swap_stat_in).start()

    def att_copy(i, t, block, place):
        d, cross = near[t]
        return pltpu.make_async_remote_copy(
            src_ref=att.at[block, place],
            dst_ref=att.at[block, place],
            send_sem=d_send.at[t, i],
            recv_sem=d_recv.at[block, place],
            device_id=zone_id(d, cross),
        )

    def finish(i):
        block = side * waves + i
        swap_copy(i, 0, swap, swap_in).wait_recv()
        swap_copy(i, 1, swap_stat, swap_stat_in).wait_recv()
        tiles = []
        for k in range(2):
            stats = [tile_rows(st[i, k], 8) for st in (swap_stat, swap_stat_in)]
            best = jnp.maximum(stats[0], stats[1])
            factors = [jnp.exp(st - best) for st in stats]
            denom = functools.reduce(jnp.add, [f * lift(st) for f, st in zip(factors, stats)])
            tiles += [f / denom for f in factors]
        wide = turn(tiles)
        for k in range(2):
            att[block, place_in, k] = weigh(wide, 2 * k, (held[i, k], swap_in[i, k])).astype(BF16)
        for t in range(len(near)):
            att_copy(i, t, block, place_in).start()

    per_tp = seqs // n_tp

    def e_copy(s, t):
        k = jnp.maximum(lax.rem(tp - t + n_tp, n_tp) - 1, 0)
        return pltpu.make_async_remote_copy(
            src_ref=terms.at[s],
            dst_ref=terms_in.at[k, lax.rem(s, per_tp)],
            send_sem=e_send.at[s],
            recv_sem=e_recv.at[k, lax.rem(s, per_tp)],
            device_id={"tp": t},
        )

    def output(i, cross):
        place = 1 - side if cross else side
        block = place * waves + i
        for t, (d, over) in enumerate(near):
            if over == cross:
                att_copy(i, t, block, place_at(d)).wait_recv()
        attended = jnp.concatenate([att[block, f % zone, f // zone] for f in range(n_far)], axis=1)
        term = dot(attended, out_w[...])
        for j in range(wave):
            s = place * half_seqs + i * wave + j
            terms[s] = fold(term[j * props : (j + 1) * props]).astype(BF16)
            t = lax.div(s, per_tp)
            pl.when(tp != t)(e_copy(s, t).start)

    advanced = [0] * waves

    def advance(count):
        for i in range(waves):
            if count and advanced[i] + 1 < len(strides):
                advanced[i] += 1
                pass_kv(i, advanced[i])
                count -= 1

    pass_on(0, q_direct[0], *q_route)
    attend(0, 0)
    pass_kv(waves - 1, 0)
    advance(1)
    for i in range(1, waves):
        pass_on(i, q_direct[i], *q_route)
        if i == 1:
            attend(1, 0)
            advance(1)
    attend(0, 1)
    advance(1)
    for i in range(1, waves):
        if i == waves - 1:
            for k in range(2, waves):
                attend(k, 0)
        attend(i, 1)
    advance(waves * len(strides))
    load_of["out"].wait()
    for i in range(waves):
        tree(i)
        merge(i)
    for i in range(waves):
        finish(i)
    for i in range(waves):
        output(i, 0)
        output(i, 1)

    done = []
    for j in range(per_tp):
        total = unfold(terms[tp * per_tp + j])
        for k in range(1, n_tp):
            pltpu.make_async_remote_copy(
                src_ref=terms.at[0],
                dst_ref=terms_in.at[k - 1, j],
                send_sem=e_send.at[0],
                recv_sem=e_recv.at[k - 1, j],
                device_id={"tp": lax.rem(tp + k, n_tp)},
            ).wait_recv()
            total = total + unfold(terms_in[k - 1, j])
        done.append(total)
    out[...] = jnp.concatenate(done, axis=0).astype(BF16)

    for i in range(waves):
        if i < waves - 1:
            x_copy(i, q_out, q_in, qx_send, qx_recv).wait_send()
            for d in range(1, n_far):
                z_copy(i, d, q_own, q_far, qz_send, qz_recv).wait_send()
        x_copy(i, kv_out, kv_in, kx_send, kx_recv).wait_send()
        for st in strides:
            for m in range(n_far // (2 * st)):
                halve_copy(i, st, m).wait_send()
        sent(i, q_direct[i], *q_route)
        swap_copy(i, 0, swap, swap_in).wait_send()
        swap_copy(i, 1, swap_stat, swap_stat_in).wait_send()
        for t in range(len(near)):
            att_copy(i, t, side * waves + i, place_in).wait_send()
            mix_copy(i, t, 0, mix, mix_in).wait_send()
            mix_copy(i, t, 1, stat, stat_in).wait_send()
    for d in range(1, n_far):
        last_copy(d).wait_send()
    last_cross().wait_send()
    for s in range(seqs):
        t = s // per_tp
        pl.when(tp != t)(e_copy(s, t).wait_send)


def wave_size(n, n_tp, seqs, props, heads, width):
    n_far = n // 2
    if n < 4 or n & (n - 1) or seqs % 2 or seqs % n_tp or heads % n_far or width % (n_far * LANES):
        return 0
    head_dim = width // heads
    own = heads // n_far
    if own > 4 or 16 * (n_far + 1) > LANES or (heads % min(heads, max(256 // head_dim, 1))):
        return 0
    for wave in range(1, seqs // 2 + 1):
        fits = wave * props % 16 == 0 and wave * props <= LANES
        if seqs // 2 % wave == 0 and fits and props % 8 == 0:
            return wave
    return 0


def solution(mesh):
    n, n_tp = mesh.shape["kv"], mesh.shape["tp"]

    def body(
        tokens,
        norm_gain,
        query_weight,
        key_weight,
        value_weight,
        gate_weight,
        gate_bias,
        out_weight,
        cache_keys,
        cache_values,
        cache_decay,
        lengths,
        parents,
    ):
        rows, depth = tokens.shape
        seqs, props = parents.shape
        heads = cache_decay.shape[1]
        pos_dev = cache_keys.shape[1]
        width = query_weight.shape[1]
        cols = out_weight.shape[1]
        slots = -(-seqs // n)
        block = rows // n_tp
        all_w = 2 * width + LANES
        folded = (2 * props, width // 2)
        vmem = pl.BlockSpec(memory_space=pltpu.VMEM)
        hbm = pl.BlockSpec(memory_space=pltpu.HBM)
        dma = pltpu.SemaphoreType.DMA
        wave = wave_size(n, n_tp, seqs, props, heads, width)
        if wave:
            n_far = n // 2
            waves = seqs // 2 // wave
            q_waves = max(waves - 1, 1)
            zone = n_far // 2
            wrows = wave * props
            wcols = width // n_far
            per_tp = seqs // n_tp
            s_rows = max(4, 2 * (heads // n_far))
            block_q = (n_far, wrows + 8, wcols)
            block_kv = (n_far, 2 * wrows, wcols)
            body_of = functools.partial(by_heads, n, n_tp, wave)
            scratch = [
                pltpu.VMEM(tokens.shape, BF16),
                pltpu.VMEM((1, depth), F32),
                pltpu.VMEM(query_weight.shape, BF16),
                pltpu.VMEM(key_weight.shape, BF16),
                pltpu.VMEM(value_weight.shape, BF16),
                pltpu.VMEM((gate_weight.shape[1], depth), BF16),
                pltpu.VMEM((1, gate_bias.shape[0]), F32),
                pltpu.VMEM(cache_decay.shape, F32),
                pltpu.SMEM(lengths.shape, jnp.int32),
                pltpu.VMEM(parents.shape, jnp.int32),
                pltpu.VMEM(out_weight.shape, BF16),
                pltpu.VMEM(cache_keys.shape, BF16),
                pltpu.VMEM(cache_values.shape, BF16),
                pltpu.VMEM((rows, 3 * depth), BF16),
                pltpu.VMEM((q_waves,) + block_q, F32),
                pltpu.VMEM((q_waves,) + block_q, F32),
                pltpu.VMEM((q_waves,) + block_q, F32),
                pltpu.VMEM((n_far - 1, q_waves) + block_q[1:], F32),
                pltpu.VMEM((n_far, 2) + block_q[1:], F32),
                pltpu.VMEM((n_far - 1, 2) + block_q[1:], F32),
                pltpu.VMEM(block_q[1:], F32),
                pltpu.VMEM((waves,) + block_kv, BF16),
                pltpu.VMEM((waves,) + block_kv, BF16),
                pltpu.VMEM((waves,) + block_kv, F32),
                pltpu.VMEM((waves,) + block_kv, BF16),
                pltpu.VMEM((n_far - 1, waves) + block_kv[1:], BF16),
                pltpu.VMEM((2 * waves, n_far, wrows, wcols), BF16),
                pltpu.VMEM((2 * waves, zone, 2, wrows, wcols), BF16),
                pltpu.VMEM((n_far - 1, waves, 2, wrows, wcols), BF16),
                pltpu.VMEM((2 * waves, zone, 2, s_rows, LANES), F32),
                pltpu.VMEM((n_far - 1, waves, 2, s_rows, LANES), F32),
                pltpu.VMEM((2 * waves, zone, 2, wrows, wcols), BF16),
                pltpu.VMEM((seqs,) + folded, BF16),
                pltpu.VMEM((n_tp - 1, per_tp) + folded, BF16),
                pltpu.VMEM((-(-seqs // 8) * 8, LANES), jnp.int32),
                pltpu.VMEM((waves, LANES, LANES), BF16),
                pltpu.VMEM((waves, LANES, LANES), F32),
                pltpu.VMEM((waves, 8, LANES), F32),
                pltpu.VMEM((waves, wrows, wcols), F32),
                pltpu.VMEM((waves, wrows, wcols), F32),
                pltpu.VMEM((waves, 8, LANES), F32),
                pltpu.VMEM((waves, 2, wrows, wcols), F32),
                pltpu.VMEM((waves, 2, wrows, wcols), BF16),
                pltpu.VMEM((waves, 2, wrows, wcols), BF16),
                pltpu.VMEM((waves, 2, s_rows, LANES), F32),
                pltpu.VMEM((waves, 2, s_rows, LANES), F32),
                pltpu.VMEM((2 * LANES, 2 * (n_far + 1) * wcols), BF16),
                dma((11,)),
                dma((2, seqs)),
                dma((waves,)),
                dma((waves,)),
                dma((waves,)),
                dma((waves,)),
                dma((n_far - 1, waves)),
                dma((n_far - 1, waves)),
                dma((n_far - 1, waves)),
                dma((n_far - 1, waves)),
                dma((n - 1, waves)),
                dma((2 * waves, n_far)),
                dma((2, n_far - 1, waves)),
                dma((2, n_far - 1, waves)),
                dma((n_far - 1, waves)),
                dma((2 * waves, zone)),
                dma((seqs,)),
                dma((n_tp - 1, per_tp)),
                dma((waves,)),
                dma((waves,)),
                dma((2, waves)),
                dma((2, waves)),
                dma((n_far,)),
                dma((n_far,)),
            ]
        else:
            body_of = functools.partial(by_sequence, n, n_tp)
            scratch = [
                pltpu.VMEM(tokens.shape, BF16),
                pltpu.VMEM((1, depth), F32),
                pltpu.VMEM(query_weight.shape, BF16),
                pltpu.VMEM(key_weight.shape, BF16),
                pltpu.VMEM(value_weight.shape, BF16),
                pltpu.VMEM((1, gate_bias.shape[0]), F32),
                pltpu.VMEM(cache_decay.shape, F32),
                pltpu.SMEM(lengths.shape, jnp.int32),
                pltpu.VMEM(parents.shape, jnp.int32),
                dma((9,)),
                pltpu.VMEM((seqs, props, all_w), F32),
                pltpu.VMEM((seqs,) + folded, BF16),
                pltpu.VMEM((seqs, props, all_w), F32),
                pltpu.VMEM((seqs,) + folded, BF16),
                pltpu.VMEM((n // 2 - 1, slots, props, all_w), F32),
                pltpu.VMEM((n // 2 - 1, slots) + folded, BF16),
                pltpu.VMEM((gate_weight.shape[1], depth), BF16),
                pltpu.VMEM(out_weight.shape, BF16),
                pltpu.VMEM(cache_keys.shape, BF16),
                pltpu.VMEM(cache_values.shape, BF16),
                pltpu.VMEM((seqs,) + folded, BF16),
                pltpu.VMEM((seqs,) + folded, BF16),
                pltpu.VMEM((seqs, props, LANES), F32),
                pltpu.VMEM((n - 1, slots) + folded, BF16),
                pltpu.VMEM((n - 1, slots, props, LANES), F32),
                pltpu.VMEM((seqs,) + folded, BF16),
                pltpu.VMEM((slots, props, LANES), F32),
                pltpu.VMEM((slots, props, LANES), F32),
                pltpu.VMEM((slots, props, width), F32),
                pltpu.VMEM((slots, 2, props, LANES), F32),
                pltpu.VMEM((slots, 2, LANES, width), F32),
                pltpu.VMEM((n_tp, block, cols), BF16),
                pltpu.VMEM((n_tp - 1, block, cols), BF16),
                pltpu.VMEM((-(-seqs // 8) * 8, LANES), jnp.int32),
                dma((2,)),
                dma((2, seqs)),
                dma((2, seqs)),
                dma((2, seqs)),
                dma((2, seqs)),
                dma((2, n // 2 - 1, slots)),
                dma((slots, n - 1)),
                dma((seqs,)),
                dma((2, seqs)),
                dma((2, n - 1, slots)),
                dma((slots, n - 1)),
                dma((seqs,)),
                dma((n_tp,)),
                dma((n_tp - 1,)),
            ]
        return pl.pallas_call(
            body_of,
            out_shape=pltpu.VMEM((block, cols), BF16),
            in_specs=[hbm] * 13,
            out_specs=vmem,
            scratch_shapes=scratch,
            compiler_params=pltpu.CompilerParams(
                collective_id=0, has_side_effects=True, vmem_limit_bytes=67_043_328 - 131072
            ),
        )(
            tokens,
            norm_gain.reshape(1, depth),
            query_weight,
            key_weight,
            value_weight,
            gate_weight.T,
            gate_bias.reshape(1, gate_bias.shape[0]),
            out_weight,
            cache_keys,
            cache_values,
            cache_decay,
            lengths,
            parents,
        )

    in_specs = (
        P(None, "kv"),
        P("kv"),
        P("kv", "tp"),
        P("kv", "tp"),
        P("kv", "tp"),
        P(),
        P(),
        P("tp", "kv"),
        P(None, "kv", "tp"),
        P(None, "kv", "tp"),
        P(None, "tp", "kv"),
        P(),
        P(),
    )
    out_specs = P("tp", "kv")
    return jax.shard_map(body, mesh=mesh, in_specs=in_specs, out_specs=out_specs, check_vma=False)
```
